512 devices in a mesh: sp: 32 (over z, x), tp: 16 (over y, core).
Axes of the slice: x: 4, y: 8, z: 8, core: 2. Of those that a mesh axis runs over, the one named last changes fastest.
Arguments:
- latent: bfloat16 [8192, 2048], P(('sp', 'tp')), may hold values from -6 to 6
- cond: float32 [2048], replicated, may hold values from -6 to 6
- ctx_mod: float32 [2048], replicated, may hold values from -6 to 6
- context: bfloat16 [512, 2048], P(('sp', 'tp')), may hold values from -6 to 6
- shift_w: float32 [2048, 2048], P('sp', 'tp'), may hold values from -0.125 to 0.125
- scale_w: float32 [2048, 2048], P('sp', 'tp'), may hold values from -0.125 to 0.125
- gate_w: float32 [2048, 2048], P('sp', 'tp'), may hold values from -0.125 to 0.125
- norm_gain: float32 [2048], replicated, may hold values from 0.1 to 1.9
- w_qn: bfloat16 [2048, 2048], P(None, 'tp'), may hold values from -0.125 to 0.125
- w_qr: bfloat16 [2048, 1024], P(None, 'tp'), may hold values from -0.13258252 to 0.13258252
- w_kv_down: bfloat16 [2048, 512], replicated, may hold values from -0.125 to 0.125
- w_rope_key: bfloat16 [2048, 64], replicated, may hold values from -0.13258252 to 0.13258252
- kv_gain: float32 [512], replicated, may hold values from 0.1 to 1.9
- w_key_up: bfloat16 [512, 2048], P(None, 'tp'), may hold values from -0.66015625 to 0.66015625
- w_value_up: bfloat16 [512, 2048], P(None, 'tp'), may hold values from -0.25 to 0.25
- ctx_bias: float32 [16], P('tp'), may hold values from 2 to 3.5
- w_out: bfloat16 [2048, 2048], P('tp'), may hold values from -0.52734375 to 0.52734375
Outputs:
- mixed: bfloat16 [8192, 2048], P(('sp', 'tp'))
The draws below stay inside these ranges and needn't reach their ends.
All inputs are finite; a program needn't handle non-finite values.
Results may differ from the reference program's by a relative error of at most 0.018.
Values may be sent and summed in bfloat16 or wider, within the bound.
No kernel may reach another device: no remote copies, remote signals or barrier semaphores. Data moves between devices by JAX's collectives and lax.ppermute only.
A program may use at most 64 MiB of HBM per device.

```python
import jax
import jax.numpy as jnp
from jax import lax

D = 2048
HEADS = 16
NOPE = 128
ROPE = 64
VDIM = 128
KV_RANK = 512
GRID_W = 128
CTX = 512
SEQ = 8192
HEADS_DEV = 1
N_TP = 16


def weight_base(key, shape):
    return jax.random.normal(key, shape, jnp.float32) * D ** (-0.5)


def draw_latent(key, part):
    tokens = jax.random.normal(jax.random.fold_in(key, 1), (SEQ, D), jnp.float32)
    return jnp.clip(tokens, -6.0, 6.0).astype(jnp.bfloat16)


def draw_w_qr(key, part):
    matrix = weight_base(jax.random.fold_in(key, 5), (D, HEADS * ROPE))
    bound = 6.0 * D ** (-0.5)
    return jnp.clip(matrix, -bound, bound).astype(jnp.bfloat16)


def draw_w_rope_key(key, part):
    matrix = weight_base(jax.random.fold_in(key, 6), (D, ROPE))
    bound = 6.0 * D ** (-0.5)
    return jnp.clip(matrix, -bound, bound).astype(jnp.bfloat16)


def steps_of(own_key, shape, cuts, smallest, largest):
    loudness = 1.0
    for position, shards_of in cuts:
        steps = jax.random.uniform(jax.random.fold_in(jax.random.fold_in(own_key, 6), position), (shards_of,), jnp.float32, smallest / len(cuts), largest / len(cuts))
        loudness = loudness * jnp.repeat(jnp.exp(steps), shape[position] // shards_of).reshape((-1,) + (1,) * (len(shape) - 1 - position))
    return loudness


def bell_draw(key, extent, deviation, most, split=(), kind=jnp.bfloat16):
    loudness = steps_of(key, extent, split, -0.22, 0.18) if split else 1.0
    array = jax.random.normal(key, extent, jnp.float32) * deviation * loudness
    return jnp.minimum(jnp.maximum(array, -most), most).astype(kind)


def setup_inputs(seed: int = 0) -> dict:
    seeds = jax.random.split(jax.random.key(seed), 18)
    return {
        "latent": draw_latent(jax.random.fold_in(seeds[17], 71), 0),
        "cond": bell_draw(seeds[1], (D,), 1.0, 6.0, (), jnp.float32),
        "ctx_mod": bell_draw(seeds[2], (D,), 1.0, 6.0, (), jnp.float32),
        "context": bell_draw(seeds[3], (CTX, D), 1.0, 6.0, ((0, 512),)),
        "shift_w": bell_draw(seeds[4], (D, D), D ** -0.5, 0.125, ((0, 32), (1, 16)), jnp.float32),
        "scale_w": bell_draw(seeds[5], (D, D), D ** -0.5, 0.125, ((0, 32), (1, 16)), jnp.float32),
        "gate_w": bell_draw(seeds[6], (D, D), D ** -0.5, 0.125, ((0, 32), (1, 16)), jnp.float32),
        "norm_gain": jnp.clip(1.0 + 0.18 * jax.random.normal(seeds[7], (D,), jnp.float32), 0.1, 1.9),
        "w_qn": bell_draw(seeds[8], (D, HEADS * NOPE), D ** -0.5, 0.125, ((1, 16),)),
        "w_qr": draw_w_qr(jax.random.fold_in(seeds[17], 71), 0),
        "w_kv_down": bell_draw(seeds[10], (D, KV_RANK), D ** -0.5, 0.125),
        "w_rope_key": draw_w_rope_key(jax.random.fold_in(seeds[17], 71), 0),
        "kv_gain": jnp.clip(1.0 + 0.18 * jax.random.normal(seeds[12], (KV_RANK,), jnp.float32), 0.1, 1.9),
        "w_key_up": bell_draw(seeds[13], (KV_RANK, HEADS * NOPE), (2.5 * KV_RANK ** -0.5), 0.66015625, ((1, 16),)),
        "w_value_up": bell_draw(seeds[14], (KV_RANK, HEADS * VDIM), KV_RANK ** -0.5, 0.25, ((1, 16),)),
        "ctx_bias": jnp.clip(2.0 + 1.5 * jax.random.uniform(seeds[15], (HEADS,), jnp.float32) ** steps_of(seeds[15], (HEADS,), ((0, 16),), -0.2, 0.2), 2.0, 3.5),
        "w_out": bell_draw(seeds[16], (HEADS * VDIM, D), (4.0 * (HEADS * VDIM) ** -0.5), 0.52734375, ((0, 16),)),
    }


EPS = 1e-06
ROPE_BASE = 10000.0

def modulate(rows_in, gain, shift, scale):
    values = rows_in.astype(jnp.float32)
    normed = values * lax.rsqrt(lax.optimization_barrier(jnp.mean(values * values, axis=-1, keepdims=True)) + EPS)
    return (normed * gain * (1.0 + scale) + shift).astype(jnp.bfloat16)

def compress(rows_in, w_kv_down, kv_gain):
    inner = jnp.dot(rows_in, w_kv_down, preferred_element_type=jnp.float32)
    normed = inner * lax.rsqrt(lax.optimization_barrier(jnp.mean(inner * inner, axis=-1, keepdims=True)) + EPS)
    return (normed * kv_gain).astype(jnp.bfloat16)

def angles(positions):
    quarter = ROPE // 4
    inverse = ROPE_BASE ** (-jnp.arange(quarter, dtype=jnp.float32) / quarter)
    row = (positions // GRID_W).astype(jnp.float32)
    column = (positions % GRID_W).astype(jnp.float32)
    return jnp.concatenate([row[:, None] * inverse[None, :], column[:, None] * inverse[None, :]], axis=-1)

def rotate(values, angle):
    pairs = values.reshape(values.shape[:-1] + (values.shape[-1] // 2, 2))
    first = pairs[..., 0]
    second = pairs[..., 1]
    cosine = jnp.cos(angle)
    sine = jnp.sin(angle)
    turned = jnp.stack([first * cosine - second * sine, first * sine + second * cosine], axis=-1)
    return turned.reshape(values.shape)

def reference(latent, cond, ctx_mod, context, shift_w, scale_w, gate_w, norm_gain, w_qn, w_qr, w_kv_down, w_rope_key, kv_gain, w_key_up, w_value_up, ctx_bias, w_out):
    pair = jnp.stack([jax.nn.silu(cond), jax.nn.silu(ctx_mod)])
    shift = jnp.dot(pair, shift_w, precision=lax.Precision.HIGHEST)
    scale = jnp.dot(pair, scale_w, precision=lax.Precision.HIGHEST)
    gate = jnp.dot(pair, gate_w, precision=lax.Precision.HIGHEST)
    h_rows = modulate(latent, norm_gain, shift[0], scale[0])
    h_ctx = modulate(context, norm_gain, shift[1], scale[1])
    turn = angles(jnp.arange(SEQ, dtype=jnp.int32))
    query_nope = jnp.dot(h_rows, w_qn, preferred_element_type=jnp.float32).astype(jnp.bfloat16)
    query_nope = query_nope.reshape(SEQ, HEADS, NOPE)
    query_rope = jnp.dot(h_rows, w_qr, preferred_element_type=jnp.float32).reshape(SEQ, HEADS, ROPE)
    query_rope = rotate(query_rope, turn[:, None, :]).astype(jnp.bfloat16)
    latents = jnp.concatenate([compress(h_rows, w_kv_down, kv_gain), compress(h_ctx, w_kv_down, kv_gain)], axis=0)
    rope_rows = rotate(jnp.dot(h_rows, w_rope_key, preferred_element_type=jnp.float32), turn).astype(jnp.bfloat16)
    rope_ctx = jnp.dot(h_ctx, w_rope_key, preferred_element_type=jnp.float32).astype(jnp.bfloat16)
    rope_keys = jnp.concatenate([rope_rows, rope_ctx], axis=0)
    total_keys = SEQ + CTX
    keys = jnp.dot(latents, w_key_up, preferred_element_type=jnp.float32).astype(jnp.bfloat16)
    keys = keys.reshape(total_keys, HEADS, NOPE).astype(jnp.float32)
    values = jnp.dot(latents, w_value_up, preferred_element_type=jnp.float32).astype(jnp.bfloat16)
    values = values.reshape(total_keys, HEADS, VDIM).astype(jnp.float32)
    rope_wide = rope_keys.astype(jnp.float32)
    is_ctx = jnp.concatenate([jnp.zeros((SEQ,), jnp.float32), jnp.ones((CTX,), jnp.float32)])
    offset = ctx_bias[:, None] * is_ctx[None, :]
    factor = (NOPE + ROPE) ** (-0.5)
    block = 512
    count = SEQ // block

    def attend(pieces):
        nope_block, rope_block = pieces
        scores = jnp.einsum('qhd,khd->hqk', nope_block.astype(jnp.float32), keys)
        scores = scores + jnp.einsum('qhr,kr->hqk', rope_block.astype(jnp.float32), rope_wide)
        scores = scores * factor + offset[:, None, :]
        top = lax.optimization_barrier(jnp.max(scores, axis=-1, keepdims=True))
        weights = jnp.exp(scores - top)
        total = lax.optimization_barrier(jnp.sum(weights, axis=-1))
        rounded = lax.optimization_barrier(weights.astype(jnp.bfloat16))
        mixed_heads = jnp.einsum('hqk,khd->qhd', rounded.astype(jnp.float32), values)
        result = mixed_heads / jnp.transpose(total)[:, :, None]
        return result.reshape(block, HEADS * VDIM).astype(jnp.bfloat16)
    attended = lax.map(attend, (query_nope.reshape(count, block, HEADS, NOPE), query_rope.reshape(count, block, HEADS, ROPE)))
    attended = attended.reshape(SEQ, HEADS * VDIM)
    group = HEADS_DEV * VDIM

    def add_group(index, total):
        part = lax.dynamic_slice_in_dim(attended, index * group, group, 1)
        rows_part = lax.dynamic_slice_in_dim(w_out, index * group, group, 0)
        term = jnp.dot(part, rows_part, preferred_element_type=jnp.float32).astype(jnp.bfloat16)
        term = lax.optimization_barrier(term)
        return total + term.astype(jnp.float32)
    branch = lax.fori_loop(0, N_TP, add_group, jnp.zeros((SEQ, D), jnp.float32))
    return (latent.astype(jnp.float32) + gate[0] * branch).astype(jnp.bfloat16)
```

```python
import functools

import jax
import jax.numpy as jnp
from jax import lax
from jax.experimental import pallas as pl
from jax.experimental.pallas import tpu as pltpu
from jax.sharding import Mesh
from jax.sharding import PartitionSpec as P

GRID_W = 128
EPS = 1e-06
ROPE_BASE = 10000.0
LOG2E = 1.4426950408889634
F32 = jnp.float32
BF16 = jnp.bfloat16
SP = ("za", "zb", "x")
TP = ("y", "c")
CORE_FIRST = ("c", "y")
KV_AXES = ("zb", "x")
Q_AXES = ("za",)


def copies(array, axes):
    n = lax.axis_size(axes)
    return lax.all_to_all(jnp.broadcast_to(array[None], (n, *array.shape)), axes, 0, 0, tiled=True)


def exchanged(array, axes):
    return lax.all_to_all(array, axes, 0, 0, tiled=True)


def modulate(rows_in, gain, shift, scale):
    values = rows_in.astype(F32)
    normed = values * lax.rsqrt(jnp.mean(values * values, axis=-1, keepdims=True) + EPS)
    return (normed * gain * (1.0 + scale) + shift).astype(BF16)


def angles(positions, rope_dim):
    quarter = rope_dim // 4
    inverse = ROPE_BASE ** (-jnp.arange(quarter, dtype=F32) / quarter)
    row = (positions // GRID_W).astype(F32)
    column = (positions % GRID_W).astype(F32)
    return jnp.concatenate([row[:, None] * inverse[None, :], column[:, None] * inverse[None, :]], axis=-1)


def split_pairs(weight):
    return jnp.concatenate([weight[:, 0::2], weight[:, 1::2]], axis=1)


def rotate_halves(values, cosine, sine):
    half = values.shape[-1] // 2
    first = values[:, :half]
    second = values[:, half:]
    return jnp.concatenate([first * cosine - second * sine, first * sine + second * cosine], axis=-1)


def attend_kernel(q_ref, k_ref, v_ref, b_ref, o_ref, s_ref, *, factor, latents):
    q = q_ref[...]
    dims = (((1,), (1,)), ((), ()))
    bias = b_ref[0, 0] * LOG2E
    main = lax.dot_general(q, k_ref[:latents], dims, preferred_element_type=F32) * (factor * LOG2E)
    side = lax.dot_general(q, k_ref[latents:], dims, preferred_element_type=F32) * (factor * LOG2E) + bias
    top = jnp.maximum(jnp.max(main, axis=1, keepdims=True), jnp.max(side, axis=1, keepdims=True))
    main = jnp.exp2(main - top)
    side = jnp.exp2(side - top)
    total = jnp.sum(main, axis=1, keepdims=True) + jnp.sum(side, axis=1, keepdims=True)
    out = jnp.dot(main.astype(BF16), v_ref[:latents], preferred_element_type=F32)
    out = out + jnp.dot(side.astype(BF16), v_ref[latents:], preferred_element_type=F32)
    o_ref[...] = (out / total).astype(BF16)
    s_ref[...] = top + jnp.log2(total)


def attend(queries, keys, values, bias, factor, latents):
    tile = 256
    count, width = queries.shape
    n_keys = keys.shape[0]
    vsize = values.shape[1]
    return pl.pallas_call(
        functools.partial(attend_kernel, factor=factor, latents=latents),
        grid=(count // tile,),
        in_specs=[
            pl.BlockSpec((tile, width), lambda i: (i, 0)),
            pl.BlockSpec((n_keys, width), lambda i: (0, 0)),
            pl.BlockSpec((n_keys, vsize), lambda i: (0, 0)),
            pl.BlockSpec((1, 1), lambda i: (0, 0), memory_space=pltpu.SMEM),
        ],
        out_specs=[pl.BlockSpec((tile, vsize), lambda i: (i, 0)), pl.BlockSpec((tile, 1), lambda i: (i, 0))],
        out_shape=[jax.ShapeDtypeStruct((count, vsize), BF16), jax.ShapeDtypeStruct((count, 1), F32)],
        name="attend",
    )(queries, keys, values, bias)


def three_parts(value):
    high = value.astype(BF16)
    rest = value - high.astype(F32)
    middle = rest.astype(BF16)
    low = (rest - middle.astype(F32)).astype(BF16)
    return jnp.stack([high, middle, low], axis=-2)


def body(
    latent, cond, ctx_mod, context, shift_w, scale_w, gate_w, norm_gain, w_qn, w_qr, w_kv_down, w_rope_key, kv_gain,
    w_key_up, w_value_up, ctx_bias, w_out,
):
    n_tp = lax.axis_size(TP)
    n_c = lax.axis_size("c")
    n_y = lax.axis_size("y")
    sp_index = lax.axis_index(SP)
    rows, width = latent.shape
    lanes = width // rows
    tok = rows * n_tp
    nope = w_key_up.shape[1]
    vsize = w_value_up.shape[1]
    rope = w_rope_key.shape[1]
    rank = w_kv_down.shape[1]
    factor = (nope + rope) ** (-0.5)

    raw = copies(jnp.concatenate([latent, context.reshape(rows, lanes)], axis=1), CORE_FIRST)

    feat = shift_w.shape[0]
    own = jnp.stack([lax.dynamic_slice_in_dim(v, sp_index * feat, feat) for v in (cond, ctx_mod)])
    own = jax.nn.silu(own)
    parts = [jnp.sum(own[i][:, None] * w, axis=0) for w, i in ((shift_w, 0), (shift_w, 1), (scale_w, 0), (scale_w, 1), (gate_w, 0))]
    summed = jnp.sum(copies(jnp.stack(parts), SP), axis=0)
    vectors = copies(summed, TP)
    vectors = jnp.moveaxis(vectors, 0, 1).reshape(5, width)
    gate = vectors[4]

    w_pair = copies(w_out, ("c",)).reshape(n_c * vsize, width)

    rows_all = raw[:, :, :width].reshape(tok, width)
    ctx_all = raw[:, :, width:].reshape(n_tp, width)
    h_rows = modulate(rows_all, norm_gain, vectors[0], vectors[2])
    h_ctx = modulate(ctx_all, norm_gain, vectors[1], vectors[3])
    h = jnp.concatenate([h_rows, h_ctx], axis=0)

    place = jnp.arange(tok, dtype=jnp.int32)
    place = (place // rows % n_y * n_c + place // (rows * n_y)) * rows + place % rows
    turn = angles(sp_index * tok + place, rope)
    cosine = jnp.cos(turn)
    sine = jnp.sin(turn)
    q_nope = jnp.dot(h_rows, w_qn, preferred_element_type=F32).astype(BF16)
    q_rope = rotate_halves(jnp.dot(h_rows, split_pairs(w_qr), preferred_element_type=F32), cosine, sine).astype(BF16)
    queries = copies(jnp.concatenate([q_nope, q_rope], axis=1), Q_AXES)
    n_q = queries.shape[0]
    queries = queries.reshape(n_q * tok, nope + rope)

    inner = jnp.dot(h, w_kv_down, preferred_element_type=F32)
    inner = (inner * lax.rsqrt(jnp.mean(inner * inner, axis=-1, keepdims=True) + EPS) * kv_gain).astype(BF16)
    k_rope = jnp.dot(h, split_pairs(w_rope_key), preferred_element_type=F32)
    k_rope = jnp.concatenate([rotate_halves(k_rope[:tok], cosine, sine), k_rope[tok:]], axis=0).astype(BF16)
    k_nope = jnp.dot(inner, w_key_up, preferred_element_type=F32).astype(BF16)
    value = jnp.dot(inner, w_value_up, preferred_element_type=F32).astype(BF16)
    kv = copies(jnp.concatenate([k_nope, k_rope, value], axis=1), KV_AXES)
    kv = jnp.concatenate([kv[:, :tok].reshape(-1, kv.shape[2]), kv[:, tok:].reshape(-1, kv.shape[2])], axis=0)
    n_keys = kv.shape[0]
    latents = n_keys // (tok + n_tp) * tok

    out, lse = attend(queries, kv[:, : nope + rope], kv[:, nope + rope :], ctx_bias.reshape(1, 1), factor, latents)

    half = tok // n_c
    out = out.reshape(n_q * n_c, half, vsize)
    stats = three_parts(lse.reshape(n_q * n_c, half))
    stats = jnp.pad(stats, ((0, 0), (0, 16 - stats.shape[1]), (0, vsize - half)))
    got = exchanged(jnp.concatenate([out, stats], axis=1), (*Q_AXES, "c")).reshape(n_q, n_c, half + 16, vsize)
    lse = jnp.sum(got[:, :, half : half + 3, :half].astype(F32), axis=2)
    share = jnp.exp2(lse - jnp.max(lse, axis=0))
    share = share / jnp.sum(share, axis=0)
    attended = jnp.sum(got[:, :, :half].astype(F32) * share[..., None], axis=0).astype(BF16)
    attended = jnp.moveaxis(attended, 0, 1).reshape(half, n_c * vsize)

    term = jnp.dot(attended, w_pair, preferred_element_type=F32).astype(BF16)
    branch = jnp.sum(exchanged(term.reshape(n_y, rows, width), ("y",)).astype(F32), axis=0)
    return (latent.astype(F32) + gate * branch).astype(BF16)


def solution(mesh):
    fine = Mesh(mesh.devices.reshape(4, 2, 4, 8, 2), ("za", "zb", "x", "y", "c"))
    row = P((*SP, *TP), None)
    placed = (
        row, P(), P(), row, P(SP, TP), P(SP, TP), P(SP, TP), P(), P(None, TP), P(None, TP), P(), P(), P(), P(None, TP),
        P(None, TP), P(TP), P(TP, None),
    )
    return jax.shard_map(body, mesh=fine, in_specs=placed, out_specs=row, check_vma=False)
```

```python
import functools

import jax
import jax.numpy as jnp
from jax import lax
from jax.experimental import pallas as pl
from jax.experimental.pallas import tpu as pltpu
from jax.sharding import Mesh
from jax.sharding import PartitionSpec as P

GRID_W = 128
EPS = 1e-06
ROPE_BASE = 10000.0
LOG2E = 1.4426950408889634
F32 = jnp.float32
BF16 = jnp.bfloat16
SP = ("za", "zb", "x")
TP = ("y", "c")
CORE_FIRST = ("c", "y")
KV_AXES = ("zb", "x")
Q_AXIS = "za"


def copies(array, axes):
    n = lax.axis_size(axes)
    return lax.all_to_all(jnp.broadcast_to(array[None], (n, *array.shape)), axes, 0, 0, tiled=True)


def exchanged(array, axes):
    return lax.all_to_all(array, axes, 0, 0, tiled=True)


def angles(positions, rope_dim):
    quarter = rope_dim // 4
    inverse = ROPE_BASE ** (-jnp.arange(quarter, dtype=F32) / quarter)
    row = (positions // GRID_W).astype(F32)
    column = (positions % GRID_W).astype(F32)
    return jnp.concatenate([row[:, None] * inverse[None, :], column[:, None] * inverse[None, :]], axis=-1)


def split_pairs(weight):
    return jnp.concatenate([weight[:, 0::2], weight[:, 1::2]], axis=1)


def shifted(array, axis, k):
    n = lax.axis_size(axis)
    return lax.ppermute(array, axis, [(i, (i + k) % n) for i in range(n)])


def three_parts(value):
    high = lax.reduce_precision(value, 8, 7)
    middle = lax.reduce_precision(value - high, 8, 7)
    return jnp.concatenate([high, middle, value - high - middle], axis=0).astype(BF16)


def project_kernel(raw_ref, gain_ref, kv_gain_ref, turn_ref, w_side_ref, w_down_ref, w_up_ref, q_ref, kv_ref, ctx_ref, h_ref, *, n_y, n_c):
    n_tp, rows, _ = raw_ref.shape
    tok = n_tp * rows
    width = gain_ref.shape[1]
    lanes = width // n_tp
    order = [c * n_y + y for y in range(n_y) for c in range(n_c)]
    vectors = []
    for j in range(5):
        pieces = []
        for t in order:
            part = [raw_ref[t, :, width + lanes :].astype(F32)[p * 5 + j : p * 5 + j + 1] for p in range(3)]
            pieces.append(part[0] + part[1] + part[2])
        vectors.append(jnp.concatenate(pieces, axis=1))
    gain = gain_ref[...]
    for t in range(n_tp):
        ctx_ref[t * rows : (t + 1) * rows, :] = raw_ref[t, :, width : width + lanes].astype(F32)
    context = jnp.concatenate([ctx_ref[pl.ds(i, n_tp, stride=rows), :] for i in range(rows)], axis=1)

    def modulated(values, shift, scale):
        normed = values * lax.rsqrt(jnp.mean(values * values, axis=1, keepdims=True) + EPS)
        return (normed * (gain * (1.0 + scale)) + shift).astype(BF16)

    for t in range(n_tp):
        h_ref[t * rows : (t + 1) * rows, :] = modulated(raw_ref[t, :, :width].astype(F32), vectors[0], vectors[2])
    h_ref[tok:, :] = modulated(context, vectors[1], vectors[3])
    h = h_ref[...]
    side = jnp.dot(h, w_side_ref[...], preferred_element_type=F32)
    q_ref[:tok, :] = side[:tok, :lanes].astype(BF16)
    pair = side[:, lanes:]
    own = pair[:tok]
    lane = lax.broadcasted_iota(jnp.int32, own.shape, 1)
    other = jnp.where(lane % (lanes // 2) < lanes // 4, pltpu.roll(own, lanes - lanes // 4, 1), pltpu.roll(own, lanes // 4, 1))
    turned = own * turn_ref[:, :lanes] + other * turn_ref[:, lanes:]
    half = tok // 2
    swapped = pltpu.roll(turned, lanes // 2, 1)
    low = lax.broadcasted_iota(jnp.int32, (half, lanes), 1) < lanes // 2
    q_ref[tok:, :] = jnp.where(low, turned[:half], swapped[half:]).astype(BF16)
    inner = jnp.dot(h, w_down_ref[...], preferred_element_type=F32)
    inner = inner * lax.rsqrt(jnp.mean(inner * inner, axis=1, keepdims=True) + EPS) * kv_gain_ref[...]
    both = jnp.dot(inner.astype(BF16), w_up_ref[...], preferred_element_type=F32).astype(BF16)
    count = tok + n_tp
    kv_ref[:count, :] = both[:, :lanes]
    kv_ref[count : 2 * count, :] = both[:, lanes:]
    kv_ref[2 * count : 2 * count + half, :] = jnp.where(low, swapped[:half], turned[half:]).astype(BF16)
    kv_ref[2 * count + half :, :] = pltpu.roll(pair[tok:], lanes // 2, 1).astype(BF16)


def attend_kernel(place_ref, bias_ref, q0, q1, q2, q3, kv_ref, o_ref, k_ref, kc_ref, vc_ref, *, factor, tok, n_ctx):
    n_blocks, _, lanes = kv_ref.shape
    count = tok + n_ctx
    half = tok // 2
    rope = lanes // 2
    for i in range(n_blocks):
        k_ref[i, :, :lanes] = kv_ref[i, :tok]
        k_ref[i, :half, lanes:] = kv_ref[i, 2 * count : 2 * count + half, :rope]
        k_ref[i, half:, lanes:] = kv_ref[i, 2 * count : 2 * count + half, rope:]
        at = slice(i * n_ctx, (i + 1) * n_ctx)
        kc_ref[at, :lanes] = kv_ref[i, tok:count]
        kc_ref[at, lanes:] = kv_ref[i, 2 * count + half :, :rope]
        vc_ref[at, :] = kv_ref[i, count + tok : 2 * count]
    dims = (((1,), (1,)), ((), ()))
    step = factor * LOG2E
    bias = bias_ref[0, 0] * LOG2E
    blocks = (q0, q1, q2, q3)
    for k, block in enumerate(blocks):
        to = (place_ref[0, 0] + (len(blocks) - k)) % len(blocks)
        for part in range(2):
            rows = slice(part * half, (part + 1) * half)
            q = jnp.concatenate([block[rows, :], block[tok:, part * rope : (part + 1) * rope]], axis=1)
            scores = [lax.dot_general(q, k_ref[i], dims, preferred_element_type=F32) * step for i in range(n_blocks)]
            scores.append(lax.dot_general(q, kc_ref[...], dims, preferred_element_type=F32) * step + bias)
            tops = [jnp.max(s, axis=1, keepdims=True) for s in scores]
            top = functools.reduce(jnp.maximum, tops)
            weights = [jnp.exp2(s - top) for s in scores]
            total = functools.reduce(jnp.add, [jnp.sum(w, axis=1, keepdims=True) for w in weights])
            values = [kv_ref[i, count : count + tok] for i in range(n_blocks)] + [vc_ref[...]]
            out = functools.reduce(
                jnp.add, [jnp.dot(w.astype(BF16), v, preferred_element_type=F32) for w, v in zip(weights, values, strict=True)]
            )
            o_ref[to, part, :half, :] = (out / total).astype(BF16)
            lse = jnp.transpose(jnp.broadcast_to(top + jnp.log2(total), (half, lanes)))[:16]
            high = lse.astype(BF16).astype(F32)
            middle = (lse - high).astype(BF16).astype(F32)
            row = lax.broadcasted_iota(jnp.int32, lse.shape, 0)
            stats = jnp.where(row == 0, high, jnp.where(row == 1, middle, jnp.where(row == 2, lse - high - middle, 0.0)))
            o_ref[to, part, half:, :] = stats.astype(BF16)


def body(
    latent, cond, ctx_mod, context, shift_w, scale_w, gate_w, norm_gain, w_qn, w_qr, w_kv_down, w_rope_key, kv_gain,
    w_key_up, w_value_up, ctx_bias, w_out,
):
    n_tp = lax.axis_size(TP)
    n_c = lax.axis_size("c")
    n_y = lax.axis_size("y")
    n_q = lax.axis_size(Q_AXIS)
    sp_index = lax.axis_index(SP)
    rows, width = latent.shape
    lanes = width // rows
    tok = rows * n_tp
    half = tok // n_c
    nope = w_key_up.shape[1]
    vsize = w_value_up.shape[1]
    rope = w_rope_key.shape[1]
    factor = (nope + rope) ** (-0.5)

    feat = shift_w.shape[0]
    own = jnp.stack([lax.dynamic_slice_in_dim(v, sp_index * feat, feat) for v in (cond, ctx_mod)])
    own = jax.nn.silu(own)
    parts = [jnp.sum(own[i][:, None] * w, axis=0) for w, i in ((shift_w, 0), (shift_w, 1), (scale_w, 0), (scale_w, 1), (gate_w, 0))]
    summed = jnp.sum(copies(jnp.stack(parts), SP), axis=0)

    w_other = shifted(w_out, "c", 1)
    first = lax.axis_index("c") == 0
    w_pair = jnp.concatenate([jnp.where(first, w_out, w_other), jnp.where(first, w_other, w_out)], axis=0)

    w_side = jnp.concatenate([w_qn, split_pairs(w_qr), split_pairs(w_rope_key)], axis=1)
    w_up = jnp.concatenate([w_key_up, w_value_up], axis=1)
    place = jnp.arange(tok, dtype=jnp.int32)
    place = (place // rows % n_y * n_c + place // (rows * n_y)) * rows + place % rows
    turn = angles(sp_index * tok + place, rope)
    cosine = jnp.cos(turn)
    sine = jnp.sin(turn)
    turn = jnp.concatenate([cosine] * 4 + [-sine, sine] * 2, axis=1)

    message = jnp.concatenate(
        [latent, context.reshape(rows, lanes), jnp.pad(three_parts(summed), ((0, rows - 15), (0, 0)))], axis=1
    )
    message, w_pair, w_side, w_up, turn = lax.optimization_barrier((message, w_pair, w_side, w_up, turn))
    raw = copies(message, CORE_FIRST)
    columns = raw[:, :15, width + lanes :].astype(F32).reshape(n_c, n_y, 3, 5, lanes)[:, :, :, 4]
    gate = jnp.transpose(jnp.sum(columns, axis=2), (1, 0, 2)).reshape(width)

    q_own, kv_own = pl.pallas_call(
        functools.partial(project_kernel, n_y=n_y, n_c=n_c),
        out_shape=[
            jax.ShapeDtypeStruct((tok + tok // 2, lanes), BF16),
            jax.ShapeDtypeStruct((2 * (tok + n_tp) + tok // 2 + n_tp, lanes), BF16),
        ],
        scratch_shapes=[pltpu.VMEM((tok, lanes), F32), pltpu.VMEM((tok + n_tp, width), BF16)],
        name="project",
    )(raw, norm_gain.reshape(1, width), kv_gain.reshape(1, -1), turn, w_side, w_kv_down, w_up)

    queries = [q_own] + [shifted(q_own, Q_AXIS, k) for k in range(1, n_q)]
    kv = copies(kv_own, KV_AXES)
    n_kv = kv.shape[0]
    vmem = pl.BlockSpec(memory_space=pltpu.VMEM)
    smem = pl.BlockSpec(memory_space=pltpu.SMEM)
    out = pl.pallas_call(
        functools.partial(attend_kernel, factor=factor, tok=tok, n_ctx=n_tp),
        in_specs=[smem, smem] + [vmem] * 5,
        out_specs=vmem,
        out_shape=jax.ShapeDtypeStruct((n_q, n_c, half + 16, vsize), BF16),
        scratch_shapes=[
            pltpu.VMEM((n_kv, tok, nope + rope), BF16),
            pltpu.VMEM((n_kv * n_tp, nope + rope), BF16),
            pltpu.VMEM((n_kv * n_tp, vsize), BF16),
        ],
        name="attend",
    )(lax.axis_index(Q_AXIS).astype(jnp.int32).reshape(1, 1), ctx_bias.reshape(1, 1), *queries, kv)

    got = exchanged(out.reshape(n_q * n_c, half + 16, vsize), (Q_AXIS, "c")).reshape(n_q, n_c, half + 16, vsize)
    lse = jnp.sum(got[:, :, half : half + 3, :half].astype(F32), axis=2)
    share = jnp.exp2(lse - jnp.max(lse, axis=0))
    share = share / jnp.sum(share, axis=0)
    attended = jnp.sum(got[:, :, :half].astype(F32) * share[..., None], axis=0).astype(BF16)
    attended = jnp.moveaxis(attended, 0, 1).reshape(half, n_c * vsize)

    term = jnp.dot(attended, w_pair, preferred_element_type=F32).astype(BF16)
    branch = jnp.sum(exchanged(term.reshape(n_y, rows, width), ("y",)).astype(F32), axis=0)
    return (latent.astype(F32) + gate * branch).astype(BF16)


def solution(mesh):
    fine = Mesh(mesh.devices.reshape(4, 2, 4, 8, 2), ("za", "zb", "x", "y", "c"))
    row = P((*SP, *TP), None)
    placed = (
        row, P(), P(), row, P(SP, TP), P(SP, TP), P(SP, TP), P(), P(None, TP), P(None, TP), P(), P(), P(), P(None, TP),
        P(None, TP), P(TP), P(TP, None),
    )
    return jax.shard_map(body, mesh=fine, in_specs=placed, out_specs=row, check_vma=False)
```

```python
import functools

import jax
import jax.numpy as jnp
from jax import lax
from jax.experimental import pallas as pl
from jax.experimental.pallas import tpu as pltpu
from jax.sharding import Mesh
from jax.sharding import PartitionSpec as P


GRID_W = 128
EPS = 1e-06
ROPE_BASE = 10000.0
LOG2E = 1.4426950408889634
F32 = jnp.float32
BF16 = jnp.bfloat16
SP = ("za", "zb", "x")
TP = ("y", "c")
KV_AXES = ("zb", "x")
Q_AXIS = "za"


def copies(array, axes):
    n = lax.axis_size(axes)
    return lax.all_to_all(jnp.broadcast_to(array[None], (n, *array.shape)), axes, 0, 0, tiled=True)


def exchanged(array, axes):
    return lax.all_to_all(array, axes, 0, 0, tiled=True)


def turn_table(positions, rope_dim, lanes):
    quarter = rope_dim // 4
    lane = jnp.arange(lanes, dtype=jnp.int32) % rope_dim
    inverse = ROPE_BASE ** (-(lane // 2 % quarter).astype(F32) / quarter)
    by_row = jnp.where(lane < rope_dim // 2, inverse, 0.0)
    by_column = jnp.where(lane < rope_dim // 2, 0.0, inverse)
    row = (positions // GRID_W).astype(F32)
    column = (positions % GRID_W).astype(F32)
    angle = row[:, None] * by_row[None, :] + column[:, None] * by_column[None, :]
    sign = jnp.where(lane % 2 == 0, -1.0, 1.0)
    return jnp.cos(angle), jnp.sin(angle) * sign[None, :]


def shifted(array, axis, k):
    n = lax.axis_size(axis)
    return lax.ppermute(array, axis, [(i, (i + k) % n) for i in range(n)])


def project_kernel(
    at_ref, own_ref, other_ref, vec_ref, gain_ref, kv_gain_ref, cos_ref, sin_ref, w_qn_ref, w_turn_ref, w_down_ref, w_key_ref, w_value_ref,
    q_ref, kv_ref, ctx_ref, h_ref,
):
    n_y, rows, _ = own_ref.shape
    tok = 2 * n_y * rows
    width = gain_ref.shape[1]
    lanes = width // rows
    n_ctx = 2 * n_y
    columns = jnp.concatenate([vec_ref[t] for t in range(vec_ref.shape[0])], axis=1)
    shift, shift_ctx, scale, scale_ctx = (columns[j : j + 1] for j in range(4))
    gain = gain_ref[...]

    def modulated(values, shift, scale):
        normed = values * lax.rsqrt(jnp.mean(values * values, axis=1, keepdims=True) + EPS)
        return (normed * (gain * (1.0 + scale)) + shift).astype(BF16)

    for side, ref in enumerate((own_ref, other_ref)):
        core = (at_ref[0, 1] + side) % 2
        for k in range(n_y):
            block = core * n_y + (at_ref[0, 0] + (n_y - k)) % n_y
            h_ref[pl.ds(pl.multiple_of(block * rows, rows), rows), :] = modulated(ref[k, :, :width].astype(F32), shift, scale)
            t = side * n_y + k
            ctx_ref[t * rows : (t + 1) * rows, :] = ref[k, :, width:].astype(F32)
    context = jnp.concatenate([ctx_ref[pl.ds(i, n_ctx, stride=rows), :] for i in range(rows)], axis=1)
    h_ref[tok:, :] = modulated(context, shift_ctx, scale_ctx)
    h = h_ref[...]
    q_ref[:tok, :] = jnp.dot(h[:tok], w_qn_ref[...], preferred_element_type=F32).astype(BF16)
    pair = lax.dot_general(h, w_turn_ref[...], (((1,), (1,)), ((), ())), preferred_element_type=F32)
    own = pair[:tok]
    lane = lax.broadcasted_iota(jnp.int32, own.shape, 1)
    other = jnp.where(lane % 2 == 0, pltpu.roll(own, lanes - 1, 1), pltpu.roll(own, 1, 1))
    turned = own * cos_ref[...] + other * sin_ref[...]
    half = tok // 2
    swapped = pltpu.roll(turned, lanes // 2, 1)
    low = lax.broadcasted_iota(jnp.int32, (half, lanes), 1) < lanes // 2
    q_ref[tok:, :] = jnp.where(low, turned[:half], swapped[half:]).astype(BF16)
    inner = jnp.dot(h, w_down_ref[...], preferred_element_type=F32)
    inner = (inner * lax.rsqrt(jnp.mean(inner * inner, axis=1, keepdims=True) + EPS) * kv_gain_ref[...]).astype(BF16)
    keys = jnp.dot(inner, w_key_ref[...], preferred_element_type=F32).astype(BF16)
    values = jnp.dot(inner, w_value_ref[...], preferred_element_type=F32).astype(BF16)
    turned = jnp.where(low, swapped[:half], turned[half:]).astype(BF16)
    still = pltpu.roll(pair[tok:], lanes // 2, 1).astype(BF16)
    count = tok + n_ctx
    for i in range(kv_ref.shape[0]):
        kv_ref[i, :count, :] = keys
        kv_ref[i, count : 2 * count, :] = values
        kv_ref[i, 2 * count : 2 * count + half, :] = turned
        kv_ref[i, 2 * count + half :, :] = still


def attend_kernel(place_ref, bias_ref, q0, q1, q2, q3, kv_ref, o_ref, k_ref, kc_ref, vc_ref, *, factor, tok, n_ctx):
    n_blocks, _, lanes = kv_ref.shape
    count = tok + n_ctx
    half = tok // 2
    rope = lanes // 2
    for i in range(n_blocks):
        k_ref[i, :, :lanes] = kv_ref[i, :tok]
        k_ref[i, :half, lanes:] = kv_ref[i, 2 * count : 2 * count + half, :rope]
        k_ref[i, half:, lanes:] = kv_ref[i, 2 * count : 2 * count + half, rope:]
        at = slice(i * n_ctx, (i + 1) * n_ctx)
        kc_ref[at, :lanes] = kv_ref[i, tok:count]
        kc_ref[at, lanes:] = kv_ref[i, 2 * count + half :, :rope]
        vc_ref[at, :] = kv_ref[i, count + tok : 2 * count]
    dims = (((1,), (1,)), ((), ()))
    step = factor * LOG2E
    bias = bias_ref[0, 0] * LOG2E
    blocks = (q0, q1, q2, q3)
    for k, block in enumerate(blocks):
        to = (place_ref[0, 0] + (len(blocks) - k)) % len(blocks)
        for part in range(2):
            rows = slice(part * half, (part + 1) * half)
            q = jnp.concatenate([block[rows, :], block[tok:, part * rope : (part + 1) * rope]], axis=1)
            scores = [lax.dot_general(q, k_ref[i], dims, preferred_element_type=F32) * step for i in range(n_blocks)]
            scores.append(lax.dot_general(q, kc_ref[...], dims, preferred_element_type=F32) * step + bias)
            tops = [jnp.max(s, axis=1, keepdims=True) for s in scores]
            top = functools.reduce(jnp.maximum, tops)
            weights = [jnp.exp2(s - top) for s in scores]
            total = functools.reduce(jnp.add, [jnp.sum(w, axis=1, keepdims=True) for w in weights])
            values = [kv_ref[i, count : count + tok] for i in range(n_blocks)] + [vc_ref[...]]
            out = functools.reduce(
                jnp.add, [jnp.dot(w.astype(BF16), v, preferred_element_type=F32) for w, v in zip(weights, values, strict=True)]
            )
            o_ref[to, part, :half, :] = (out / total).astype(BF16)
            lse = jnp.transpose(jnp.broadcast_to(top + jnp.log2(total), (half, lanes)))[:16]
            high = lse.astype(BF16).astype(F32)
            middle = (lse - high).astype(BF16).astype(F32)
            row = lax.broadcasted_iota(jnp.int32, lse.shape, 0)
            stats = jnp.where(row == 0, high, jnp.where(row == 1, middle, jnp.where(row == 2, lse - high - middle, 0.0)))
            o_ref[to, part, half:, :] = stats.astype(BF16)


def merge_kernel(at_ref, got_ref, w_own_ref, w_other_ref, o_ref):
    n_q, _, height, lanes = got_ref.shape
    half = height - 16
    n_y, rows, width = o_ref.shape
    term = None
    for side, w_ref in enumerate((w_own_ref, w_other_ref)):
        core = (at_ref[0, 0] + side) % 2
        lse = [jnp.sum(got_ref[i, core, half:, :].astype(F32), axis=0, keepdims=True) for i in range(n_q)]
        top = functools.reduce(jnp.maximum, lse)
        shares = [jnp.exp2(v - top) for v in lse]
        total = functools.reduce(jnp.add, shares)
        mixed = None
        for i in range(n_q):
            share = jnp.transpose(jnp.broadcast_to(shares[i] / total, (lanes, half)))
            piece = got_ref[i, core, :half, :].astype(F32) * share
            mixed = piece if mixed is None else mixed + piece
        out = jnp.dot(mixed.astype(BF16), w_ref[...], preferred_element_type=F32)
        term = out if term is None else term + out
    o_ref[...] = term.astype(BF16).reshape(n_y, rows, width)


def step(
    latent, cond, ctx_mod, context, shift_w, scale_w, gate_w, norm_gain, w_qn, w_qr, w_kv_down, w_rope_key, kv_gain,
    w_key_up, w_value_up, ctx_bias, w_out,
):
    n_tp = lax.axis_size(TP)
    n_c = lax.axis_size("c")
    n_y = lax.axis_size("y")
    n_q = lax.axis_size(Q_AXIS)
    sp_index = lax.axis_index(SP)
    rows, width = latent.shape
    lanes = width // rows
    tok = rows * n_tp
    half = tok // n_c
    nope = w_key_up.shape[1]
    vsize = w_value_up.shape[1]
    rope = w_rope_key.shape[1]
    factor = (nope + rope) ** (-0.5)

    block = jnp.concatenate([latent, context.reshape(rows, lanes)], axis=1)
    moved = [shifted(block, "y", k) for k in range(1, n_y)]
    mine = jnp.stack([block] + moved)
    other = shifted(mine, "c", 1)

    feat = shift_w.shape[0]
    own = jnp.stack([lax.dynamic_slice_in_dim(v, sp_index * feat, feat) for v in (cond, ctx_mod)])
    own = jax.nn.silu(own)
    parts = [jnp.sum(own[i][:, None] * w, axis=0) for w, i in ((shift_w, 0), (shift_w, 1), (scale_w, 0), (scale_w, 1), (gate_w, 0))]
    summed = copies(jnp.stack(parts), SP)
    summed = jnp.sum(summed, axis=0)
    vectors = copies(summed, TP)
    gate = vectors[:, 4].reshape(width)

    w_other = shifted(w_out, "c", 1)
    w_turn = jnp.concatenate([w_qr.T, w_rope_key.T], axis=0)
    place = jnp.arange(tok, dtype=jnp.int32)
    place = (place // rows % n_y * n_c + place // (rows * n_y)) * rows + place % rows
    cosine, sine = turn_table(sp_index * tok + place, rope, lanes)
    vectors, w_turn, cosine, sine, w_other = lax.optimization_barrier((vectors, w_turn, cosine, sine, w_other))

    at = jnp.stack([lax.axis_index("y"), lax.axis_index("c")]).astype(jnp.int32).reshape(1, 2)
    smem = pl.BlockSpec(memory_space=pltpu.SMEM)
    vmem = pl.BlockSpec(memory_space=pltpu.VMEM)
    q_own, kv_copies = pl.pallas_call(
        project_kernel,
        in_specs=[smem] + [vmem] * 12,
        out_specs=[vmem, vmem],
        out_shape=[
            jax.ShapeDtypeStruct((tok + tok // 2, lanes), BF16),
            jax.ShapeDtypeStruct((lax.axis_size(KV_AXES), 2 * (tok + n_tp) + tok // 2 + n_tp, lanes), BF16),
        ],
        scratch_shapes=[pltpu.VMEM((tok, lanes), F32), pltpu.VMEM((tok + n_tp, width), BF16)],
        name="project",
    )(
        at, mine, other, vectors, norm_gain.reshape(1, width), kv_gain.reshape(1, -1), cosine, sine, w_qn, w_turn, w_kv_down, w_key_up,
        w_value_up,
    )

    queries = [q_own] + [shifted(q_own, Q_AXIS, k) for k in range(1, n_q)]
    kv = exchanged(kv_copies, KV_AXES)
    n_kv = kv.shape[0]
    out = pl.pallas_call(
        functools.partial(attend_kernel, factor=factor, tok=tok, n_ctx=n_tp),
        in_specs=[smem, smem] + [vmem] * 5,
        out_specs=vmem,
        out_shape=jax.ShapeDtypeStruct((n_q, n_c, half + 16, vsize), BF16),
        scratch_shapes=[
            pltpu.VMEM((n_kv, tok, nope + rope), BF16),
            pltpu.VMEM((n_kv * n_tp, nope + rope), BF16),
            pltpu.VMEM((n_kv * n_tp, vsize), BF16),
        ],
        name="attend",
    )(lax.axis_index(Q_AXIS).astype(jnp.int32).reshape(1, 1), ctx_bias.reshape(1, 1), *queries, kv)

    got = exchanged(out.reshape(n_q * n_c, half + 16, vsize), (Q_AXIS, "c")).reshape(n_q, n_c, half + 16, vsize)
    term = pl.pallas_call(
        merge_kernel,
        in_specs=[smem] + [vmem] * 3,
        out_specs=vmem,
        out_shape=jax.ShapeDtypeStruct((n_y, rows, width), BF16),
        name="merge",
    )(lax.axis_index("c").astype(jnp.int32).reshape(1, 1), got, w_out, w_other)
    branch = jnp.sum(exchanged(term, ("y",)).astype(F32), axis=0)
    return (latent.astype(F32) + gate * branch).astype(BF16)


def solution(mesh):
    fine = Mesh(mesh.devices.reshape(4, 2, 4, 8, 2), ("za", "zb", "x", "y", "c"))
    row = P((*SP, *TP), None)
    placed = (
        row, P(), P(), row, P(SP, TP), P(SP, TP), P(SP, TP), P(), P(None, TP), P(None, TP), P(), P(), P(), P(None, TP),
        P(None, TP), P(TP), P(TP, None),
    )
    return jax.shard_map(step, mesh=fine, in_specs=placed, out_specs=row, check_vma=False)
```

```python
import functools

import jax
import jax.numpy as jnp
from jax import lax
from jax.experimental import pallas as pl
from jax.experimental.pallas import tpu as pltpu
from jax.sharding import Mesh
from jax.sharding import PartitionSpec as P


GRID_W = 128
EPS = 1e-06
ROPE_BASE = 10000.0
LOG2E = 1.4426950408889634
F32 = jnp.float32
BF16 = jnp.bfloat16
SP = ("z", "x")
TP = ("y", "c")
Q_AXIS = "x"


def copies(array, axes):
    n = lax.axis_size(axes)
    return lax.all_to_all(jnp.broadcast_to(array[None], (n, *array.shape)), axes, 0, 0, tiled=True)


def exchanged(array, axes):
    return lax.all_to_all(array, axes, 0, 0, tiled=True)


def turn_table(positions, rope_dim, lanes):
    quarter = rope_dim // 4
    lane = jnp.arange(lanes, dtype=jnp.int32) % rope_dim
    inverse = ROPE_BASE ** (-(lane // 2 % quarter).astype(F32) / quarter)
    by_row = jnp.where(lane < rope_dim // 2, inverse, 0.0)
    by_column = jnp.where(lane < rope_dim // 2, 0.0, inverse)
    row = (positions // GRID_W).astype(F32)
    column = (positions % GRID_W).astype(F32)
    angle = row[:, None] * by_row[None, :] + column[:, None] * by_column[None, :]
    sign = jnp.where(lane % 2 == 0, -1.0, 1.0)
    return jnp.cos(angle), jnp.sin(angle) * sign[None, :]


def shifted(array, axis, k):
    n = lax.axis_size(axis)
    return lax.ppermute(array, axis, [(i, (i + k) % n) for i in range(n)])


def ring_step(up, down, axis):
    return shifted(up, axis, 1), shifted(down, axis, lax.axis_size(axis) - 1)


def project_kernel(
    at_ref, own_ref, other_ref, vec_ref, gain_ref, kv_gain_ref, cos_ref, sin_ref, w_qn_ref, w_turn_ref, w_down_ref, w_key_ref, w_value_ref,
    q_ref, kv_ref, ctx_ref, h_ref,
):
    n_y, rows, _ = own_ref.shape
    tok = 2 * n_y * rows
    width = gain_ref.shape[1]
    lanes = width // rows
    n_ctx = 2 * n_y
    columns = jnp.concatenate([vec_ref[t] for t in range(vec_ref.shape[0])], axis=1)
    shift, shift_ctx, scale, scale_ctx = (columns[j : j + 1] for j in range(4))
    gain = gain_ref[...]

    def modulated(values, shift, scale):
        normed = values * lax.rsqrt(jnp.mean(values * values, axis=1, keepdims=True) + EPS)
        return (normed * (gain * (1.0 + scale)) + shift).astype(BF16)

    for side, ref in enumerate((own_ref, other_ref)):
        core = (at_ref[0, 1] + side) % 2
        for k in range(n_y):
            block = core * n_y + (at_ref[0, 0] + (n_y - k)) % n_y
            h_ref[pl.ds(pl.multiple_of(block * rows, rows), rows), :] = modulated(ref[k, :, :width].astype(F32), shift, scale)
            t = side * n_y + k
            ctx_ref[t * rows : (t + 1) * rows, :] = ref[k, :, width:].astype(F32)
    context = jnp.concatenate([ctx_ref[pl.ds(i, n_ctx, stride=rows), :] for i in range(rows)], axis=1)
    h_ref[tok:, :] = modulated(context, shift_ctx, scale_ctx)
    h = h_ref[...]
    query = jnp.dot(h[:tok], w_qn_ref[...], preferred_element_type=F32).astype(BF16)
    pair = lax.dot_general(h, w_turn_ref[...], (((1,), (1,)), ((), ())), preferred_element_type=F32)
    own = pair[:tok]
    lane = lax.broadcasted_iota(jnp.int32, own.shape, 1)
    other = jnp.where(lane % 2 == 0, pltpu.roll(own, lanes - 1, 1), pltpu.roll(own, 1, 1))
    turned = own * cos_ref[...] + other * sin_ref[...]
    half = tok // 2
    swapped = pltpu.roll(turned, lanes // 2, 1)
    low = lax.broadcasted_iota(jnp.int32, (half, lanes), 1) < lanes // 2
    query_turned = jnp.where(low, turned[:half], swapped[half:]).astype(BF16)
    for i in range(q_ref.shape[0]):
        q_ref[i, :tok, :] = query
        q_ref[i, tok:, :] = query_turned
    inner = jnp.dot(h, w_down_ref[...], preferred_element_type=F32)
    inner = (inner * lax.rsqrt(jnp.mean(inner * inner, axis=1, keepdims=True) + EPS) * kv_gain_ref[...]).astype(BF16)
    keys = jnp.dot(inner, w_key_ref[...], preferred_element_type=F32).astype(BF16)
    values = jnp.dot(inner, w_value_ref[...], preferred_element_type=F32).astype(BF16)
    turned = jnp.where(low, swapped[:half], turned[half:]).astype(BF16)
    still = pltpu.roll(pair[tok:], lanes // 2, 1).astype(BF16)
    count = tok + n_ctx
    kv_ref[:count, :] = keys
    kv_ref[count : 2 * count, :] = values
    kv_ref[2 * count : 2 * count + half, :] = turned
    kv_ref[2 * count + half :, :] = still


def attend_kernel(bias_ref, q_ref, *refs, n_blocks, first, last, factor, tok, n_ctx):
    kv_refs, refs = refs[:n_blocks], refs[n_blocks:]
    if not first:
        old_acc_ref, old_stat_ref, refs = refs[0], refs[1], refs[2:]
    if last:
        o_ref, refs = refs[0], refs[1:]
    else:
        acc_ref, stat_ref, refs = refs[0], refs[1], refs[2:]
    k_ref, kc_ref, vc_ref = refs
    lanes = q_ref.shape[2]
    count = tok + n_ctx
    half = tok // 2
    rope = lanes // 2
    for i, kv_ref in enumerate(kv_refs):
        k_ref[i, :, :lanes] = kv_ref[:tok]
        k_ref[i, :half, lanes:] = kv_ref[2 * count : 2 * count + half, :rope]
        k_ref[i, half:, lanes:] = kv_ref[2 * count : 2 * count + half, rope:]
        at = slice(i * n_ctx, (i + 1) * n_ctx)
        kc_ref[at, :lanes] = kv_ref[tok:count]
        kc_ref[at, lanes:] = kv_ref[2 * count + half :, :rope]
        vc_ref[at, :] = kv_ref[count + tok : 2 * count]
    dims = (((1,), (1,)), ((), ()))
    step = factor * LOG2E
    bias = bias_ref[0, 0] * LOG2E
    for k in range(q_ref.shape[0]):
        for part in range(2):
            rows = slice(part * half, (part + 1) * half)
            flat = slice(k * tok + part * half, k * tok + (part + 1) * half)
            q = jnp.concatenate([q_ref[k, rows, :], q_ref[k, tok:, part * rope : (part + 1) * rope]], axis=1)
            scores = [lax.dot_general(q, k_ref[i], dims, preferred_element_type=F32) * step for i in range(n_blocks)]
            scores.append(lax.dot_general(q, kc_ref[...], dims, preferred_element_type=F32) * step + bias)
            tops = [jnp.max(s, axis=1, keepdims=True) for s in scores]
            if not first:
                tops.append(old_stat_ref[flat, 0:1])
            top = functools.reduce(jnp.maximum, tops)
            weights = [jnp.exp2(s - top) for s in scores]
            total = functools.reduce(jnp.add, [jnp.sum(w, axis=1, keepdims=True) for w in weights])
            values = [kv_ref[count : count + tok] for kv_ref in kv_refs] + [vc_ref[...]]
            out = functools.reduce(
                jnp.add, [jnp.dot(w.astype(BF16), v, preferred_element_type=F32) for w, v in zip(weights, values, strict=True)]
            )
            if not first:
                kept = jnp.exp2(tops[-1] - top)
                total = total + old_stat_ref[flat, 1:2] * kept
                out = out + old_acc_ref[flat, :] * kept
            if not last:
                acc_ref[flat, :] = out
                lane = lax.broadcasted_iota(jnp.int32, (half, lanes), 1)
                stat_ref[flat, :] = jnp.where(lane == 0, top, total)
                continue
            o_ref[k, part, :half, :] = (out / total).astype(BF16)
            lse = jnp.transpose(jnp.broadcast_to(top + jnp.log2(total), (half, lanes)))[:16]
            high = lse.astype(BF16).astype(F32)
            middle = (lse - high).astype(BF16).astype(F32)
            row = lax.broadcasted_iota(jnp.int32, lse.shape, 0)
            stats = jnp.where(row == 0, high, jnp.where(row == 1, middle, jnp.where(row == 2, lse - high - middle, 0.0)))
            o_ref[k, part, half:, :] = stats.astype(BF16)


def attend(queries, blocks, state, bias, last, factor, tok, n_ctx):
    n_q, _, lanes = queries.shape
    n = len(blocks)
    vmem = pl.BlockSpec(memory_space=pltpu.VMEM)
    if last:
        out_shape = jax.ShapeDtypeStruct((n_q, 2, tok // 2 + 16, lanes), BF16)
        out_specs = vmem
    else:
        out_shape = [jax.ShapeDtypeStruct((n_q * tok, lanes), F32)] * 2
        out_specs = [vmem, vmem]
    return pl.pallas_call(
        functools.partial(attend_kernel, n_blocks=n, first=not state, last=last, factor=factor, tok=tok, n_ctx=n_ctx),
        in_specs=[pl.BlockSpec(memory_space=pltpu.SMEM)] + [vmem] * (1 + n + len(state)),
        out_specs=out_specs,
        out_shape=out_shape,
        scratch_shapes=[
            pltpu.VMEM((n, tok, lanes + lanes // 2), BF16),
            pltpu.VMEM((n * n_ctx, lanes + lanes // 2), BF16),
            pltpu.VMEM((n * n_ctx, lanes), BF16),
        ],
        name="attend",
    )(bias, queries, *blocks, *state)


def merge_kernel(at_ref, got_ref, w_own_ref, w_other_ref, o_ref):
    n_q, _, height, lanes = got_ref.shape
    half = height - 16
    n_y, rows, width = o_ref.shape
    term = None
    for side, w_ref in enumerate((w_own_ref, w_other_ref)):
        core = (at_ref[0, 0] + side) % 2
        lse = [jnp.sum(got_ref[i, core, half:, :].astype(F32), axis=0, keepdims=True) for i in range(n_q)]
        top = functools.reduce(jnp.maximum, lse)
        shares = [jnp.exp2(v - top) for v in lse]
        total = functools.reduce(jnp.add, shares)
        mixed = None
        for i in range(n_q):
            share = jnp.transpose(jnp.broadcast_to(shares[i] / total, (lanes, half)))
            piece = got_ref[i, core, :half, :].astype(F32) * share
            mixed = piece if mixed is None else mixed + piece
        out = jnp.dot(mixed.astype(BF16), w_ref[...], preferred_element_type=F32)
        term = out if term is None else term + out
    o_ref[...] = term.astype(BF16).reshape(n_y, rows, width)


def step(
    latent, cond, ctx_mod, context, shift_w, scale_w, gate_w, norm_gain, w_qn, w_qr, w_kv_down, w_rope_key, kv_gain,
    w_key_up, w_value_up, ctx_bias, w_out,
):
    n_tp = lax.axis_size(TP)
    n_c = lax.axis_size("c")
    n_y = lax.axis_size("y")
    n_q = lax.axis_size(Q_AXIS)
    sp_index = lax.axis_index(SP)
    rows, width = latent.shape
    lanes = width // rows
    tok = rows * n_tp
    half = tok // n_c
    nope = w_key_up.shape[1]
    vsize = w_value_up.shape[1]
    rope = w_rope_key.shape[1]
    factor = (nope + rope) ** (-0.5)

    block = jnp.concatenate([latent, context.reshape(rows, lanes)], axis=1)
    up1, down1 = ring_step(block, block, "y")
    up2, down2 = ring_step(up1, down1, "y")
    up3, down3 = ring_step(up2, down2, "y")
    up4 = shifted(up3, "y", 1)
    mine = jnp.stack([block, up1, up2, up3, up4, down3, down2, down1])
    other = shifted(mine, "c", 1)

    feat = shift_w.shape[0]
    own = jnp.stack([lax.dynamic_slice_in_dim(v, sp_index * feat, feat) for v in (cond, ctx_mod)])
    own = jax.nn.silu(own)
    parts = [jnp.sum(own[i][:, None] * w, axis=0) for w, i in ((shift_w, 0), (shift_w, 1), (scale_w, 0), (scale_w, 1), (gate_w, 0))]
    summed = copies(jnp.stack(parts), SP)
    summed = jnp.sum(summed, axis=0)
    vectors = copies(summed, TP)
    gate = vectors[:, 4].reshape(width)

    w_other = shifted(w_out, "c", 1)
    w_turn = jnp.concatenate([w_qr.T, w_rope_key.T], axis=0)
    place = jnp.arange(tok, dtype=jnp.int32)
    place = (place // rows % n_y * n_c + place // (rows * n_y)) * rows + place % rows
    cosine, sine = turn_table(sp_index * tok + place, rope, lanes)
    vectors, w_turn, cosine, sine, w_other = lax.optimization_barrier((vectors, w_turn, cosine, sine, w_other))

    at = jnp.stack([lax.axis_index("y"), lax.axis_index("c")]).astype(jnp.int32).reshape(1, 2)
    smem = pl.BlockSpec(memory_space=pltpu.SMEM)
    vmem = pl.BlockSpec(memory_space=pltpu.VMEM)
    q_copies, kv_own = pl.pallas_call(
        project_kernel,
        in_specs=[smem] + [vmem] * 12,
        out_specs=[vmem, vmem],
        out_shape=[
            jax.ShapeDtypeStruct((n_q, tok + tok // 2, lanes), BF16),
            jax.ShapeDtypeStruct((2 * (tok + n_tp) + tok // 2 + n_tp, lanes), BF16),
        ],
        scratch_shapes=[pltpu.VMEM((tok, lanes), F32), pltpu.VMEM((tok + n_tp, width), BF16)],
        name="project",
    )(
        at, mine, other, vectors, norm_gain.reshape(1, width), kv_gain.reshape(1, -1), cosine, sine, w_qn, w_turn, w_kv_down, w_key_up,
        w_value_up,
    )

    up1, down1 = ring_step(kv_own, kv_own, "z")
    queries = exchanged(q_copies, Q_AXIS)
    up2, down2 = ring_step(up1, down1, "z")
    up3, down3 = ring_step(up2, down2, "z")
    up4 = shifted(up3, "z", 1)
    bias = ctx_bias.reshape(1, 1)
    rest = (factor, tok, n_tp)
    state = attend(queries, [kv_own, up1, down1], [], bias, False, *rest)
    state = attend(queries, [up2, down2], state, bias, False, *rest)
    state = attend(queries, [up3, down3], state, bias, False, *rest)
    out = attend(queries, [up4], state, bias, True, *rest)

    got = exchanged(out.reshape(n_q * n_c, half + 16, vsize), (Q_AXIS, "c")).reshape(n_q, n_c, half + 16, vsize)
    term = pl.pallas_call(
        merge_kernel,
        in_specs=[smem] + [vmem] * 3,
        out_specs=vmem,
        out_shape=jax.ShapeDtypeStruct((n_y, rows, width), BF16),
        name="merge",
    )(lax.axis_index("c").astype(jnp.int32).reshape(1, 1), got, w_out, w_other)
    branch = jnp.sum(exchanged(term, ("y",)).astype(F32), axis=0)
    return (latent.astype(F32) + gate * branch).astype(BF16)


def solution(mesh):
    fine = Mesh(mesh.devices.reshape(8, 4, 8, 2), ("z", "x", "y", "c"))
    row = P((*SP, *TP), None)
    placed = (
        row, P(), P(), row, P(SP, TP), P(SP, TP), P(SP, TP), P(), P(None, TP), P(None, TP), P(), P(), P(), P(None, TP),
        P(None, TP), P(TP), P(TP, None),
    )
    return jax.shard_map(step, mesh=fine, in_specs=placed, out_specs=row, check_vma=False)
```

```python
import functools

import jax
import jax.numpy as jnp
from jax import lax
from jax.experimental import pallas as pl
from jax.experimental.pallas import tpu as pltpu
from jax.sharding import Mesh
from jax.sharding import PartitionSpec as P


GRID_W = 128
EPS = 1e-06
ROPE_BASE = 10000.0
LOG2E = 1.4426950408889634
F32 = jnp.float32
BF16 = jnp.bfloat16
SP = ("za", "zb", "x")
TP = ("y", "c")
KV_AXES = ("zb", "x")
Q_AXIS = "za"


def copies(array, axes):
    n = lax.axis_size(axes)
    return lax.all_to_all(jnp.broadcast_to(array[None], (n, *array.shape)), axes, 0, 0, tiled=True)


def exchanged(array, axes):
    return lax.all_to_all(array, axes, 0, 0, tiled=True)


def turn_table(positions, rope_dim, lanes):
    quarter = rope_dim // 4
    lane = jnp.arange(lanes, dtype=jnp.int32) % rope_dim
    inverse = ROPE_BASE ** (-(lane // 2 % quarter).astype(F32) / quarter)
    by_row = jnp.where(lane < rope_dim // 2, inverse, 0.0)
    by_column = jnp.where(lane < rope_dim // 2, 0.0, inverse)
    row = (positions // GRID_W).astype(F32)
    column = (positions % GRID_W).astype(F32)
    angle = row[:, None] * by_row[None, :] + column[:, None] * by_column[None, :]
    sign = jnp.where(lane % 2 == 0, -1.0, 1.0)
    return jnp.cos(angle), jnp.sin(angle) * sign[None, :]


def shifted(array, axis, k):
    n = lax.axis_size(axis)
    return lax.ppermute(array, axis, [(i, (i + k) % n) for i in range(n)])


def pack_kernel(sums_ref, block_ref, o_ref):
    n_sp = sums_ref.shape[0]
    rows, width = block_ref.shape
    total = functools.reduce(jnp.add, [sums_ref[i] for i in range(n_sp)])
    high = total.astype(BF16).astype(F32)
    middle = (total - high).astype(BF16).astype(F32)
    low = total - high - middle
    spare = jnp.zeros((rows - 3 * total.shape[0], total.shape[1]), F32)
    parts = jnp.concatenate([high, middle, low, spare], axis=0).astype(BF16)
    block = block_ref[...]
    for i in range(o_ref.shape[0]):
        o_ref[i, :, :width] = block
        o_ref[i, :, width:] = parts


def project_kernel(
    at_ref, own_ref, other_ref, gain_ref, kv_gain_ref, cos_ref, sin_ref, w_qn_ref, w_turn_ref, w_down_ref, w_key_ref, w_value_ref,
    q_ref, kv_ref, gate_ref, ctx_ref, h_ref,
):
    n_y, rows, _ = own_ref.shape
    side_rows = n_y * rows
    tok = 2 * side_rows
    width = gain_ref.shape[1]
    lanes = width // rows
    n_ctx = 2 * n_y
    core = at_ref[0, 0]
    columns = []
    for y in range(n_y):
        pair = []
        for ref in (own_ref, other_ref):
            part = ref[y, :, width + lanes :].astype(F32)
            pair.append(part[0:5] + part[5:10] + part[10:15])
        columns += [jnp.where(core == 0, pair[0], pair[1]), jnp.where(core == 0, pair[1], pair[0])]
    columns = jnp.concatenate(columns, axis=1)
    shift, shift_ctx, scale, scale_ctx = (columns[j : j + 1] for j in range(4))
    gate_ref[...] = columns[4:5]
    gain = gain_ref[...]

    def modulated(values, shift, scale):
        normed = values * lax.rsqrt(jnp.mean(values * values, axis=1, keepdims=True) + EPS)
        return (normed * (gain * (1.0 + scale)) + shift).astype(BF16)

    for side, ref in enumerate((own_ref, other_ref)):
        at = pl.multiple_of((core + side) % 2 * side_rows, side_rows)
        h_ref[pl.ds(at, side_rows), :] = modulated(ref[:, :, :width].reshape(side_rows, width).astype(F32), shift, scale)
        ctx_ref[side * side_rows : (side + 1) * side_rows, :] = (
            ref[:, :, width : width + lanes].reshape(side_rows, lanes).astype(F32)
        )
    context = jnp.concatenate([ctx_ref[pl.ds(i, n_ctx, stride=rows), :] for i in range(rows)], axis=1)
    h_ref[tok:, :] = modulated(context, shift_ctx, scale_ctx)
    h = h_ref[...]
    q_ref[:tok, :] = jnp.dot(h[:tok], w_qn_ref[...], preferred_element_type=F32).astype(BF16)
    pair = lax.dot_general(h, w_turn_ref[...], (((1,), (1,)), ((), ())), preferred_element_type=F32)
    own = pair[:tok]
    lane = lax.broadcasted_iota(jnp.int32, own.shape, 1)
    other = jnp.where(lane % 2 == 0, pltpu.roll(own, lanes - 1, 1), pltpu.roll(own, 1, 1))
    turned = own * cos_ref[...] + other * sin_ref[...]
    half = tok // 2
    swapped = pltpu.roll(turned, lanes // 2, 1)
    low = lax.broadcasted_iota(jnp.int32, (half, lanes), 1) < lanes // 2
    q_ref[tok:, :] = jnp.where(low, turned[:half], swapped[half:]).astype(BF16)
    inner = jnp.dot(h, w_down_ref[...], preferred_element_type=F32)
    inner = (inner * lax.rsqrt(jnp.mean(inner * inner, axis=1, keepdims=True) + EPS) * kv_gain_ref[...]).astype(BF16)
    keys = jnp.dot(inner, w_key_ref[...], preferred_element_type=F32).astype(BF16)
    values = jnp.dot(inner, w_value_ref[...], preferred_element_type=F32).astype(BF16)
    turned = jnp.where(low, swapped[:half], turned[half:]).astype(BF16)
    still = pltpu.roll(pair[tok:], lanes // 2, 1).astype(BF16)
    count = tok + n_ctx
    for i in range(kv_ref.shape[0]):
        kv_ref[i, :count, :] = keys
        kv_ref[i, count : 2 * count, :] = values
        kv_ref[i, 2 * count : 2 * count + half, :] = turned
        kv_ref[i, 2 * count + half :, :] = still


def attend_kernel(place_ref, bias_ref, q0, q1, q2, q3, kv_ref, o_ref, k_ref, kc_ref, vc_ref, *, factor, tok, n_ctx):
    n_blocks, _, lanes = kv_ref.shape
    count = tok + n_ctx
    half = tok // 2
    rope = lanes // 2
    for i in range(n_blocks):
        k_ref[i, :, :lanes] = kv_ref[i, :tok]
        k_ref[i, :half, lanes:] = kv_ref[i, 2 * count : 2 * count + half, :rope]
        k_ref[i, half:, lanes:] = kv_ref[i, 2 * count : 2 * count + half, rope:]
        at = slice(i * n_ctx, (i + 1) * n_ctx)
        kc_ref[at, :lanes] = kv_ref[i, tok:count]
        kc_ref[at, lanes:] = kv_ref[i, 2 * count + half :, :rope]
        vc_ref[at, :] = kv_ref[i, count + tok : 2 * count]
    dims = (((1,), (1,)), ((), ()))
    step = factor * LOG2E
    bias = bias_ref[0, 0] * LOG2E
    blocks = (q0, q1, q2, q3)
    size = len(blocks)
    values = [kv_ref[i, count : count + tok] for i in range(n_blocks)] + [vc_ref[...]]
    for first in range(0, size, 2):
        pieces = []
        for block in blocks[first : first + 2]:
            turned = jnp.concatenate([block[tok:, :rope], block[tok:, rope:]], axis=0)
            pieces.append(jnp.concatenate([block[:tok, :], turned], axis=1))
        q = jnp.concatenate(pieces, axis=0)
        scores = [lax.dot_general(q, k_ref[i], dims, preferred_element_type=F32) * step for i in range(n_blocks)]
        scores.append(lax.dot_general(q, kc_ref[...], dims, preferred_element_type=F32) * step + bias)
        widest = functools.reduce(jnp.maximum, scores[:-1])
        top = jnp.maximum(jnp.max(widest, axis=1, keepdims=True), jnp.max(scores[-1], axis=1, keepdims=True))
        weights = [jnp.exp2(s - top) for s in scores]
        total = jnp.sum(functools.reduce(jnp.add, weights[:-1]), axis=1, keepdims=True) + jnp.sum(weights[-1], axis=1, keepdims=True)
        out = functools.reduce(
            jnp.add, [jnp.dot(w.astype(BF16), v, preferred_element_type=F32) for w, v in zip(weights, values, strict=True)]
        )
        out = (out / total).astype(BF16)
        lse = jnp.transpose(jnp.broadcast_to(top + jnp.log2(total), (2 * tok, lanes)))[:16]
        high = lse.astype(BF16).astype(F32)
        middle = (lse - high).astype(BF16).astype(F32)
        row = lax.broadcasted_iota(jnp.int32, lse.shape, 0)
        stats = jnp.where(row == 0, high, jnp.where(row == 1, middle, jnp.where(row == 2, lse - high - middle, 0.0))).astype(BF16)
        for k in range(2):
            to = (place_ref[0, 0] + (size - first - k)) % size
            for part in range(2):
                rows = slice(k * tok + part * half, k * tok + (part + 1) * half)
                o_ref[to, part, :half, :] = out[rows]
                o_ref[to, part, half:, :] = stats[:, rows]


def merge_kernel(at_ref, got_ref, w_own_ref, w_other_ref, o_ref):
    n_q, _, height, lanes = got_ref.shape
    half = height - 16
    n_y, rows, width = o_ref.shape
    cores = [(at_ref[0, 0] + side) % 2 for side in range(2)]
    shares = []
    for core in cores:
        lse = [jnp.sum(got_ref[i, core, half:, :].astype(F32), axis=0, keepdims=True) for i in range(n_q)]
        top = functools.reduce(jnp.maximum, lse)
        raised = [jnp.exp2(v - top) for v in lse]
        total = functools.reduce(jnp.add, raised)
        shares += [v / total for v in raised]
    shares = jnp.transpose(jnp.concatenate(shares + [jnp.zeros((lanes - len(shares), half), F32)], axis=0))
    mixed = []
    for side, core in enumerate(cores):
        pieces = [got_ref[i, core, :half, :].astype(F32) * shares[:, side * n_q + i : side * n_q + i + 1] for i in range(n_q)]
        mixed.append(functools.reduce(jnp.add, pieces).astype(BF16))
    term = jnp.dot(mixed[0], w_own_ref[...], preferred_element_type=F32)
    term = term + jnp.dot(mixed[1], w_other_ref[...], preferred_element_type=F32)
    o_ref[...] = term.astype(BF16).reshape(n_y, rows, width)


def step(
    latent, cond, ctx_mod, context, shift_w, scale_w, gate_w, norm_gain, w_qn, w_qr, w_kv_down, w_rope_key, kv_gain,
    w_key_up, w_value_up, ctx_bias, w_out,
):
    n_tp = lax.axis_size(TP)
    n_c = lax.axis_size("c")
    n_y = lax.axis_size("y")
    n_q = lax.axis_size(Q_AXIS)
    sp_index = lax.axis_index(SP)
    rows, width = latent.shape
    lanes = width // rows
    tok = rows * n_tp
    half = tok // n_c
    nope = w_key_up.shape[1]
    vsize = w_value_up.shape[1]
    rope = w_rope_key.shape[1]
    factor = (nope + rope) ** (-0.5)

    feat = shift_w.shape[0]
    own = jnp.stack([lax.dynamic_slice_in_dim(v, sp_index * feat, feat) for v in (cond, ctx_mod)])
    own = jax.nn.silu(own)
    parts = [jnp.sum(own[i][:, None] * w, axis=0) for w, i in ((shift_w, 0), (shift_w, 1), (scale_w, 0), (scale_w, 1), (gate_w, 0))]
    summed = copies(jnp.stack(parts), SP)
    smem = pl.BlockSpec(memory_space=pltpu.SMEM)
    vmem = pl.BlockSpec(memory_space=pltpu.VMEM)
    block = jnp.concatenate([latent, context.reshape(rows, lanes)], axis=1)
    message = pl.pallas_call(
        pack_kernel,
        in_specs=[vmem, vmem],
        out_specs=vmem,
        out_shape=jax.ShapeDtypeStruct((n_y, rows, width + 2 * lanes), BF16),
        name="pack",
    )(summed, block)

    mine = exchanged(message, "y")
    other = shifted(mine, "c", 1)

    w_other = shifted(w_out, "c", 1)
    w_turn = jnp.concatenate([w_qr.T, w_rope_key.T], axis=0)
    place = jnp.arange(tok, dtype=jnp.int32)
    place = (place // rows % n_y * n_c + place // (rows * n_y)) * rows + place % rows
    cosine, sine = turn_table(sp_index * tok + place, rope, lanes)
    at = lax.axis_index("c").astype(jnp.int32).reshape(1, 1)
    to = lax.axis_index(Q_AXIS).astype(jnp.int32).reshape(1, 1)
    mine, w_turn, cosine, sine, w_other, at, to = lax.optimization_barrier((mine, w_turn, cosine, sine, w_other, at, to))

    q_own, kv_copies, gate = pl.pallas_call(
        project_kernel,
        in_specs=[smem] + [vmem] * 11,
        out_specs=[vmem, vmem, vmem],
        out_shape=[
            jax.ShapeDtypeStruct((tok + tok // 2, lanes), BF16),
            jax.ShapeDtypeStruct((lax.axis_size(KV_AXES), 2 * (tok + n_tp) + tok // 2 + n_tp, lanes), BF16),
            jax.ShapeDtypeStruct((1, width), F32),
        ],
        scratch_shapes=[pltpu.VMEM((tok, lanes), F32), pltpu.VMEM((tok + n_tp, width), BF16)],
        name="project",
    )(
        at, mine, other, norm_gain.reshape(1, width), kv_gain.reshape(1, -1), cosine, sine, w_qn, w_turn, w_kv_down, w_key_up,
        w_value_up,
    )

    queries = [q_own] + [shifted(q_own, Q_AXIS, k) for k in range(1, n_q)]
    kv = exchanged(kv_copies, KV_AXES)
    n_kv = kv.shape[0]
    out = pl.pallas_call(
        functools.partial(attend_kernel, factor=factor, tok=tok, n_ctx=n_tp),
        in_specs=[smem, smem] + [vmem] * 5,
        out_specs=vmem,
        out_shape=jax.ShapeDtypeStruct((n_q, n_c, half + 16, vsize), BF16),
        scratch_shapes=[
            pltpu.VMEM((n_kv, tok, nope + rope), BF16),
            pltpu.VMEM((n_kv * n_tp, nope + rope), BF16),
            pltpu.VMEM((n_kv * n_tp, vsize), BF16),
        ],
        name="attend",
    )(to, ctx_bias.reshape(1, 1), *queries, kv)

    got = exchanged(out.reshape(n_q * n_c, half + 16, vsize), (Q_AXIS, "c")).reshape(n_q, n_c, half + 16, vsize)
    term = pl.pallas_call(
        merge_kernel,
        in_specs=[smem] + [vmem] * 3,
        out_specs=vmem,
        out_shape=jax.ShapeDtypeStruct((n_y, rows, width), BF16),
        name="merge",
    )(at, got, w_out, w_other)
    branch = jnp.sum(exchanged(term, ("y",)).astype(F32), axis=0)
    return (latent.astype(F32) + gate * branch).astype(BF16)


def solution(mesh):
    fine = Mesh(mesh.devices.reshape(4, 2, 4, 8, 2), ("za", "zb", "x", "y", "c"))
    row = P((*SP, *TP), None)
    placed = (
        row, P(), P(), row, P(SP, TP), P(SP, TP), P(SP, TP), P(), P(None, TP), P(None, TP), P(), P(), P(), P(None, TP),
        P(None, TP), P(TP), P(TP, None),
    )
    return jax.shard_map(step, mesh=fine, in_specs=placed, out_specs=row, check_vma=False)
```

```python
import functools

import jax
import jax.numpy as jnp
from jax import lax
from jax.experimental import pallas as pl
from jax.experimental.pallas import tpu as pltpu
from jax.sharding import Mesh
from jax.sharding import PartitionSpec as P


GRID_W = 128
EPS = 1e-06
ROPE_BASE = 10000.0
LOG2E = 1.4426950408889634
F32 = jnp.float32
BF16 = jnp.bfloat16
SP = ("za", "zb", "x")
Y = ("ya", "yb")
TP = ("ya", "yb", "c")
KV_AXES = ("zb", "x")
Q_AXIS = "za"


def copies(array, axes):
    n = lax.axis_size(axes)
    return lax.all_to_all(jnp.broadcast_to(array[None], (n, *array.shape)), axes, 0, 0, tiled=True)


def exchanged(array, axes):
    return lax.all_to_all(array, axes, 0, 0, tiled=True)


def turn_table(positions, rope_dim, lanes):
    quarter = rope_dim // 4
    lane = jnp.arange(lanes, dtype=jnp.int32) % rope_dim
    inverse = ROPE_BASE ** (-(lane // 2 % quarter).astype(F32) / quarter)
    by_row = jnp.where(lane < rope_dim // 2, inverse, 0.0)
    by_column = jnp.where(lane < rope_dim // 2, 0.0, inverse)
    row = (positions // GRID_W).astype(F32)
    column = (positions % GRID_W).astype(F32)
    angle = row[:, None] * by_row[None, :] + column[:, None] * by_column[None, :]
    sign = jnp.where(lane % 2 == 0, -1.0, 1.0)
    return jnp.cos(angle), jnp.sin(angle) * sign[None, :]


def shifted(array, axis, k):
    n = lax.axis_size(axis)
    return lax.ppermute(array, axis, [(i, (i + k) % n) for i in range(n)])


def pack_kernel(sums_ref, block_ref, o_ref):
    n_sp = sums_ref.shape[0]
    rows, width = block_ref.shape
    total = functools.reduce(jnp.add, [sums_ref[i] for i in range(n_sp)])
    high = total.astype(BF16).astype(F32)
    middle = (total - high).astype(BF16).astype(F32)
    low = total - high - middle
    spare = jnp.zeros((rows - 3 * total.shape[0], total.shape[1]), F32)
    parts = jnp.concatenate([high, middle, low, spare], axis=0).astype(BF16)
    block = block_ref[...]
    for i in range(o_ref.shape[0]):
        o_ref[i, :, :width] = block
        o_ref[i, :, width:] = parts


def project_kernel(
    at_ref, own_ref, other_ref, gain_ref, kv_gain_ref, cos_ref, sin_ref, w_side_hbm, w_down_hbm, w_up_hbm,
    q_ref, kv_ref, gate_ref, ctx_ref, h_ref, w_side_ref, w_down_ref, w_up_ref, side_sem, down_sem, up_sem,
):
    loads = [
        pltpu.make_async_copy(w_side_hbm, w_side_ref, side_sem), pltpu.make_async_copy(w_down_hbm, w_down_ref, down_sem),
        pltpu.make_async_copy(w_up_hbm, w_up_ref, up_sem),
    ]
    for load in loads:
        load.start()
    n_y, rows, _ = own_ref.shape
    side_rows = n_y * rows
    tok = 2 * side_rows
    half = tok // 2
    width = gain_ref.shape[1]
    lanes = width // rows
    n_ctx = 2 * n_y
    core = at_ref[0, 0]
    columns = []
    for y in range(n_y):
        pair = []
        for ref in (own_ref, other_ref):
            part = ref[y, :, width + lanes :].astype(F32)
            pair.append(part[0:5] + part[5:10] + part[10:15])
        columns += [jnp.where(core == 0, pair[0], pair[1]), jnp.where(core == 0, pair[1], pair[0])]
    columns = jnp.concatenate(columns, axis=1)
    shift, shift_ctx, scale, scale_ctx = (columns[j : j + 1] for j in range(4))
    gate_ref[...] = columns[4:5]
    gain = gain_ref[...]

    def modulated(values, shift, scale):
        normed = values * lax.rsqrt(jnp.mean(values * values, axis=1, keepdims=True) + EPS)
        return (normed * (gain * (1.0 + scale)) + shift).astype(BF16)

    quarter = side_rows // 2
    for side, ref in enumerate((own_ref, other_ref)):
        ctx_ref[side * side_rows : (side + 1) * side_rows, :] = (
            ref[:, :, width : width + lanes].reshape(side_rows, lanes).astype(F32)
        )
        for yb in range(2):
            at = pl.multiple_of((yb * 2 + (core + side) % 2) * quarter, quarter)
            some = jnp.concatenate([ref[y, :, :width] for y in range(yb, n_y, 2)], axis=0)
            h_ref[pl.ds(at, quarter), :] = modulated(some.astype(F32), shift, scale)
    context = jnp.concatenate([ctx_ref[pl.ds(i, n_ctx, stride=rows), :] for i in range(rows)], axis=1)
    h_ref[tok:, :] = modulated(context, shift_ctx, scale_ctx)
    h = h_ref[...]
    loads[0].wait()
    mixed = jnp.dot(h, w_side_ref[...], preferred_element_type=F32)
    loads[1].wait()
    inner = jnp.dot(h, w_down_ref[...], preferred_element_type=F32)
    inner = (inner * lax.rsqrt(jnp.mean(inner * inner, axis=1, keepdims=True) + EPS) * kv_gain_ref[...]).astype(BF16)
    loads[2].wait()
    both = jnp.dot(inner, w_up_ref[...], preferred_element_type=F32).astype(BF16)
    q_ref[:tok, :] = mixed[:tok, :lanes].astype(BF16)
    pair = mixed[:, lanes:]
    own = pair[:tok]
    lane = lax.broadcasted_iota(jnp.int32, own.shape, 1)
    other = jnp.where(lane % 2 == 0, pltpu.roll(own, lanes - 1, 1), pltpu.roll(own, 1, 1))
    turned = own * cos_ref[...] + other * sin_ref[...]
    swapped = pltpu.roll(turned, lanes // 2, 1)
    low = lax.broadcasted_iota(jnp.int32, (half, lanes), 1) < lanes // 2
    q_ref[tok:, :] = jnp.where(low, turned[:half], swapped[half:]).astype(BF16)
    turned = jnp.where(low, swapped[:half], turned[half:]).astype(BF16)
    still = pltpu.roll(pair[tok:], lanes // 2, 1).astype(BF16)
    count = tok + n_ctx
    for i in range(kv_ref.shape[0]):
        kv_ref[i, :count, :] = both[:, :lanes]
        kv_ref[i, count : 2 * count, :] = both[:, lanes:]
        kv_ref[i, 2 * count : 2 * count + half, :] = turned
        kv_ref[i, 2 * count + half :, :] = still


def attend_kernel(place_ref, bias_ref, q0, q1, q2, q3, kv_ref, o_ref, k_ref, kc_ref, vc_ref, *, factor, tok, n_ctx):
    n_blocks, _, lanes = kv_ref.shape
    count = tok + n_ctx
    half = tok // 2
    rope = lanes // 2
    for i in range(n_blocks):
        k_ref[i, :, :lanes] = kv_ref[i, :tok]
        k_ref[i, :half, lanes:] = kv_ref[i, 2 * count : 2 * count + half, :rope]
        k_ref[i, half:, lanes:] = kv_ref[i, 2 * count : 2 * count + half, rope:]
        at = slice(i * n_ctx, (i + 1) * n_ctx)
        kc_ref[at, :lanes] = kv_ref[i, tok:count]
        kc_ref[at, lanes:] = kv_ref[i, 2 * count + half :, :rope]
        vc_ref[at, :] = kv_ref[i, count + tok : 2 * count]
    dims = (((1,), (1,)), ((), ()))
    step = factor * LOG2E
    bias = bias_ref[0, 0] * LOG2E
    blocks = (q0, q1, q2, q3)
    size = len(blocks)
    values = [kv_ref[i, count : count + tok] for i in range(n_blocks)] + [vc_ref[...]]
    for first in range(0, size, 2):
        pieces = []
        for block in blocks[first : first + 2]:
            turned = jnp.concatenate([block[tok:, :rope], block[tok:, rope:]], axis=0)
            pieces.append(jnp.concatenate([block[:tok, :], turned], axis=1))
        q = jnp.concatenate(pieces, axis=0)
        scores = [lax.dot_general(q, k_ref[i], dims, preferred_element_type=F32) * step for i in range(n_blocks)]
        scores.append(lax.dot_general(q, kc_ref[...], dims, preferred_element_type=F32) * step + bias)
        widest = functools.reduce(jnp.maximum, scores[:-1])
        top = jnp.maximum(jnp.max(widest, axis=1, keepdims=True), jnp.max(scores[-1], axis=1, keepdims=True))
        weights = [jnp.exp2(s - top) for s in scores]
        total = jnp.sum(functools.reduce(jnp.add, weights[:-1]), axis=1, keepdims=True) + jnp.sum(weights[-1], axis=1, keepdims=True)
        out = functools.reduce(
            jnp.add, [jnp.dot(w.astype(BF16), v, preferred_element_type=F32) for w, v in zip(weights, values, strict=True)]
        )
        out = (out / total).astype(BF16)
        lse = jnp.transpose(jnp.broadcast_to(top + jnp.log2(total), (2 * tok, lanes)))[:16]
        high = lse.astype(BF16).astype(F32)
        middle = (lse - high).astype(BF16).astype(F32)
        row = lax.broadcasted_iota(jnp.int32, lse.shape, 0)
        stats = jnp.where(row == 0, high, jnp.where(row == 1, middle, jnp.where(row == 2, lse - high - middle, 0.0))).astype(BF16)
        quarter = tok // 4
        for k in range(2):
            to = (place_ref[0, 0] + (size - first - k)) % size
            for part in range(4):
                at = k * tok + part * quarter
                o_ref[to, part, :quarter, :] = out[at : at + quarter]
                o_ref[to, part, quarter:, :quarter] = stats[:, at : at + quarter]
                o_ref[to, part, quarter:, quarter:] = jnp.zeros((16, lanes - quarter), BF16)


def merge_kernel(at_ref, got_ref, *refs):
    hbm, o_ref, w_refs, sems = refs[:4], refs[4], refs[5:9], refs[9:]
    loads = [pltpu.make_async_copy(src, dst, sem) for src, dst, sem in zip(hbm, w_refs, sems, strict=True)]
    for load in loads:
        load.start()
    n_q, _, height, lanes = got_ref.shape
    quarter = height - 16
    n_ya, rows, width = o_ref.shape
    core, yb = at_ref[0, 0], at_ref[0, 1]
    sources = [(yb + i) % 2 * 2 + (core + j) % 2 for i in range(2) for j in range(2)]
    shares = []
    for source in sources:
        lse = [jnp.sum(got_ref[i, source, quarter:, :].astype(F32), axis=0, keepdims=True) for i in range(n_q)]
        top = functools.reduce(jnp.maximum, lse)
        raised = [jnp.exp2(v - top) for v in lse]
        total = functools.reduce(jnp.add, raised)
        shares += [v / total for v in raised]
    shares = jnp.transpose(jnp.concatenate(shares + [jnp.zeros((lanes - len(shares), lanes), F32)], axis=0))[:quarter]
    term = None
    for s, source in enumerate(sources):
        pieces = [got_ref[i, source, :quarter, :].astype(F32) * shares[:, s * n_q + i : s * n_q + i + 1] for i in range(n_q)]
        mixed = functools.reduce(jnp.add, pieces).astype(BF16)
        loads[s].wait()
        out = jnp.dot(mixed, w_refs[s][...], preferred_element_type=F32)
        term = out if term is None else term + out
    o_ref[...] = term.astype(BF16).reshape(n_ya, rows, width)


def step(
    latent, cond, ctx_mod, context, shift_w, scale_w, gate_w, norm_gain, w_qn, w_qr, w_kv_down, w_rope_key, kv_gain,
    w_key_up, w_value_up, ctx_bias, w_out,
):
    n_tp = lax.axis_size(TP)
    n_c = lax.axis_size("c")
    n_y = lax.axis_size(Y)
    n_ya = lax.axis_size("ya")
    n_q = lax.axis_size(Q_AXIS)
    sp_index = lax.axis_index(SP)
    rows, width = latent.shape
    lanes = width // rows
    tok = rows * n_tp
    quarter = tok // (2 * n_c)
    nope = w_key_up.shape[1]
    vsize = w_value_up.shape[1]
    rope = w_rope_key.shape[1]
    factor = (nope + rope) ** (-0.5)

    feat = shift_w.shape[0]
    own = jnp.stack([lax.dynamic_slice_in_dim(v, sp_index * feat, feat) for v in (cond, ctx_mod)])
    own = jax.nn.silu(own)
    parts = [jnp.sum(own[i][:, None] * w, axis=0) for w, i in ((shift_w, 0), (shift_w, 1), (scale_w, 0), (scale_w, 1), (gate_w, 0))]
    summed = copies(jnp.stack(parts), SP)
    w_other = shifted(w_out, "c", 1)
    w_side = jnp.concatenate([w_qn, w_qr, w_rope_key], axis=1)
    w_up = jnp.concatenate([w_key_up, w_value_up], axis=1)
    place = jnp.arange(tok, dtype=jnp.int32)
    place = (place // rows % n_ya * 2 + place // (tok // 2)) * (n_c * rows) + place // quarter % n_c * rows + place % rows
    cosine, sine = turn_table(sp_index * tok + place, rope, lanes)
    at = jnp.stack([lax.axis_index("c"), lax.axis_index("yb")]).astype(jnp.int32).reshape(1, 2)
    to = lax.axis_index(Q_AXIS).astype(jnp.int32).reshape(1, 1)
    block = jnp.concatenate([latent, context.reshape(rows, lanes)], axis=1)
    block, w_side, w_up, cosine, sine, at, to = lax.optimization_barrier((block, w_side, w_up, cosine, sine, at, to))
    smem = pl.BlockSpec(memory_space=pltpu.SMEM)
    vmem = pl.BlockSpec(memory_space=pltpu.VMEM)
    any_space = pl.BlockSpec(memory_space=pl.ANY)
    pack = pl.pallas_call(
        pack_kernel,
        in_specs=[vmem, vmem],
        out_specs=vmem,
        out_shape=jax.ShapeDtypeStruct((n_y, rows, width + 2 * lanes), BF16),
        name="pack",
    )
    message = pack(summed, block)

    mine = exchanged(message, Y)
    other = shifted(mine, "c", 1)

    q_own, kv_copies, gate = pl.pallas_call(
        project_kernel,
        in_specs=[smem] + [vmem] * 6 + [any_space] * 3,
        out_specs=[vmem, vmem, vmem],
        out_shape=[
            jax.ShapeDtypeStruct((tok + tok // 2, lanes), BF16),
            jax.ShapeDtypeStruct((lax.axis_size(KV_AXES), 2 * (tok + n_tp) + tok // 2 + n_tp, lanes), BF16),
            jax.ShapeDtypeStruct((1, width), F32),
        ],
        scratch_shapes=[
            pltpu.VMEM((tok, lanes), F32),
            pltpu.VMEM((tok + n_tp, width), BF16),
            pltpu.VMEM(w_side.shape, BF16),
            pltpu.VMEM(w_kv_down.shape, BF16),
            pltpu.VMEM(w_up.shape, BF16),
            pltpu.SemaphoreType.DMA,
            pltpu.SemaphoreType.DMA,
            pltpu.SemaphoreType.DMA,
        ],
        name="project",
    )(at, mine, other, norm_gain.reshape(1, width), kv_gain.reshape(1, -1), cosine, sine, w_side, w_kv_down, w_up)

    queries = [q_own] + [shifted(q_own, Q_AXIS, k) for k in range(1, n_q)]
    kv = exchanged(kv_copies, KV_AXES)
    w_near = [shifted(w, "yb", 1) for w in (w_out, w_other)]
    n_kv = kv.shape[0]
    attend = pl.pallas_call(
        functools.partial(attend_kernel, factor=factor, tok=tok, n_ctx=n_tp),
        in_specs=[smem, smem] + [vmem] * 5,
        out_specs=vmem,
        out_shape=jax.ShapeDtypeStruct((n_q, 2 * n_c, quarter + 16, vsize), BF16),
        scratch_shapes=[
            pltpu.VMEM((n_kv, tok, nope + rope), BF16),
            pltpu.VMEM((n_kv * n_tp, nope + rope), BF16),
            pltpu.VMEM((n_kv * n_tp, vsize), BF16),
        ],
        name="attend",
    )
    out = attend(to, ctx_bias.reshape(1, 1), *queries, kv)

    got = exchanged(out.reshape(n_q * 2 * n_c, quarter + 16, vsize), (Q_AXIS, "yb", "c"))
    term = pl.pallas_call(
        merge_kernel,
        in_specs=[smem, vmem] + [any_space] * 4,
        out_specs=vmem,
        out_shape=jax.ShapeDtypeStruct((n_ya, rows, width), BF16),
        scratch_shapes=[pltpu.VMEM(w_out.shape, BF16)] * 4 + [pltpu.SemaphoreType.DMA] * 4,
        name="merge",
    )(at, got.reshape(n_q, 2 * n_c, quarter + 16, vsize), w_out, w_other, *w_near)
    branch = jnp.sum(exchanged(term, ("ya",)).astype(F32), axis=0)
    return (latent.astype(F32) + gate * branch).astype(BF16)


def solution(mesh):
    fine = Mesh(mesh.devices.reshape(4, 2, 4, 4, 2, 2), ("za", "zb", "x", "ya", "yb", "c"))
    row = P((*SP, *TP), None)
    placed = (
        row, P(), P(), row, P(SP, TP), P(SP, TP), P(SP, TP), P(), P(None, TP), P(None, TP), P(), P(), P(), P(None, TP),
        P(None, TP), P(TP), P(TP, None),
    )
    return jax.shard_map(step, mesh=fine, in_specs=placed, out_specs=row, check_vma=False)
```

```python
import functools

import jax
import jax.numpy as jnp
from jax import lax
from jax.experimental import pallas as pl
from jax.experimental.pallas import tpu as pltpu
from jax.sharding import Mesh
from jax.sharding import PartitionSpec as P


GRID_W = 128
EPS = 1e-06
ROPE_BASE = 10000.0
LOG2E = 1.4426950408889634
F32 = jnp.float32
BF16 = jnp.bfloat16
SP = ("za", "zb", "x")
Y = ("ya", "yb")
TP = ("ya", "yb", "c")
KV_AXES = ("zb", "x")
Q_AXIS = "za"


def copies(array, axes):
    n = lax.axis_size(axes)
    return lax.all_to_all(jnp.broadcast_to(array[None], (n, *array.shape)), axes, 0, 0, tiled=True)


def exchanged(array, axes):
    return lax.all_to_all(array, axes, 0, 0, tiled=True)


def turn_table(positions, rope_dim, lanes):
    quarter = rope_dim // 4
    lane = jnp.arange(lanes, dtype=jnp.int32) % rope_dim
    inverse = ROPE_BASE ** (-(lane // 2 % quarter).astype(F32) / quarter)
    by_row = jnp.where(lane < rope_dim // 2, inverse, 0.0)
    by_column = jnp.where(lane < rope_dim // 2, 0.0, inverse)
    row = (positions // GRID_W).astype(F32)
    column = (positions % GRID_W).astype(F32)
    angle = row[:, None] * by_row[None, :] + column[:, None] * by_column[None, :]
    sign = jnp.where(lane % 2 == 0, -1.0, 1.0)
    return jnp.cos(angle), jnp.sin(angle) * sign[None, :]


def shifted(array, axis, k):
    n = lax.axis_size(axis)
    return lax.ppermute(array, axis, [(i, (i + k) % n) for i in range(n)])


def pack_kernel(sums_ref, block_ref, o_ref):
    n_sp = sums_ref.shape[0]
    rows, width = block_ref.shape
    total = functools.reduce(jnp.add, [sums_ref[i] for i in range(n_sp)])
    high = total.astype(BF16).astype(F32)
    middle = (total - high).astype(BF16).astype(F32)
    low = total - high - middle
    spare = jnp.zeros((rows - 3 * total.shape[0], total.shape[1]), F32)
    parts = jnp.concatenate([high, middle, low, spare], axis=0).astype(BF16)
    block = block_ref[...]
    for i in range(o_ref.shape[0]):
        o_ref[i, :, :width] = block
        o_ref[i, :, width:] = parts


def project_kernel(
    at_ref, own_ref, other_ref, gain_ref, kv_gain_ref, cos_ref, sin_ref, w_side_hbm, w_down_hbm, w_up_hbm,
    q_ref, kv_ref, gate_ref, ctx_ref, h_ref, w_side_ref, w_down_ref, w_up_ref, side_sem, down_sem, up_sem,
):
    loads = [
        pltpu.make_async_copy(w_side_hbm, w_side_ref, side_sem), pltpu.make_async_copy(w_down_hbm, w_down_ref, down_sem),
        pltpu.make_async_copy(w_up_hbm, w_up_ref, up_sem),
    ]
    for load in loads:
        load.start()
    n_y, rows, _ = own_ref.shape
    side_rows = n_y * rows
    tok = 2 * side_rows
    half = tok // 2
    width = gain_ref.shape[1]
    lanes = width // rows
    n_ctx = 2 * n_y
    core = at_ref[0, 0]
    columns = []
    for y in range(n_y):
        pair = []
        for ref in (own_ref, other_ref):
            part = ref[y, :, width + lanes :].astype(F32)
            pair.append(part[0:5] + part[5:10] + part[10:15])
        columns += [jnp.where(core == 0, pair[0], pair[1]), jnp.where(core == 0, pair[1], pair[0])]
    columns = jnp.concatenate(columns, axis=1)
    shift, shift_ctx, scale, scale_ctx = (columns[j : j + 1] for j in range(4))
    gate_ref[...] = columns[4:5]
    gain = gain_ref[...]

    def modulated(values, shift, scale):
        normed = values * lax.rsqrt(jnp.mean(values * values, axis=1, keepdims=True) + EPS)
        return (normed * (gain * (1.0 + scale)) + shift).astype(BF16)

    quarter = side_rows // 2
    for side, ref in enumerate((own_ref, other_ref)):
        ctx_ref[side * side_rows : (side + 1) * side_rows, :] = (
            ref[:, :, width : width + lanes].reshape(side_rows, lanes).astype(F32)
        )
        for yb in range(2):
            at = pl.multiple_of((yb * 2 + (core + side) % 2) * quarter, quarter)
            some = jnp.concatenate([ref[y, :, :width] for y in range(yb, n_y, 2)], axis=0)
            h_ref[pl.ds(at, quarter), :] = modulated(some.astype(F32), shift, scale)
    context = jnp.concatenate([ctx_ref[pl.ds(i, n_ctx, stride=rows), :] for i in range(rows)], axis=1)
    h_ref[tok:, :] = modulated(context, shift_ctx, scale_ctx)
    h = h_ref[...]
    loads[0].wait()
    mixed = jnp.dot(h, w_side_ref[...], preferred_element_type=F32)
    loads[1].wait()
    inner = jnp.dot(h, w_down_ref[...], preferred_element_type=F32)
    inner = (inner * lax.rsqrt(jnp.mean(inner * inner, axis=1, keepdims=True) + EPS) * kv_gain_ref[...]).astype(BF16)
    loads[2].wait()
    both = jnp.dot(inner, w_up_ref[...], preferred_element_type=F32).astype(BF16)
    q_ref[:tok, :] = mixed[:tok, :lanes].astype(BF16)
    pair = mixed[:, lanes:]
    own = pair[:tok]
    lane = lax.broadcasted_iota(jnp.int32, own.shape, 1)
    other = jnp.where(lane % 2 == 0, pltpu.roll(own, lanes - 1, 1), pltpu.roll(own, 1, 1))
    turned = own * cos_ref[...] + other * sin_ref[...]
    swapped = pltpu.roll(turned, lanes // 2, 1)
    low = lax.broadcasted_iota(jnp.int32, (half, lanes), 1) < lanes // 2
    q_ref[tok:, :] = jnp.where(low, turned[:half], swapped[half:]).astype(BF16)
    turned = jnp.where(low, swapped[:half], turned[half:]).astype(BF16)
    still = pltpu.roll(pair[tok:], lanes // 2, 1).astype(BF16)
    count = tok + n_ctx
    for i in range(kv_ref.shape[0]):
        kv_ref[i, :count, :] = both[:, :lanes]
        kv_ref[i, count : 2 * count, :] = both[:, lanes:]
        kv_ref[i, 2 * count : 2 * count + half, :] = turned
        kv_ref[i, 2 * count + half :, :] = still


def attend_kernel(place_ref, bias_ref, q0, q1, q2, q3, kv_ref, o_ref, k_ref, kc_ref, vc_ref, *, factor, tok, n_ctx):
    n_blocks, _, lanes = kv_ref.shape
    count = tok + n_ctx
    half = tok // 2
    rope = lanes // 2
    for i in range(n_blocks):
        k_ref[i, :, :lanes] = kv_ref[i, :tok]
        k_ref[i, :half, lanes:] = kv_ref[i, 2 * count : 2 * count + half, :rope]
        k_ref[i, half:, lanes:] = kv_ref[i, 2 * count : 2 * count + half, rope:]
        at = slice(i * n_ctx, (i + 1) * n_ctx)
        kc_ref[at, :lanes] = kv_ref[i, tok:count]
        kc_ref[at, lanes:] = kv_ref[i, 2 * count + half :, :rope]
        vc_ref[at, :] = kv_ref[i, count + tok : 2 * count]
    dims = (((1,), (1,)), ((), ()))
    step = factor * LOG2E
    bias = bias_ref[0, 0] * LOG2E
    blocks = (q0, q1, q2, q3)
    size = len(blocks)
    values = [kv_ref[i, count : count + tok] for i in range(n_blocks)] + [vc_ref[...]]
    for first in range(0, size, 2):
        pieces = []
        for block in blocks[first : first + 2]:
            turned = jnp.concatenate([block[tok:, :rope], block[tok:, rope:]], axis=0)
            pieces.append(jnp.concatenate([block[:tok, :], turned], axis=1))
        q = jnp.concatenate(pieces, axis=0)
        scores = [lax.dot_general(q, k_ref[i], dims, preferred_element_type=F32) * step for i in range(n_blocks)]
        scores.append(lax.dot_general(q, kc_ref[...], dims, preferred_element_type=F32) * step + bias)
        widest = functools.reduce(jnp.maximum, scores[:-1])
        top = jnp.maximum(jnp.max(widest, axis=1, keepdims=True), jnp.max(scores[-1], axis=1, keepdims=True))
        weights = [jnp.exp2(s - top) for s in scores]
        total = jnp.sum(functools.reduce(jnp.add, weights[:-1]), axis=1, keepdims=True) + jnp.sum(weights[-1], axis=1, keepdims=True)
        out = functools.reduce(
            jnp.add, [jnp.dot(w.astype(BF16), v, preferred_element_type=F32) for w, v in zip(weights, values, strict=True)]
        )
        out = (out / total).astype(BF16)
        lse = jnp.transpose(jnp.broadcast_to(top + jnp.log2(total), (2 * tok, lanes)))[:16]
        high = lse.astype(BF16).astype(F32)
        middle = (lse - high).astype(BF16).astype(F32)
        row = lax.broadcasted_iota(jnp.int32, lse.shape, 0)
        stats = jnp.where(row == 0, high, jnp.where(row == 1, middle, jnp.where(row == 2, lse - high - middle, 0.0))).astype(BF16)
        quarter = tok // 4
        for k in range(2):
            to = (place_ref[0, 0] + (size - first - k)) % size
            for part in range(4):
                at = k * tok + part * quarter
                o_ref[to, part, :quarter, :] = out[at : at + quarter]
                o_ref[to, part, quarter:, :quarter] = stats[:, at : at + quarter]
                o_ref[to, part, quarter:, quarter:] = jnp.zeros((16, lanes - quarter), BF16)


def merge_kernel(at_ref, got_ref, *refs):
    hbm, o_ref, w_ref, sems = refs[:4], refs[4], refs[5], refs[6:]
    deep = hbm[0].shape[0]
    loads = [
        pltpu.make_async_copy(src, w_ref.at[pl.ds(i * deep, deep)], sem) for i, (src, sem) in enumerate(zip(hbm, sems, strict=True))
    ]
    for load in loads:
        load.start()
    n_q, _, height, lanes = got_ref.shape
    quarter = height - 16
    n_ya, rows, width = o_ref.shape
    core, yb = at_ref[0, 0], at_ref[0, 1]
    sources = [(yb + i) % 2 * 2 + (core + j) % 2 for i in range(2) for j in range(2)]
    shares = []
    for source in sources:
        lse = [jnp.sum(got_ref[i, source, quarter:, :].astype(F32), axis=0, keepdims=True) for i in range(n_q)]
        top = functools.reduce(jnp.maximum, lse)
        raised = [jnp.exp2(v - top) for v in lse]
        total = functools.reduce(jnp.add, raised)
        shares += [v / total for v in raised]
    shares = jnp.transpose(jnp.concatenate(shares + [jnp.zeros((lanes - len(shares), lanes), F32)], axis=0))[:quarter]
    mixed = []
    for s, source in enumerate(sources):
        pieces = [got_ref[i, source, :quarter, :].astype(F32) * shares[:, s * n_q + i : s * n_q + i + 1] for i in range(n_q)]
        mixed.append(functools.reduce(jnp.add, pieces).astype(BF16))
    for load in loads:
        load.wait()
    term = jnp.dot(jnp.concatenate(mixed, axis=1), w_ref[...], preferred_element_type=F32)
    o_ref[...] = term.astype(BF16).reshape(n_ya, rows, width)


def step(
    latent, cond, ctx_mod, context, shift_w, scale_w, gate_w, norm_gain, w_qn, w_qr, w_kv_down, w_rope_key, kv_gain,
    w_key_up, w_value_up, ctx_bias, w_out,
):
    n_tp = lax.axis_size(TP)
    n_c = lax.axis_size("c")
    n_y = lax.axis_size(Y)
    n_ya = lax.axis_size("ya")
    n_q = lax.axis_size(Q_AXIS)
    sp_index = lax.axis_index(SP)
    rows, width = latent.shape
    lanes = width // rows
    tok = rows * n_tp
    quarter = tok // (2 * n_c)
    nope = w_key_up.shape[1]
    vsize = w_value_up.shape[1]
    rope = w_rope_key.shape[1]
    factor = (nope + rope) ** (-0.5)

    feat = shift_w.shape[0]
    own = jnp.stack([lax.dynamic_slice_in_dim(v, sp_index * feat, feat) for v in (cond, ctx_mod)])
    own = jax.nn.silu(own)
    parts = [jnp.sum(own[i][:, None] * w, axis=0) for w, i in ((shift_w, 0), (shift_w, 1), (scale_w, 0), (scale_w, 1), (gate_w, 0))]
    summed = copies(jnp.stack(parts), SP)
    w_near = shifted(w_out, "yb", 1)
    block = jnp.concatenate([latent, context.reshape(rows, lanes)], axis=1)
    smem = pl.BlockSpec(memory_space=pltpu.SMEM)
    vmem = pl.BlockSpec(memory_space=pltpu.VMEM)
    any_space = pl.BlockSpec(memory_space=pl.ANY)
    pack = pl.pallas_call(
        pack_kernel,
        in_specs=[vmem, vmem],
        out_specs=vmem,
        out_shape=jax.ShapeDtypeStruct((n_y, rows, width + 2 * lanes), BF16),
        name="pack",
    )
    message = pack(summed, block)

    mine = exchanged(message, Y)
    w_other = shifted(w_out, "c", 1)
    w_far = shifted(w_near, "c", 1)
    w_side = jnp.concatenate([w_qn, w_qr, w_rope_key], axis=1)
    w_up = jnp.concatenate([w_key_up, w_value_up], axis=1)
    place = jnp.arange(tok, dtype=jnp.int32)
    place = (place // rows % n_ya * 2 + place // (tok // 2)) * (n_c * rows) + place // quarter % n_c * rows + place % rows
    cosine, sine = turn_table(sp_index * tok + place, rope, lanes)
    at = jnp.stack([lax.axis_index("c"), lax.axis_index("yb")]).astype(jnp.int32).reshape(1, 2)
    to = lax.axis_index(Q_AXIS).astype(jnp.int32).reshape(1, 1)
    other = shifted(mine, "c", 1)

    project = pl.pallas_call(
        project_kernel,
        in_specs=[smem] + [vmem] * 6 + [any_space] * 3,
        out_specs=[vmem, vmem, vmem],
        out_shape=[
            jax.ShapeDtypeStruct((tok + tok // 2, lanes), BF16),
            jax.ShapeDtypeStruct((lax.axis_size(KV_AXES), 2 * (tok + n_tp) + tok // 2 + n_tp, lanes), BF16),
            jax.ShapeDtypeStruct((1, width), F32),
        ],
        scratch_shapes=[
            pltpu.VMEM((tok, lanes), F32),
            pltpu.VMEM((tok + n_tp, width), BF16),
            pltpu.VMEM(w_side.shape, BF16),
            pltpu.VMEM(w_kv_down.shape, BF16),
            pltpu.VMEM(w_up.shape, BF16),
            pltpu.SemaphoreType.DMA,
            pltpu.SemaphoreType.DMA,
            pltpu.SemaphoreType.DMA,
        ],
        name="project",
    )
    q_own, kv_copies, gate = project(
        at, mine, other, norm_gain.reshape(1, width), kv_gain.reshape(1, -1), cosine, sine, w_side, w_kv_down, w_up
    )

    queries = [q_own] + [shifted(q_own, Q_AXIS, k) for k in range(1, n_q)]
    kv = exchanged(kv_copies, KV_AXES)
    n_kv = kv.shape[0]
    attend = pl.pallas_call(
        functools.partial(attend_kernel, factor=factor, tok=tok, n_ctx=n_tp),
        in_specs=[smem, smem] + [vmem] * 5,
        out_specs=vmem,
        out_shape=jax.ShapeDtypeStruct((n_q, 2 * n_c, quarter + 16, vsize), BF16),
        scratch_shapes=[
            pltpu.VMEM((n_kv, tok, nope + rope), BF16),
            pltpu.VMEM((n_kv * n_tp, nope + rope), BF16),
            pltpu.VMEM((n_kv * n_tp, vsize), BF16),
        ],
        name="attend",
    )
    out = attend(to, ctx_bias.reshape(1, 1), *queries, kv)

    got = exchanged(out.reshape(n_q * 2 * n_c, quarter + 16, vsize), (Q_AXIS, "yb", "c"))
    term = pl.pallas_call(
        merge_kernel,
        in_specs=[smem, vmem] + [any_space] * 4,
        out_specs=vmem,
        out_shape=jax.ShapeDtypeStruct((n_ya, rows, width), BF16),
        scratch_shapes=[pltpu.VMEM((4 * w_out.shape[0], width), BF16)] + [pltpu.SemaphoreType.DMA] * 4,
        name="merge",
    )(at, got.reshape(n_q, 2 * n_c, quarter + 16, vsize), w_out, w_other, w_near, w_far)
    branch = jnp.sum(exchanged(term, ("ya",)).astype(F32), axis=0)
    return (latent.astype(F32) + gate * branch).astype(BF16)


def solution(mesh):
    fine = Mesh(mesh.devices.reshape(4, 2, 4, 4, 2, 2), ("za", "zb", "x", "ya", "yb", "c"))
    row = P((*SP, *TP), None)
    placed = (
        row, P(), P(), row, P(SP, TP), P(SP, TP), P(SP, TP), P(), P(None, TP), P(None, TP), P(), P(), P(), P(None, TP),
        P(None, TP), P(TP), P(TP, None),
    )
    return jax.shard_map(step, mesh=fine, in_specs=placed, out_specs=row, check_vma=False)
```

```python
import functools

import jax
import jax.numpy as jnp
from jax import lax
from jax.experimental import pallas as pl
from jax.experimental.pallas import tpu as pltpu
from jax.sharding import Mesh
from jax.sharding import PartitionSpec as P


GRID_W = 128
EPS = 1e-06
ROPE_BASE = 10000.0
LOG2E = 1.4426950408889634
F32 = jnp.float32
BF16 = jnp.bfloat16
SP = ("za", "zb", "x")
Y = ("ya", "yb")
TP = ("ya", "yb", "c")
KV_AXES = ("zb", "x")
Q_AXIS = "za"


def copies(array, axes):
    n = lax.axis_size(axes)
    return lax.all_to_all(jnp.broadcast_to(array[None], (n, *array.shape)), axes, 0, 0, tiled=True)


def exchanged(array, axes):
    return lax.all_to_all(array, axes, 0, 0, tiled=True)


def turn_table(positions, rope_dim, lanes):
    quarter = rope_dim // 4
    lane = jnp.arange(lanes, dtype=jnp.int32) % rope_dim
    inverse = ROPE_BASE ** (-(lane // 2 % quarter).astype(F32) / quarter)
    by_row = jnp.where(lane < rope_dim // 2, inverse, 0.0)
    by_column = jnp.where(lane < rope_dim // 2, 0.0, inverse)
    row = (positions // GRID_W).astype(F32)
    column = (positions % GRID_W).astype(F32)
    angle = row[:, None] * by_row[None, :] + column[:, None] * by_column[None, :]
    sign = jnp.where(lane % 2 == 0, -1.0, 1.0)
    return jnp.cos(angle), jnp.sin(angle) * sign[None, :]


def shifted(array, axis, k):
    n = lax.axis_size(axis)
    return lax.ppermute(array, axis, [(i, (i + k) % n) for i in range(n)])


def project_kernel(
    at_ref, own_ref, other_ref, vec_ref, gain_ref, kv_gain_ref, cos_ref, sin_ref, w_side_hbm, w_down_hbm, w_up_hbm,
    q_ref, kv_ref, ctx_ref, h_ref, w_side_ref, w_down_ref, w_up_ref, side_sem, down_sem, up_sem,
):
    loads = [
        pltpu.make_async_copy(w_side_hbm, w_side_ref, side_sem), pltpu.make_async_copy(w_down_hbm, w_down_ref, down_sem),
        pltpu.make_async_copy(w_up_hbm, w_up_ref, up_sem),
    ]
    for load in loads:
        load.start()
    n_y, rows, _ = own_ref.shape
    side_rows = n_y * rows
    tok = 2 * side_rows
    half = tok // 2
    width = gain_ref.shape[1]
    lanes = width // rows
    n_ctx = 2 * n_y
    core = at_ref[0, 0]
    columns = jnp.concatenate([vec_ref[t] for t in range(vec_ref.shape[0])], axis=1)
    shift, shift_ctx, scale, scale_ctx = (columns[j : j + 1] for j in range(4))
    gain = gain_ref[...]

    def modulated(values, shift, scale):
        normed = values * lax.rsqrt(jnp.mean(values * values, axis=1, keepdims=True) + EPS)
        return (normed * (gain * (1.0 + scale)) + shift).astype(BF16)

    for side, ref in enumerate((own_ref, other_ref)):
        ctx_ref[side * side_rows : (side + 1) * side_rows, :] = ref[:, :, width:].reshape(side_rows, lanes).astype(F32)
        some = modulated(ref[:, :, :width].reshape(side_rows, width).astype(F32), shift, scale)
        for k in range(n_y):
            y = (at_ref[0, 2] + k) % n_y
            block = (y % 2 * 2 + (core + side) % 2) * (n_y // 2) + y // 2
            h_ref[pl.ds(pl.multiple_of(block * rows, rows), rows), :] = some[k * rows : (k + 1) * rows]
    context = jnp.concatenate([ctx_ref[pl.ds(i, n_ctx, stride=rows), :] for i in range(rows)], axis=1)
    h_ref[tok:, :] = modulated(context, shift_ctx, scale_ctx)
    h = h_ref[...]
    loads[0].wait()
    mixed = jnp.dot(h, w_side_ref[...], preferred_element_type=F32)
    loads[1].wait()
    inner = jnp.dot(h, w_down_ref[...], preferred_element_type=F32)
    inner = (inner * lax.rsqrt(jnp.mean(inner * inner, axis=1, keepdims=True) + EPS) * kv_gain_ref[...]).astype(BF16)
    loads[2].wait()
    both = jnp.dot(inner, w_up_ref[...], preferred_element_type=F32).astype(BF16)
    q_ref[:tok, :] = mixed[:tok, :lanes].astype(BF16)
    pair = mixed[:, lanes:]
    own = pair[:tok]
    lane = lax.broadcasted_iota(jnp.int32, own.shape, 1)
    other = jnp.where(lane % 2 == 0, pltpu.roll(own, lanes - 1, 1), pltpu.roll(own, 1, 1))
    turned = own * cos_ref[...] + other * sin_ref[...]
    swapped = pltpu.roll(turned, lanes // 2, 1)
    low = lax.broadcasted_iota(jnp.int32, (half, lanes), 1) < lanes // 2
    q_ref[tok:, :] = jnp.where(low, turned[:half], swapped[half:]).astype(BF16)
    turned = jnp.where(low, swapped[:half], turned[half:]).astype(BF16)
    still = pltpu.roll(pair[tok:], lanes // 2, 1).astype(BF16)
    count = tok + n_ctx
    for i in range(kv_ref.shape[0]):
        kv_ref[i, :count, :] = both[:, :lanes]
        kv_ref[i, count : 2 * count, :] = both[:, lanes:]
        kv_ref[i, 2 * count : 2 * count + half, :] = turned
        kv_ref[i, 2 * count + half :, :] = still


def attend_kernel(place_ref, bias_ref, q0, q1, q2, q3, kv_ref, o_ref, k_ref, kc_ref, vc_ref, *, factor, tok, n_ctx):
    n_blocks, _, lanes = kv_ref.shape
    count = tok + n_ctx
    half = tok // 2
    rope = lanes // 2
    for i in range(n_blocks):
        k_ref[i, :, :lanes] = kv_ref[i, :tok]
        k_ref[i, :half, lanes:] = kv_ref[i, 2 * count : 2 * count + half, :rope]
        k_ref[i, half:, lanes:] = kv_ref[i, 2 * count : 2 * count + half, rope:]
        at = slice(i * n_ctx, (i + 1) * n_ctx)
        kc_ref[at, :lanes] = kv_ref[i, tok:count]
        kc_ref[at, lanes:] = kv_ref[i, 2 * count + half :, :rope]
        vc_ref[at, :] = kv_ref[i, count + tok : 2 * count]
    dims = (((1,), (1,)), ((), ()))
    step = factor * LOG2E
    bias = bias_ref[0, 0] * LOG2E
    blocks = (q0, q1, q2, q3)
    size = len(blocks)
    values = [kv_ref[i, count : count + tok] for i in range(n_blocks)] + [vc_ref[...]]
    for first in range(0, size, 2):
        pieces = []
        for block in blocks[first : first + 2]:
            turned = jnp.concatenate([block[tok:, :rope], block[tok:, rope:]], axis=0)
            pieces.append(jnp.concatenate([block[:tok, :], turned], axis=1))
        q = jnp.concatenate(pieces, axis=0)
        scores = [lax.dot_general(q, k_ref[i], dims, preferred_element_type=F32) * step for i in range(n_blocks)]
        scores.append(lax.dot_general(q, kc_ref[...], dims, preferred_element_type=F32) * step + bias)
        widest = functools.reduce(jnp.maximum, scores[:-1])
        top = jnp.maximum(jnp.max(widest, axis=1, keepdims=True), jnp.max(scores[-1], axis=1, keepdims=True))
        weights = [jnp.exp2(s - top) for s in scores]
        total = jnp.sum(functools.reduce(jnp.add, weights[:-1]), axis=1, keepdims=True) + jnp.sum(weights[-1], axis=1, keepdims=True)
        out = functools.reduce(
            jnp.add, [jnp.dot(w.astype(BF16), v, preferred_element_type=F32) for w, v in zip(weights, values, strict=True)]
        )
        out = (out / total).astype(BF16)
        lse = jnp.transpose(jnp.broadcast_to(top + jnp.log2(total), (2 * tok, lanes)))[:16]
        high = lse.astype(BF16).astype(F32)
        middle = (lse - high).astype(BF16).astype(F32)
        row = lax.broadcasted_iota(jnp.int32, lse.shape, 0)
        stats = jnp.where(row == 0, high, jnp.where(row == 1, middle, jnp.where(row == 2, lse - high - middle, 0.0))).astype(BF16)
        quarter = tok // 4
        for k in range(2):
            to = (place_ref[0, 0] + (size - first - k)) % size
            for part in range(4):
                at = k * tok + part * quarter
                o_ref[to, part, :quarter, :] = out[at : at + quarter]
                o_ref[to, part, quarter:, :quarter] = stats[:, at : at + quarter]
                o_ref[to, part, quarter:, quarter:] = jnp.zeros((16, lanes - quarter), BF16)


def merge_kernel(at_ref, got_ref, *refs):
    hbm, o_ref, w_ref, sems = refs[:4], refs[4], refs[5], refs[6:]
    deep = hbm[0].shape[0]
    loads = [
        pltpu.make_async_copy(src, w_ref.at[pl.ds(i * deep, deep)], sem) for i, (src, sem) in enumerate(zip(hbm, sems, strict=True))
    ]
    for load in loads:
        load.start()
    n_q, _, height, lanes = got_ref.shape
    quarter = height - 16
    n_ya, rows, width = o_ref.shape
    core, yb = at_ref[0, 0], at_ref[0, 1]
    sources = [(yb + i) % 2 * 2 + (core + j) % 2 for i in range(2) for j in range(2)]
    shares = []
    for source in sources:
        lse = [jnp.sum(got_ref[i, source, quarter:, :].astype(F32), axis=0, keepdims=True) for i in range(n_q)]
        top = functools.reduce(jnp.maximum, lse)
        raised = [jnp.exp2(v - top) for v in lse]
        total = functools.reduce(jnp.add, raised)
        shares += [v / total for v in raised]
    shares = jnp.transpose(jnp.concatenate(shares + [jnp.zeros((lanes - len(shares), lanes), F32)], axis=0))[:quarter]
    mixed = []
    for s, source in enumerate(sources):
        pieces = [got_ref[i, source, :quarter, :].astype(F32) * shares[:, s * n_q + i : s * n_q + i + 1] for i in range(n_q)]
        mixed.append(functools.reduce(jnp.add, pieces).astype(BF16))
    for load in loads:
        load.wait()
    term = jnp.dot(jnp.concatenate(mixed, axis=1), w_ref[...], preferred_element_type=F32)
    o_ref[...] = term.astype(BF16).reshape(n_ya, rows, width)


def step(
    latent, cond, ctx_mod, context, shift_w, scale_w, gate_w, norm_gain, w_qn, w_qr, w_kv_down, w_rope_key, kv_gain,
    w_key_up, w_value_up, ctx_bias, w_out,
):
    n_tp = lax.axis_size(TP)
    n_c = lax.axis_size("c")
    n_y = lax.axis_size(Y)
    n_ya = lax.axis_size("ya")
    n_q = lax.axis_size(Q_AXIS)
    sp_index = lax.axis_index(SP)
    rows, width = latent.shape
    lanes = width // rows
    tok = rows * n_tp
    quarter = tok // (2 * n_c)
    nope = w_key_up.shape[1]
    vsize = w_value_up.shape[1]
    rope = w_rope_key.shape[1]
    factor = (nope + rope) ** (-0.5)

    block = jnp.concatenate([latent, context.reshape(rows, lanes)], axis=1)
    before = shifted(block, Y, 1)
    after = shifted(block, Y, n_y - 1)
    three = jnp.stack([before, block, after])
    behind = shifted(three, Y, 3)
    ahead = shifted(three[:2], Y, n_y - 3)
    mine = jnp.concatenate([block[None], after[None], ahead, behind, before[None]], axis=0)
    other = shifted(mine, "c", 1)

    feat = shift_w.shape[0]
    own = jnp.stack([lax.dynamic_slice_in_dim(v, sp_index * feat, feat) for v in (cond, ctx_mod)])
    own = jax.nn.silu(own)
    parts = [jnp.sum(own[i][:, None] * w, axis=0) for w, i in ((shift_w, 0), (shift_w, 1), (scale_w, 0), (scale_w, 1), (gate_w, 0))]
    summed = copies(jnp.stack(parts), SP)
    summed = jnp.sum(summed, axis=0)
    vectors = copies(summed, TP)
    gate = vectors[:, 4].reshape(width)
    w_near = shifted(w_out, "yb", 1)
    smem = pl.BlockSpec(memory_space=pltpu.SMEM)
    vmem = pl.BlockSpec(memory_space=pltpu.VMEM)
    any_space = pl.BlockSpec(memory_space=pl.ANY)
    w_other = shifted(w_out, "c", 1)
    w_far = shifted(w_near, "c", 1)
    w_side = jnp.concatenate([w_qn, w_qr, w_rope_key], axis=1)
    w_up = jnp.concatenate([w_key_up, w_value_up], axis=1)
    place = jnp.arange(tok, dtype=jnp.int32)
    place = (place // rows % n_ya * 2 + place // (tok // 2)) * (n_c * rows) + place // quarter % n_c * rows + place % rows
    cosine, sine = turn_table(sp_index * tok + place, rope, lanes)
    at = jnp.stack([lax.axis_index("c"), lax.axis_index("yb"), lax.axis_index(Y)]).astype(jnp.int32).reshape(1, 3)
    to = lax.axis_index(Q_AXIS).astype(jnp.int32).reshape(1, 1)
    project = pl.pallas_call(
        project_kernel,
        in_specs=[smem] + [vmem] * 7 + [any_space] * 3,
        out_specs=[vmem, vmem],
        out_shape=[
            jax.ShapeDtypeStruct((tok + tok // 2, lanes), BF16),
            jax.ShapeDtypeStruct((lax.axis_size(KV_AXES), 2 * (tok + n_tp) + tok // 2 + n_tp, lanes), BF16),
        ],
        scratch_shapes=[
            pltpu.VMEM((tok, lanes), F32),
            pltpu.VMEM((tok + n_tp, width), BF16),
            pltpu.VMEM(w_side.shape, BF16),
            pltpu.VMEM(w_kv_down.shape, BF16),
            pltpu.VMEM(w_up.shape, BF16),
            pltpu.SemaphoreType.DMA,
            pltpu.SemaphoreType.DMA,
            pltpu.SemaphoreType.DMA,
        ],
        name="project",
    )
    q_own, kv_copies = project(
        at, mine, other, vectors, norm_gain.reshape(1, width), kv_gain.reshape(1, -1), cosine, sine, w_side, w_kv_down, w_up
    )

    queries = [q_own] + [shifted(q_own, Q_AXIS, k) for k in range(1, n_q)]
    kv = exchanged(kv_copies, KV_AXES)
    n_kv = kv.shape[0]
    attend = pl.pallas_call(
        functools.partial(attend_kernel, factor=factor, tok=tok, n_ctx=n_tp),
        in_specs=[smem, smem] + [vmem] * 5,
        out_specs=vmem,
        out_shape=jax.ShapeDtypeStruct((n_q, 2 * n_c, quarter + 16, vsize), BF16),
        scratch_shapes=[
            pltpu.VMEM((n_kv, tok, nope + rope), BF16),
            pltpu.VMEM((n_kv * n_tp, nope + rope), BF16),
            pltpu.VMEM((n_kv * n_tp, vsize), BF16),
        ],
        name="attend",
    )
    out = attend(to, ctx_bias.reshape(1, 1), *queries, kv)

    got = exchanged(out.reshape(n_q * 2 * n_c, quarter + 16, vsize), (Q_AXIS, "yb", "c"))
    term = pl.pallas_call(
        merge_kernel,
        in_specs=[smem, vmem] + [any_space] * 4,
        out_specs=vmem,
        out_shape=jax.ShapeDtypeStruct((n_ya, rows, width), BF16),
        scratch_shapes=[pltpu.VMEM((4 * w_out.shape[0], width), BF16)] + [pltpu.SemaphoreType.DMA] * 4,
        name="merge",
    )(at, got.reshape(n_q, 2 * n_c, quarter + 16, vsize), w_out, w_other, w_near, w_far)
    branch = jnp.sum(exchanged(term, ("ya",)).astype(F32), axis=0)
    return (latent.astype(F32) + gate * branch).astype(BF16)


def solution(mesh):
    fine = Mesh(mesh.devices.reshape(4, 2, 4, 4, 2, 2), ("za", "zb", "x", "ya", "yb", "c"))
    row = P((*SP, *TP), None)
    placed = (
        row, P(), P(), row, P(SP, TP), P(SP, TP), P(SP, TP), P(), P(None, TP), P(None, TP), P(), P(), P(), P(None, TP),
        P(None, TP), P(TP), P(TP, None),
    )
    return jax.shard_map(step, mesh=fine, in_specs=placed, out_specs=row, check_vma=False)
```

```python
import functools

import jax
import jax.numpy as jnp
from jax import lax
from jax.experimental import pallas as pl
from jax.experimental.pallas import tpu as pltpu
from jax.sharding import Mesh
from jax.sharding import PartitionSpec as P


GRID_W = 128
EPS = 1e-06
ROPE_BASE = 10000.0
LOG2E = 1.4426950408889634
F32 = jnp.float32
BF16 = jnp.bfloat16
SP = ("za", "zb", "x")
Y = ("ya", "yb")
TP = ("ya", "yb", "c")
KV_AXES = ("zb", "x")
Q_AXIS = "za"


def exchanged(array, axes):
    return lax.all_to_all(array, axes, 0, 0, tiled=True)


def turn_table(positions, rope_dim, lanes):
    quarter = rope_dim // 4
    lane = jnp.arange(lanes, dtype=jnp.int32) % rope_dim
    inverse = ROPE_BASE ** (-(lane // 2 % quarter).astype(F32) / quarter)
    by_row = jnp.where(lane < rope_dim // 2, inverse, 0.0)
    by_column = jnp.where(lane < rope_dim // 2, 0.0, inverse)
    row = (positions // GRID_W).astype(F32)
    column = (positions % GRID_W).astype(F32)
    angle = row[:, None] * by_row[None, :] + column[:, None] * by_column[None, :]
    sign = jnp.where(lane % 2 == 0, -1.0, 1.0)
    return jnp.cos(angle), jnp.sin(angle) * sign[None, :]


def shifted(array, axis, k):
    n = lax.axis_size(axis)
    return lax.ppermute(array, axis, [(i, (i + k) % n) for i in range(n)])


def front_kernel(at_ref, cond_ref, mod_ref, shift_ref, scale_ref, gate_ref, o_ref):
    feat = shift_ref.shape[0]
    lanes = cond_ref.shape[1]
    per = lanes // feat
    rows = []
    for ref in (cond_ref, mod_ref):
        row = ref[pl.ds(at_ref[0, 0] // per, 1), :]
        row = jnp.where(at_ref[0, 0] % per == 0, row, pltpu.roll(row, lanes - feat, 1))
        rows.append(row / (1.0 + jnp.exp(-row)))
    pair = jnp.concatenate(rows + [jnp.zeros((6, lanes), F32)], axis=0)[:, :feat]
    shift, scale, gate = (
        jnp.dot(pair, ref[...], precision=lax.Precision.HIGHEST, preferred_element_type=F32) for ref in (shift_ref, scale_ref, gate_ref)
    )
    parts = jnp.concatenate([shift[:2], scale[:2], gate[:1]], axis=0)
    for i in range(o_ref.shape[0]):
        o_ref[i] = parts


def pack_kernel(sums_ref, block_ref, o_ref):
    n_sp = sums_ref.shape[0]
    rows, width = block_ref.shape
    total = functools.reduce(jnp.add, [sums_ref[i] for i in range(n_sp)])
    high = total.astype(BF16).astype(F32)
    middle = (total - high).astype(BF16).astype(F32)
    low = total - high - middle
    spare = jnp.zeros((rows - 3 * total.shape[0], total.shape[1]), F32)
    parts = jnp.concatenate([high, middle, low, spare], axis=0).astype(BF16)
    block = block_ref[...]
    for i in range(o_ref.shape[0]):
        o_ref[i, :, :width] = block
        o_ref[i, :, width:] = parts


def project_kernel(
    at_ref, own_ref, other_ref, gain_ref, kv_gain_ref, cos_ref, sin_ref, w_side_hbm, w_down_hbm, w_up_hbm,
    q_ref, kv_ref, gate_ref, ctx_ref, h_ref, w_side_ref, w_down_ref, w_up_ref, side_sem, down_sem, up_sem,
):
    loads = [
        pltpu.make_async_copy(w_side_hbm, w_side_ref, side_sem), pltpu.make_async_copy(w_down_hbm, w_down_ref, down_sem),
        pltpu.make_async_copy(w_up_hbm, w_up_ref, up_sem),
    ]
    for load in loads:
        load.start()
    n_y, rows, _ = own_ref.shape
    side_rows = n_y * rows
    tok = 2 * side_rows
    half = tok // 2
    width = gain_ref.shape[1]
    lanes = width // rows
    n_ctx = 2 * n_y
    core = at_ref[0, 0]
    columns = []
    for y in range(n_y):
        pair = []
        for ref in (own_ref, other_ref):
            part = ref[y, :, width + lanes :].astype(F32)
            pair.append(part[0:5] + part[5:10] + part[10:15])
        columns += [jnp.where(core == 0, pair[0], pair[1]), jnp.where(core == 0, pair[1], pair[0])]
    columns = jnp.concatenate(columns, axis=1)
    shift, shift_ctx, scale, scale_ctx = (columns[j : j + 1] for j in range(4))
    gate_ref[...] = columns[4:5]
    gain = gain_ref[...]

    def modulated(values, shift, scale):
        normed = values * lax.rsqrt(jnp.mean(values * values, axis=1, keepdims=True) + EPS)
        return (normed * (gain * (1.0 + scale)) + shift).astype(BF16)

    quarter = side_rows // 2
    for side, ref in enumerate((own_ref, other_ref)):
        ctx_ref[side * side_rows : (side + 1) * side_rows, :] = (
            ref[:, :, width : width + lanes].reshape(side_rows, lanes).astype(F32)
        )
        for yb in range(2):
            at = pl.multiple_of((yb * 2 + (core + side) % 2) * quarter, quarter)
            some = jnp.concatenate([ref[y, :, :width] for y in range(yb, n_y, 2)], axis=0)
            h_ref[pl.ds(at, quarter), :] = modulated(some.astype(F32), shift, scale)
    context = jnp.concatenate([ctx_ref[pl.ds(i, n_ctx, stride=rows), :] for i in range(rows)], axis=1)
    h_ref[tok:, :] = modulated(context, shift_ctx, scale_ctx)
    h = h_ref[...]
    loads[0].wait()
    mixed = jnp.dot(h, w_side_ref[...], preferred_element_type=F32)
    loads[1].wait()
    inner = jnp.dot(h, w_down_ref[...], preferred_element_type=F32)
    inner = (inner * lax.rsqrt(jnp.mean(inner * inner, axis=1, keepdims=True) + EPS) * kv_gain_ref[...]).astype(BF16)
    loads[2].wait()
    both = jnp.dot(inner, w_up_ref[...], preferred_element_type=F32).astype(BF16)
    q_ref[:tok, :] = mixed[:tok, :lanes].astype(BF16)
    pair = mixed[:, lanes:]
    own = pair[:tok]
    lane = lax.broadcasted_iota(jnp.int32, own.shape, 1)
    other = jnp.where(lane % 2 == 0, pltpu.roll(own, lanes - 1, 1), pltpu.roll(own, 1, 1))
    turned = own * cos_ref[...] + other * sin_ref[...]
    swapped = pltpu.roll(turned, lanes // 2, 1)
    low = lax.broadcasted_iota(jnp.int32, (half, lanes), 1) < lanes // 2
    q_ref[tok:, :] = jnp.where(low, turned[:half], swapped[half:]).astype(BF16)
    turned = jnp.where(low, swapped[:half], turned[half:]).astype(BF16)
    still = pltpu.roll(pair[tok:], lanes // 2, 1).astype(BF16)
    count = tok + n_ctx
    for i in range(kv_ref.shape[0]):
        kv_ref[i, :count, :] = both[:, :lanes]
        kv_ref[i, count : 2 * count, :] = both[:, lanes:]
        kv_ref[i, 2 * count : 2 * count + half, :] = turned
        kv_ref[i, 2 * count + half :, :] = still


def attend_kernel(place_ref, bias_ref, q0, q1, q2, q3, kv_ref, o_ref, k_ref, kc_ref, vc_ref, *, factor, tok, n_ctx):
    n_blocks, _, lanes = kv_ref.shape
    count = tok + n_ctx
    half = tok // 2
    rope = lanes // 2
    for i in range(n_blocks):
        k_ref[i, :, :lanes] = kv_ref[i, :tok]
        k_ref[i, :half, lanes:] = kv_ref[i, 2 * count : 2 * count + half, :rope]
        k_ref[i, half:, lanes:] = kv_ref[i, 2 * count : 2 * count + half, rope:]
        at = slice(i * n_ctx, (i + 1) * n_ctx)
        kc_ref[at, :lanes] = kv_ref[i, tok:count]
        kc_ref[at, lanes:] = kv_ref[i, 2 * count + half :, :rope]
        vc_ref[at, :] = kv_ref[i, count + tok : 2 * count]
    dims = (((1,), (1,)), ((), ()))
    step = factor * LOG2E
    bias = bias_ref[0, 0] * LOG2E
    blocks = (q0, q1, q2, q3)
    size = len(blocks)
    values = [kv_ref[i, count : count + tok] for i in range(n_blocks)] + [vc_ref[...]]
    quarter = tok // 4

    def scored(block):
        turned = jnp.concatenate([block[tok:, :rope], block[tok:, rope:]], axis=0)
        q = jnp.concatenate([block[:tok, :], turned], axis=1)
        scores = [lax.dot_general(q, k_ref[i], dims, preferred_element_type=F32) * step for i in range(n_blocks)]
        return scores + [lax.dot_general(q, kc_ref[...], dims, preferred_element_type=F32) * step + bias]

    ready = scored(blocks[0])
    for k in range(size):
        scores = ready
        if k + 1 < size:
            ready = scored(blocks[k + 1])
        widest = functools.reduce(jnp.maximum, scores[:-1])
        top = jnp.maximum(jnp.max(widest, axis=1, keepdims=True), jnp.max(scores[-1], axis=1, keepdims=True))
        weights = [jnp.exp2(s - top) for s in scores]
        total = jnp.sum(functools.reduce(jnp.add, weights[:-1]), axis=1, keepdims=True) + jnp.sum(weights[-1], axis=1, keepdims=True)
        out = functools.reduce(
            jnp.add, [jnp.dot(w.astype(BF16), v, preferred_element_type=F32) for w, v in zip(weights, values, strict=True)]
        )
        out = (out / total).astype(BF16)
        lse = jnp.transpose(jnp.broadcast_to(top + jnp.log2(total), (tok, lanes)))[:8]
        high = lse.astype(BF16).astype(F32)
        middle = (lse - high).astype(BF16).astype(F32)
        row = lax.broadcasted_iota(jnp.int32, lse.shape, 0)
        stats = jnp.where(row == 0, high, jnp.where(row == 1, middle, jnp.where(row == 2, lse - high - middle, 0.0))).astype(BF16)
        to = (place_ref[0, 0] + (size - k)) % size
        for part in range(4):
            at = part * quarter
            o_ref[to, part, :quarter, :] = out[at : at + quarter]
            o_ref[to, part, quarter:, :quarter] = stats[:, at : at + quarter]
            o_ref[to, part, quarter:, quarter:] = jnp.zeros((8, lanes - quarter), BF16)


def merge_kernel(at_ref, got_ref, *refs):
    hbm, o_ref, w_ref, sems = refs[:4], refs[4], refs[5], refs[6:]
    deep = hbm[0].shape[0]
    loads = [
        pltpu.make_async_copy(src, w_ref.at[pl.ds(i * deep, deep)], sem) for i, (src, sem) in enumerate(zip(hbm, sems, strict=True))
    ]
    for load in loads:
        load.start()
    n_q, _, height, lanes = got_ref.shape
    quarter = height - 8
    n_ya, rows, width = o_ref.shape
    core, yb = at_ref[0, 0], at_ref[0, 1]
    sources = [(yb + i) % 2 * 2 + (core + j) % 2 for i in range(2) for j in range(2)]
    shares = []
    for source in sources:
        lse = [jnp.sum(got_ref[i, source, quarter:, :].astype(F32), axis=0, keepdims=True) for i in range(n_q)]
        top = functools.reduce(jnp.maximum, lse)
        raised = [jnp.exp2(v - top) for v in lse]
        total = functools.reduce(jnp.add, raised)
        shares += [v / total for v in raised]
    shares = jnp.transpose(jnp.concatenate(shares + [jnp.zeros((lanes - len(shares), lanes), F32)], axis=0))[:quarter]
    mixed = []
    for s, source in enumerate(sources):
        pieces = [got_ref[i, source, :quarter, :].astype(F32) * shares[:, s * n_q + i : s * n_q + i + 1] for i in range(n_q)]
        mixed.append(functools.reduce(jnp.add, pieces).astype(BF16))
    for load in loads:
        load.wait()
    term = jnp.dot(jnp.concatenate(mixed, axis=1), w_ref[...], preferred_element_type=F32)
    o_ref[...] = term.astype(BF16).reshape(n_ya, rows, width)


def step(
    latent, cond, ctx_mod, context, shift_w, scale_w, gate_w, norm_gain, w_qn, w_qr, w_kv_down, w_rope_key, kv_gain,
    w_key_up, w_value_up, ctx_bias, w_out,
):
    n_tp = lax.axis_size(TP)
    n_c = lax.axis_size("c")
    n_y = lax.axis_size(Y)
    n_ya = lax.axis_size("ya")
    n_q = lax.axis_size(Q_AXIS)
    sp_index = lax.axis_index(SP)
    rows, width = latent.shape
    lanes = width // rows
    tok = rows * n_tp
    quarter = tok // (2 * n_c)
    nope = w_key_up.shape[1]
    vsize = w_value_up.shape[1]
    rope = w_rope_key.shape[1]
    factor = (nope + rope) ** (-0.5)

    smem = pl.BlockSpec(memory_space=pltpu.SMEM)
    vmem = pl.BlockSpec(memory_space=pltpu.VMEM)
    parts = pl.pallas_call(
        front_kernel,
        in_specs=[smem] + [vmem] * 5,
        out_specs=vmem,
        out_shape=jax.ShapeDtypeStruct((lax.axis_size(SP), 5, lanes), F32),
        name="front",
    )(sp_index.astype(jnp.int32).reshape(1, 1), cond.reshape(-1, lanes), ctx_mod.reshape(-1, lanes), shift_w, scale_w, gate_w)
    summed = exchanged(parts, SP)
    w_near = shifted(w_out, "yb", 1)
    block = jnp.concatenate([latent, context.reshape(rows, lanes)], axis=1)
    smem = pl.BlockSpec(memory_space=pltpu.SMEM)
    vmem = pl.BlockSpec(memory_space=pltpu.VMEM)
    any_space = pl.BlockSpec(memory_space=pl.ANY)
    pack = pl.pallas_call(
        pack_kernel,
        in_specs=[vmem, vmem],
        out_specs=vmem,
        out_shape=jax.ShapeDtypeStruct((n_y, rows, width + 2 * lanes), BF16),
        name="pack",
    )
    message = pack(summed, block)

    mine = exchanged(message, Y)
    w_other = shifted(w_out, "c", 1)
    w_far = shifted(w_near, "c", 1)
    w_side = jnp.concatenate([w_qn, w_qr, w_rope_key], axis=1)
    w_up = jnp.concatenate([w_key_up, w_value_up], axis=1)
    place = jnp.arange(tok, dtype=jnp.int32)
    place = (place // rows % n_ya * 2 + place // (tok // 2)) * (n_c * rows) + place // quarter % n_c * rows + place % rows
    cosine, sine = turn_table(sp_index * tok + place, rope, lanes)
    at = jnp.stack([lax.axis_index("c"), lax.axis_index("yb")]).astype(jnp.int32).reshape(1, 2)
    to = lax.axis_index(Q_AXIS).astype(jnp.int32).reshape(1, 1)
    other = shifted(mine, "c", 1)

    project = pl.pallas_call(
        project_kernel,
        in_specs=[smem] + [vmem] * 6 + [any_space] * 3,
        out_specs=[vmem, vmem, vmem],
        out_shape=[
            jax.ShapeDtypeStruct((tok + tok // 2, lanes), BF16),
            jax.ShapeDtypeStruct((lax.axis_size(KV_AXES), 2 * (tok + n_tp) + tok // 2 + n_tp, lanes), BF16),
            jax.ShapeDtypeStruct((1, width), F32),
        ],
        scratch_shapes=[
            pltpu.VMEM((tok, lanes), F32),
            pltpu.VMEM((tok + n_tp, width), BF16),
            pltpu.VMEM(w_side.shape, BF16),
            pltpu.VMEM(w_kv_down.shape, BF16),
            pltpu.VMEM(w_up.shape, BF16),
            pltpu.SemaphoreType.DMA,
            pltpu.SemaphoreType.DMA,
            pltpu.SemaphoreType.DMA,
        ],
        name="project",
    )
    q_own, kv_copies, gate = project(
        at, mine, other, norm_gain.reshape(1, width), kv_gain.reshape(1, -1), cosine, sine, w_side, w_kv_down, w_up
    )

    queries = [q_own] + [shifted(q_own, Q_AXIS, k) for k in range(1, n_q)]
    kv = exchanged(kv_copies, KV_AXES)
    n_kv = kv.shape[0]
    attend = pl.pallas_call(
        functools.partial(attend_kernel, factor=factor, tok=tok, n_ctx=n_tp),
        in_specs=[smem, smem] + [vmem] * 5,
        out_specs=vmem,
        out_shape=jax.ShapeDtypeStruct((n_q, 2 * n_c, quarter + 8, vsize), BF16),
        scratch_shapes=[
            pltpu.VMEM((n_kv, tok, nope + rope), BF16),
            pltpu.VMEM((n_kv * n_tp, nope + rope), BF16),
            pltpu.VMEM((n_kv * n_tp, vsize), BF16),
        ],
        name="attend",
    )
    out = attend(to, ctx_bias.reshape(1, 1), *queries, kv)

    got = exchanged(out.reshape(n_q * 2 * n_c, quarter + 8, vsize), (Q_AXIS, "yb", "c"))
    term = pl.pallas_call(
        merge_kernel,
        in_specs=[smem, vmem] + [any_space] * 4,
        out_specs=vmem,
        out_shape=jax.ShapeDtypeStruct((n_ya, rows, width), BF16),
        scratch_shapes=[pltpu.VMEM((4 * w_out.shape[0], width), BF16)] + [pltpu.SemaphoreType.DMA] * 4,
        name="merge",
    )(at, got.reshape(n_q, 2 * n_c, quarter + 8, vsize), w_out, w_other, w_near, w_far)
    branch = jnp.sum(exchanged(term, ("ya",)).astype(F32), axis=0)
    return (latent.astype(F32) + gate * branch).astype(BF16)


def solution(mesh):
    fine = Mesh(mesh.devices.reshape(4, 2, 4, 4, 2, 2), ("za", "zb", "x", "ya", "yb", "c"))
    row = P((*SP, *TP), None)
    placed = (
        row, P(), P(), row, P(SP, TP), P(SP, TP), P(SP, TP), P(), P(None, TP), P(None, TP), P(), P(), P(), P(None, TP),
        P(None, TP), P(TP), P(TP, None),
    )
    return jax.shard_map(step, mesh=fine, in_specs=placed, out_specs=row, check_vma=False)
```

```python
import functools

import jax
import jax.numpy as jnp
from jax import lax
from jax.experimental import pallas as pl
from jax.experimental.pallas import tpu as pltpu
from jax.sharding import Mesh
from jax.sharding import PartitionSpec as P


GRID_W = 128
EPS = 1e-06
ROPE_BASE = 10000.0
LOG2E = 1.4426950408889634
F32 = jnp.float32
BF16 = jnp.bfloat16
SP = ("za", "zb", "x")
Y = ("ya", "yb")
TP = ("ya", "yb", "c")
KV_AXES = ("zb", "x")
Q_AXIS = "za"


def exchanged(array, axes):
    return lax.all_to_all(array, axes, 0, 0, tiled=True)


def turn_table(positions, rope_dim, lanes):
    quarter = rope_dim // 4
    lane = jnp.arange(lanes, dtype=jnp.int32) % rope_dim
    inverse = ROPE_BASE ** (-(lane // 2 % quarter).astype(F32) / quarter)
    by_row = jnp.where(lane < rope_dim // 2, inverse, 0.0)
    by_column = jnp.where(lane < rope_dim // 2, 0.0, inverse)
    row = (positions // GRID_W).astype(F32)
    column = (positions % GRID_W).astype(F32)
    angle = row[:, None] * by_row[None, :] + column[:, None] * by_column[None, :]
    sign = jnp.where(lane % 2 == 0, -1.0, 1.0)
    return jnp.cos(angle), jnp.sin(angle) * sign[None, :]


def shifted(array, axis, k):
    n = lax.axis_size(axis)
    return lax.ppermute(array, axis, [(i, (i + k) % n) for i in range(n)])


def front_kernel(at_ref, cond_ref, mod_ref, shift_ref, scale_ref, gate_ref, o_ref):
    feat = shift_ref.shape[0]
    lanes = cond_ref.shape[1]
    per = lanes // feat
    rows = []
    for ref in (cond_ref, mod_ref):
        row = ref[pl.ds(at_ref[0, 0] // per, 1), :]
        row = jnp.where(at_ref[0, 0] % per == 0, row, pltpu.roll(row, lanes - feat, 1))
        rows.append(row / (1.0 + jnp.exp(-row)))
    pair = jnp.concatenate(rows + [jnp.zeros((6, lanes), F32)], axis=0)[:, :feat]
    shift, scale, gate = (
        jnp.dot(pair, ref[...], precision=lax.Precision.HIGHEST, preferred_element_type=F32) for ref in (shift_ref, scale_ref, gate_ref)
    )
    parts = jnp.concatenate([shift[:2], scale[:2], gate[:1]], axis=0)
    for i in range(o_ref.shape[0]):
        o_ref[i] = parts


def pack_kernel(sums_ref, block_ref, o_ref):
    n_sp = sums_ref.shape[0]
    rows, width = block_ref.shape
    total = functools.reduce(jnp.add, [sums_ref[i] for i in range(n_sp)])
    high = total.astype(BF16).astype(F32)
    middle = (total - high).astype(BF16).astype(F32)
    low = total - high - middle
    spare = jnp.zeros((rows - 3 * total.shape[0], total.shape[1]), F32)
    parts = jnp.concatenate([high, middle, low, spare], axis=0).astype(BF16)
    block = block_ref[...]
    for i in range(o_ref.shape[0]):
        o_ref[i, :, :width] = block
        o_ref[i, :, width:] = parts


def project_kernel(
    at_ref, own_ref, other_ref, gain_ref, kv_gain_ref, cos_ref, sin_ref, w_side_hbm, w_down_hbm, w_up_hbm,
    q_ref, kv_ref, gate_ref, ctx_ref, h_ref, w_side_ref, w_down_ref, w_up_ref, side_sem, down_sem, up_sem,
):
    loads = [
        pltpu.make_async_copy(w_side_hbm, w_side_ref, side_sem), pltpu.make_async_copy(w_down_hbm, w_down_ref, down_sem),
        pltpu.make_async_copy(w_up_hbm, w_up_ref, up_sem),
    ]
    for load in loads:
        load.start()
    n_y, rows, _ = own_ref.shape
    side_rows = n_y * rows
    tok = 2 * side_rows
    half = tok // 2
    width = gain_ref.shape[1]
    lanes = width // rows
    n_ctx = 2 * n_y
    core = at_ref[0, 0]
    columns = []
    for y in range(n_y):
        pair = []
        for ref in (own_ref, other_ref):
            part = ref[y, :, width + lanes :].astype(F32)
            pair.append(part[0:5] + part[5:10] + part[10:15])
        columns += [jnp.where(core == 0, pair[0], pair[1]), jnp.where(core == 0, pair[1], pair[0])]
    columns = jnp.concatenate(columns, axis=1)
    shift, shift_ctx, scale, scale_ctx = (columns[j : j + 1] for j in range(4))
    gate_ref[...] = columns[4:5]
    gain = gain_ref[...]

    def modulated(values, shift, scale):
        normed = values * lax.rsqrt(jnp.mean(values * values, axis=1, keepdims=True) + EPS)
        return (normed * (gain * (1.0 + scale)) + shift).astype(BF16)

    quarter = side_rows // 2
    for side, ref in enumerate((own_ref, other_ref)):
        ctx_ref[side * side_rows : (side + 1) * side_rows, :] = (
            ref[:, :, width : width + lanes].reshape(side_rows, lanes).astype(F32)
        )
        for yb in range(2):
            at = pl.multiple_of((yb * 2 + (core + side) % 2) * quarter, quarter)
            some = jnp.concatenate([ref[y, :, :width] for y in range(yb, n_y, 2)], axis=0)
            h_ref[pl.ds(at, quarter), :] = modulated(some.astype(F32), shift, scale)
    context = jnp.concatenate([ctx_ref[pl.ds(i, n_ctx, stride=rows), :] for i in range(rows)], axis=1)
    h_ref[tok:, :] = modulated(context, shift_ctx, scale_ctx)
    h = h_ref[...]
    loads[0].wait()
    mixed = jnp.dot(h, w_side_ref[...], preferred_element_type=F32)
    loads[1].wait()
    inner = jnp.dot(h, w_down_ref[...], preferred_element_type=F32)
    inner = (inner * lax.rsqrt(jnp.mean(inner * inner, axis=1, keepdims=True) + EPS) * kv_gain_ref[...]).astype(BF16)
    loads[2].wait()
    both = jnp.dot(inner, w_up_ref[...], preferred_element_type=F32).astype(BF16)
    q_ref[:tok, :] = mixed[:tok, :lanes].astype(BF16)
    pair = mixed[:, lanes:]
    own = pair[:tok]
    lane = lax.broadcasted_iota(jnp.int32, own.shape, 1)
    other = jnp.where(lane % 2 == 0, pltpu.roll(own, lanes - 1, 1), pltpu.roll(own, 1, 1))
    turned = own * cos_ref[...] + other * sin_ref[...]
    swapped = pltpu.roll(turned, lanes // 2, 1)
    low = lax.broadcasted_iota(jnp.int32, (half, lanes), 1) < lanes // 2
    q_ref[tok:, :] = jnp.where(low, turned[:half], swapped[half:]).astype(BF16)
    turned = jnp.where(low, swapped[:half], turned[half:]).astype(BF16)
    still = pltpu.roll(pair[tok:], lanes // 2, 1).astype(BF16)
    count = tok + n_ctx
    for i in range(kv_ref.shape[0]):
        kv_ref[i, :count, :] = both[:, :lanes]
        kv_ref[i, count : 2 * count, :] = both[:, lanes:]
        kv_ref[i, 2 * count : 2 * count + half, :] = turned
        kv_ref[i, 2 * count + half :, :] = still


def attend_kernel(place_ref, bias_ref, q0, q1, q2, q3, kv_ref, o_ref, k_ref, kc_ref, vc_ref, *, factor, tok, n_ctx):
    n_blocks, _, lanes = kv_ref.shape
    count = tok + n_ctx
    half = tok // 2
    rope = lanes // 2
    for i in range(n_blocks):
        k_ref[i, :, :lanes] = kv_ref[i, :tok]
        k_ref[i, :half, lanes:] = kv_ref[i, 2 * count : 2 * count + half, :rope]
        k_ref[i, half:, lanes:] = kv_ref[i, 2 * count : 2 * count + half, rope:]
        at = slice(i * n_ctx, (i + 1) * n_ctx)
        kc_ref[at, :lanes] = kv_ref[i, tok:count]
        kc_ref[at, lanes:] = kv_ref[i, 2 * count + half :, :rope]
        vc_ref[at, :] = kv_ref[i, count + tok : 2 * count]
    dims = (((1,), (1,)), ((), ()))
    step = factor * LOG2E
    bias = bias_ref[0, 0] * (1.0 / factor)
    blocks = (q0, q1, q2, q3)
    size = len(blocks)
    values = [kv_ref[i, count : count + tok] for i in range(n_blocks)] + [vc_ref[...]]
    quarter = tok // 4

    def scored(pair):
        pieces = []
        for block in pair:
            turned = jnp.concatenate([block[tok:, :rope], block[tok:, rope:]], axis=0)
            pieces.append(jnp.concatenate([block[:tok, :], turned], axis=1))
        q = jnp.concatenate(pieces, axis=0)
        scores = [lax.dot_general(q, k_ref[i], dims, preferred_element_type=F32) for i in range(n_blocks)]
        return scores + [lax.dot_general(q, kc_ref[...], dims, preferred_element_type=F32) + bias]

    ready = scored(blocks[:2])
    for first in range(0, size, 2):
        scores = ready
        if first + 2 < size:
            ready = scored(blocks[first + 2 : first + 4])
        widest = functools.reduce(jnp.maximum, scores[:-1])
        top = jnp.maximum(jnp.max(widest, axis=1, keepdims=True), jnp.max(scores[-1], axis=1, keepdims=True))
        weights = [jnp.exp2((s - top) * step) for s in scores]
        total = jnp.sum(functools.reduce(jnp.add, weights[:-1]), axis=1, keepdims=True) + jnp.sum(weights[-1], axis=1, keepdims=True)
        out = functools.reduce(
            jnp.add, [jnp.dot(w.astype(BF16), v, preferred_element_type=F32) for w, v in zip(weights, values, strict=True)]
        )
        out = (out / total).astype(BF16)
        lse = jnp.transpose(jnp.broadcast_to(top * step + jnp.log2(total), (2 * tok, lanes)))[:8]
        high = lse.astype(BF16).astype(F32)
        middle = (lse - high).astype(BF16).astype(F32)
        row = lax.broadcasted_iota(jnp.int32, lse.shape, 0)
        stats = jnp.where(row == 0, high, jnp.where(row == 1, middle, jnp.where(row == 2, lse - high - middle, 0.0))).astype(BF16)
        for k in range(2):
            to = (place_ref[0, 0] + (size - first - k)) % size
            for part in range(4):
                at = k * tok + part * quarter
                o_ref[to, part, :quarter, :] = out[at : at + quarter]
                o_ref[to, part, quarter:, :quarter] = stats[:, at : at + quarter]
                o_ref[to, part, quarter:, quarter:] = jnp.zeros((8, lanes - quarter), BF16)


def merge_kernel(at_ref, got_hbm, *refs):
    hbm, o_ref, w_ref, got_ref, sems, got_sem = refs[:4], refs[4], refs[5], refs[6], refs[7:11], refs[11]
    got_load = pltpu.make_async_copy(got_hbm, got_ref, got_sem)
    got_load.start()
    deep = hbm[0].shape[0]
    loads = [
        pltpu.make_async_copy(src, w_ref.at[pl.ds(i * deep, deep)], sem) for i, (src, sem) in enumerate(zip(hbm, sems, strict=True))
    ]
    for load in loads:
        load.start()
    n_q, _, height, lanes = got_ref.shape
    quarter = height - 8
    n_ya, rows, width = o_ref.shape
    core, yb = at_ref[0, 0], at_ref[0, 1]
    sources = [(yb + i) % 2 * 2 + (core + j) % 2 for i in range(2) for j in range(2)]
    got_load.wait()
    shares = []
    for source in sources:
        lse = [jnp.sum(got_ref[i, source, quarter:, :].astype(F32), axis=0, keepdims=True) for i in range(n_q)]
        top = functools.reduce(jnp.maximum, lse)
        raised = [jnp.exp2(v - top) for v in lse]
        total = functools.reduce(jnp.add, raised)
        shares += [v / total for v in raised]
    shares = jnp.transpose(jnp.concatenate(shares + [jnp.zeros((lanes - len(shares), lanes), F32)], axis=0))[:quarter]
    mixed = []
    for s, source in enumerate(sources):
        pieces = [got_ref[i, source, :quarter, :].astype(F32) * shares[:, s * n_q + i : s * n_q + i + 1] for i in range(n_q)]
        mixed.append(functools.reduce(jnp.add, pieces).astype(BF16))
    for load in loads:
        load.wait()
    term = jnp.dot(jnp.concatenate(mixed, axis=1), w_ref[...], preferred_element_type=F32)
    o_ref[...] = term.astype(BF16).reshape(n_ya, rows, width)


def step(
    latent, cond, ctx_mod, context, shift_w, scale_w, gate_w, norm_gain, w_qn, w_qr, w_kv_down, w_rope_key, kv_gain,
    w_key_up, w_value_up, ctx_bias, w_out,
):
    n_tp = lax.axis_size(TP)
    n_c = lax.axis_size("c")
    n_y = lax.axis_size(Y)
    n_ya = lax.axis_size("ya")
    n_q = lax.axis_size(Q_AXIS)
    sp_index = lax.axis_index(SP)
    rows, width = latent.shape
    lanes = width // rows
    tok = rows * n_tp
    quarter = tok // (2 * n_c)
    nope = w_key_up.shape[1]
    vsize = w_value_up.shape[1]
    rope = w_rope_key.shape[1]
    factor = (nope + rope) ** (-0.5)

    smem = pl.BlockSpec(memory_space=pltpu.SMEM)
    vmem = pl.BlockSpec(memory_space=pltpu.VMEM)
    parts = pl.pallas_call(
        front_kernel,
        in_specs=[smem] + [vmem] * 5,
        out_specs=vmem,
        out_shape=jax.ShapeDtypeStruct((lax.axis_size(SP), 5, lanes), F32),
        name="front",
    )(sp_index.astype(jnp.int32).reshape(1, 1), cond.reshape(-1, lanes), ctx_mod.reshape(-1, lanes), shift_w, scale_w, gate_w)
    summed = exchanged(parts, SP)
    w_near = shifted(w_out, "yb", 1)
    block = jnp.concatenate([latent, context.reshape(rows, lanes)], axis=1)
    smem = pl.BlockSpec(memory_space=pltpu.SMEM)
    vmem = pl.BlockSpec(memory_space=pltpu.VMEM)
    any_space = pl.BlockSpec(memory_space=pl.ANY)
    pack = pl.pallas_call(
        pack_kernel,
        in_specs=[vmem, vmem],
        out_specs=vmem,
        out_shape=jax.ShapeDtypeStruct((n_y, rows, width + 2 * lanes), BF16),
        name="pack",
    )
    message = pack(summed, block)

    mine = exchanged(message, Y)
    w_other = shifted(w_out, "c", 1)
    w_far = shifted(w_near, "c", 1)
    w_side = jnp.concatenate([w_qn, w_qr, w_rope_key], axis=1)
    w_up = jnp.concatenate([w_key_up, w_value_up], axis=1)
    place = jnp.arange(tok, dtype=jnp.int32)
    place = (place // rows % n_ya * 2 + place // (tok // 2)) * (n_c * rows) + place // quarter % n_c * rows + place % rows
    cosine, sine = turn_table(sp_index * tok + place, rope, lanes)
    at = jnp.stack([lax.axis_index("c"), lax.axis_index("yb")]).astype(jnp.int32).reshape(1, 2)
    to = lax.axis_index(Q_AXIS).astype(jnp.int32).reshape(1, 1)
    other = shifted(mine, "c", 1)

    project = pl.pallas_call(
        project_kernel,
        in_specs=[smem] + [vmem] * 6 + [any_space] * 3,
        out_specs=[vmem, vmem, vmem],
        out_shape=[
            jax.ShapeDtypeStruct((tok + tok // 2, lanes), BF16),
            jax.ShapeDtypeStruct((lax.axis_size(KV_AXES), 2 * (tok + n_tp) + tok // 2 + n_tp, lanes), BF16),
            jax.ShapeDtypeStruct((1, width), F32),
        ],
        scratch_shapes=[
            pltpu.VMEM((tok, lanes), F32),
            pltpu.VMEM((tok + n_tp, width), BF16),
            pltpu.VMEM(w_side.shape, BF16),
            pltpu.VMEM(w_kv_down.shape, BF16),
            pltpu.VMEM(w_up.shape, BF16),
            pltpu.SemaphoreType.DMA,
            pltpu.SemaphoreType.DMA,
            pltpu.SemaphoreType.DMA,
        ],
        name="project",
    )
    q_own, kv_copies, gate = project(
        at, mine, other, norm_gain.reshape(1, width), kv_gain.reshape(1, -1), cosine, sine, w_side, w_kv_down, w_up
    )

    queries = [q_own] + [shifted(q_own, Q_AXIS, k) for k in range(1, n_q)]
    kv = exchanged(kv_copies, KV_AXES)
    n_kv = kv.shape[0]
    attend = pl.pallas_call(
        functools.partial(attend_kernel, factor=factor, tok=tok, n_ctx=n_tp),
        in_specs=[smem, smem] + [vmem] * 5,
        out_specs=vmem,
        out_shape=jax.ShapeDtypeStruct((n_q, 2 * n_c, quarter + 8, vsize), BF16),
        scratch_shapes=[
            pltpu.VMEM((n_kv, tok, nope + rope), BF16),
            pltpu.VMEM((n_kv * n_tp, nope + rope), BF16),
            pltpu.VMEM((n_kv * n_tp, vsize), BF16),
        ],
        name="attend",
    )
    out = attend(to, ctx_bias.reshape(1, 1), *queries, kv)

    got = exchanged(out.reshape(n_q * 2 * n_c, quarter + 8, vsize), (Q_AXIS, "yb", "c"))
    term = pl.pallas_call(
        merge_kernel,
        in_specs=[smem] + [any_space] * 5,
        out_specs=vmem,
        out_shape=jax.ShapeDtypeStruct((n_ya, rows, width), BF16),
        scratch_shapes=[
            pltpu.VMEM((4 * w_out.shape[0], width), BF16),
            pltpu.VMEM((n_q, 2 * n_c, quarter + 8, vsize), BF16),
        ]
        + [pltpu.SemaphoreType.DMA] * 5,
        name="merge",
    )(at, got.reshape(n_q, 2 * n_c, quarter + 8, vsize), w_out, w_other, w_near, w_far)
    branch = jnp.sum(exchanged(term, ("ya",)).astype(F32), axis=0)
    return (latent.astype(F32) + gate * branch).astype(BF16)


def solution(mesh):
    fine = Mesh(mesh.devices.reshape(4, 2, 4, 4, 2, 2), ("za", "zb", "x", "ya", "yb", "c"))
    row = P((*SP, *TP), None)
    placed = (
        row, P(), P(), row, P(SP, TP), P(SP, TP), P(SP, TP), P(), P(None, TP), P(None, TP), P(), P(), P(), P(None, TP),
        P(None, TP), P(TP), P(TP, None),
    )
    return jax.shard_map(step, mesh=fine, in_specs=placed, out_specs=row, check_vma=False)
```

```python
import functools

import jax
import jax.numpy as jnp
from jax import lax
from jax.experimental import pallas as pl
from jax.experimental.pallas import tpu as pltpu
from jax.sharding import Mesh
from jax.sharding import PartitionSpec as P


GRID_W = 128
EPS = 1e-06
ROPE_BASE = 10000.0
LOG2E = 1.4426950408889634
F32 = jnp.float32
BF16 = jnp.bfloat16
SP = ("za", "zb", "x")
Y = ("ya", "yb")
TP = ("ya", "yb", "c")
KV_AXES = ("zb", "x")
Q_AXIS = "za"


def near(array):
    return pltpu.with_memory_space_constraint(array, pltpu.VMEM)


def exchanged(array, axes):
    return lax.all_to_all(array, axes, 0, 0, tiled=True)


def turn_table(positions, rope_dim, lanes):
    quarter = rope_dim // 4
    lane = jnp.arange(lanes, dtype=jnp.int32) % rope_dim
    inverse = ROPE_BASE ** (-(lane // 2 % quarter).astype(F32) / quarter)
    by_row = jnp.where(lane < rope_dim // 2, inverse, 0.0)
    by_column = jnp.where(lane < rope_dim // 2, 0.0, inverse)
    row = (positions // GRID_W).astype(F32)
    column = (positions % GRID_W).astype(F32)
    angle = row[:, None] * by_row[None, :] + column[:, None] * by_column[None, :]
    sign = jnp.where(lane % 2 == 0, -1.0, 1.0)
    return jnp.cos(angle), jnp.sin(angle) * sign[None, :]


def shifted(array, axis, k):
    n = lax.axis_size(axis)
    return lax.ppermute(array, axis, [(i, (i + k) % n) for i in range(n)])


def front_kernel(at_ref, cond_ref, mod_ref, shift_ref, scale_ref, gate_ref, o_ref):
    feat = shift_ref.shape[0]
    lanes = cond_ref.shape[1]
    per = lanes // feat
    rows = []
    for ref in (cond_ref, mod_ref):
        row = ref[pl.ds(at_ref[0, 0] // per, 1), :]
        row = jnp.where(at_ref[0, 0] % per == 0, row, pltpu.roll(row, lanes - feat, 1))
        rows.append(row / (1.0 + jnp.exp(-row)))
    pair = jnp.concatenate(rows + [jnp.zeros((6, lanes), F32)], axis=0)[:, :feat]
    shift, scale, gate = (
        jnp.dot(pair, ref[...], precision=lax.Precision.HIGHEST, preferred_element_type=F32) for ref in (shift_ref, scale_ref, gate_ref)
    )
    parts = jnp.concatenate([shift[:2], scale[:2], gate[:1]], axis=0)
    for i in range(o_ref.shape[0]):
        o_ref[i] = parts


def pack_kernel(sums_ref, block_ref, o_ref):
    n_sp = sums_ref.shape[0]
    rows, width = block_ref.shape
    total = functools.reduce(jnp.add, [sums_ref[i] for i in range(n_sp)])
    high = total.astype(BF16).astype(F32)
    middle = (total - high).astype(BF16).astype(F32)
    low = total - high - middle
    spare = jnp.zeros((rows - 3 * total.shape[0], total.shape[1]), F32)
    parts = jnp.concatenate([high, middle, low, spare], axis=0).astype(BF16)
    block = block_ref[...]
    for i in range(o_ref.shape[0]):
        o_ref[i, :, :width] = block
        o_ref[i, :, width:] = parts


def project_kernel(
    at_ref, own_ref, other_ref, gain_ref, kv_gain_ref, cos_ref, sin_ref, w_side_hbm, w_down_hbm, w_up_hbm,
    q_ref, kv_ref, gate_ref, ctx_ref, h_ref, w_side_ref, w_down_ref, w_up_ref, side_sem, down_sem, up_sem,
):
    loads = [
        pltpu.make_async_copy(w_side_hbm, w_side_ref, side_sem), pltpu.make_async_copy(w_down_hbm, w_down_ref, down_sem),
        pltpu.make_async_copy(w_up_hbm, w_up_ref, up_sem),
    ]
    for load in loads:
        load.start()
    n_y, rows, _ = own_ref.shape
    side_rows = n_y * rows
    tok = 2 * side_rows
    half = tok // 2
    width = gain_ref.shape[1]
    lanes = width // rows
    n_ctx = 2 * n_y
    core = at_ref[0, 0]
    columns = []
    for y in range(n_y):
        pair = []
        for ref in (own_ref, other_ref):
            part = ref[y, :, width + lanes :].astype(F32)
            pair.append(part[0:5] + part[5:10] + part[10:15])
        columns += [jnp.where(core == 0, pair[0], pair[1]), jnp.where(core == 0, pair[1], pair[0])]
    columns = jnp.concatenate(columns, axis=1)
    shift, shift_ctx, scale, scale_ctx = (columns[j : j + 1] for j in range(4))
    gate_ref[...] = columns[4:5]
    gain = gain_ref[...]

    def modulated(values, shift, scale):
        normed = values * lax.rsqrt(jnp.mean(values * values, axis=1, keepdims=True) + EPS)
        return (normed * (gain * (1.0 + scale)) + shift).astype(BF16)

    quarter = side_rows // 2
    for side, ref in enumerate((own_ref, other_ref)):
        ctx_ref[side * side_rows : (side + 1) * side_rows, :] = (
            ref[:, :, width : width + lanes].reshape(side_rows, lanes).astype(F32)
        )
        for yb in range(2):
            at = pl.multiple_of((yb * 2 + (core + side) % 2) * quarter, quarter)
            some = jnp.concatenate([ref[y, :, :width] for y in range(yb, n_y, 2)], axis=0)
            h_ref[pl.ds(at, quarter), :] = modulated(some.astype(F32), shift, scale)
    context = jnp.concatenate([ctx_ref[pl.ds(i, n_ctx, stride=rows), :] for i in range(rows)], axis=1)
    h_ref[tok:, :] = modulated(context, shift_ctx, scale_ctx)
    h = h_ref[...]
    loads[0].wait()
    mixed = jnp.dot(h, w_side_ref[...], preferred_element_type=F32)
    loads[1].wait()
    inner = jnp.dot(h, w_down_ref[...], preferred_element_type=F32)
    inner = (inner * lax.rsqrt(jnp.mean(inner * inner, axis=1, keepdims=True) + EPS) * kv_gain_ref[...]).astype(BF16)
    loads[2].wait()
    both = jnp.dot(inner, w_up_ref[...], preferred_element_type=F32).astype(BF16)
    q_ref[:tok, :] = mixed[:tok, :lanes].astype(BF16)
    pair = mixed[:, lanes:]
    own = pair[:tok]
    lane = lax.broadcasted_iota(jnp.int32, own.shape, 1)
    other = jnp.where(lane % 2 == 0, pltpu.roll(own, lanes - 1, 1), pltpu.roll(own, 1, 1))
    turned = own * cos_ref[...] + other * sin_ref[...]
    swapped = pltpu.roll(turned, lanes // 2, 1)
    low = lax.broadcasted_iota(jnp.int32, (half, lanes), 1) < lanes // 2
    q_ref[tok:, :] = jnp.where(low, turned[:half], swapped[half:]).astype(BF16)
    turned = jnp.where(low, swapped[:half], turned[half:]).astype(BF16)
    still = pltpu.roll(pair[tok:], lanes // 2, 1).astype(BF16)
    count = tok + n_ctx
    for i in range(kv_ref.shape[0]):
        kv_ref[i, :count, :] = both[:, :lanes]
        kv_ref[i, count : 2 * count, :] = both[:, lanes:]
        kv_ref[i, 2 * count : 2 * count + half, :] = turned
        kv_ref[i, 2 * count + half :, :] = still


def attend_kernel(place_ref, bias_ref, q0, q1, q2, q3, kv_ref, o_ref, k_ref, kc_ref, vc_ref, *, factor, tok, n_ctx):
    n_blocks, _, lanes = kv_ref.shape
    count = tok + n_ctx
    half = tok // 2
    rope = lanes // 2
    for i in range(n_blocks):
        k_ref[i, :, :lanes] = kv_ref[i, :tok]
        k_ref[i, :half, lanes:] = kv_ref[i, 2 * count : 2 * count + half, :rope]
        k_ref[i, half:, lanes:] = kv_ref[i, 2 * count : 2 * count + half, rope:]
        at = slice(i * n_ctx, (i + 1) * n_ctx)
        kc_ref[at, :lanes] = kv_ref[i, tok:count]
        kc_ref[at, lanes:] = kv_ref[i, 2 * count + half :, :rope]
        vc_ref[at, :] = kv_ref[i, count + tok : 2 * count]
    dims = (((1,), (1,)), ((), ()))
    step = factor * LOG2E
    bias = bias_ref[0, 0] * (1.0 / factor)
    blocks = (q0, q1, q2, q3)
    size = len(blocks)
    values = [kv_ref[i, count : count + tok] for i in range(n_blocks)] + [vc_ref[...]]
    quarter = tok // 4

    def scored(pair):
        pieces = []
        for block in pair:
            turned = jnp.concatenate([block[tok:, :rope], block[tok:, rope:]], axis=0)
            pieces.append(jnp.concatenate([block[:tok, :], turned], axis=1))
        q = jnp.concatenate(pieces, axis=0)
        scores = [lax.dot_general(q, k_ref[i], dims, preferred_element_type=F32) for i in range(n_blocks)]
        return scores + [lax.dot_general(q, kc_ref[...], dims, preferred_element_type=F32) + bias]

    ready = scored(blocks[:2])
    for first in range(0, size, 2):
        scores = ready
        if first + 2 < size:
            ready = scored(blocks[first + 2 : first + 4])
        widest = functools.reduce(jnp.maximum, scores[:-1])
        top = jnp.maximum(jnp.max(widest, axis=1, keepdims=True), jnp.max(scores[-1], axis=1, keepdims=True))
        weights = [jnp.exp2((s - top) * step) for s in scores]
        total = jnp.sum(functools.reduce(jnp.add, weights[:-1]), axis=1, keepdims=True) + jnp.sum(weights[-1], axis=1, keepdims=True)
        out = functools.reduce(
            jnp.add, [jnp.dot(w.astype(BF16), v, preferred_element_type=F32) for w, v in zip(weights, values, strict=True)]
        )
        out = (out / total).astype(BF16)
        lse = jnp.transpose(jnp.broadcast_to(top * step + jnp.log2(total), (2 * tok, lanes)))[:8]
        high = lse.astype(BF16).astype(F32)
        middle = (lse - high).astype(BF16).astype(F32)
        row = lax.broadcasted_iota(jnp.int32, lse.shape, 0)
        stats = jnp.where(row == 0, high, jnp.where(row == 1, middle, jnp.where(row == 2, lse - high - middle, 0.0))).astype(BF16)
        for k in range(2):
            to = (place_ref[0, 0] + (size - first - k)) % size
            for part in range(4):
                at = k * tok + part * quarter
                o_ref[to, part, :quarter, :] = out[at : at + quarter]
                o_ref[to, part, quarter:, :quarter] = stats[:, at : at + quarter]
                o_ref[to, part, quarter:, quarter:] = jnp.zeros((8, lanes - quarter), BF16)


def merge_kernel(at_ref, got_ref, *refs):
    hbm, o_ref, w_ref, sems = refs[:4], refs[4], refs[5], refs[6:]
    deep = hbm[0].shape[0]
    loads = [
        pltpu.make_async_copy(src, w_ref.at[pl.ds(i * deep, deep)], sem) for i, (src, sem) in enumerate(zip(hbm, sems, strict=True))
    ]
    for load in loads:
        load.start()
    n_q, _, height, lanes = got_ref.shape
    quarter = height - 8
    n_ya, rows, width = o_ref.shape
    core, yb = at_ref[0, 0], at_ref[0, 1]
    sources = [(yb + i) % 2 * 2 + (core + j) % 2 for i in range(2) for j in range(2)]
    shares = []
    for source in sources:
        lse = [jnp.sum(got_ref[i, source, quarter:, :].astype(F32), axis=0, keepdims=True) for i in range(n_q)]
        top = functools.reduce(jnp.maximum, lse)
        raised = [jnp.exp2(v - top) for v in lse]
        total = functools.reduce(jnp.add, raised)
        shares += [v / total for v in raised]
    shares = jnp.transpose(jnp.concatenate(shares + [jnp.zeros((lanes - len(shares), lanes), F32)], axis=0))[:quarter]
    mixed = []
    for s, source in enumerate(sources):
        pieces = [got_ref[i, source, :quarter, :].astype(F32) * shares[:, s * n_q + i : s * n_q + i + 1] for i in range(n_q)]
        mixed.append(functools.reduce(jnp.add, pieces).astype(BF16))
    for load in loads:
        load.wait()
    term = jnp.dot(jnp.concatenate(mixed, axis=1), w_ref[...], preferred_element_type=F32)
    o_ref[...] = term.astype(BF16).reshape(n_ya, rows, width)


def step(
    latent, cond, ctx_mod, context, shift_w, scale_w, gate_w, norm_gain, w_qn, w_qr, w_kv_down, w_rope_key, kv_gain,
    w_key_up, w_value_up, ctx_bias, w_out,
):
    n_tp = lax.axis_size(TP)
    n_c = lax.axis_size("c")
    n_y = lax.axis_size(Y)
    n_ya = lax.axis_size("ya")
    n_q = lax.axis_size(Q_AXIS)
    sp_index = lax.axis_index(SP)
    rows, width = latent.shape
    lanes = width // rows
    tok = rows * n_tp
    quarter = tok // (2 * n_c)
    nope = w_key_up.shape[1]
    vsize = w_value_up.shape[1]
    rope = w_rope_key.shape[1]
    factor = (nope + rope) ** (-0.5)

    smem = pl.BlockSpec(memory_space=pltpu.SMEM)
    vmem = pl.BlockSpec(memory_space=pltpu.VMEM)
    parts = pl.pallas_call(
        front_kernel,
        in_specs=[smem] + [vmem] * 5,
        out_specs=vmem,
        out_shape=jax.ShapeDtypeStruct((lax.axis_size(SP), 5, lanes), F32),
        name="front",
    )(sp_index.astype(jnp.int32).reshape(1, 1), cond.reshape(-1, lanes), ctx_mod.reshape(-1, lanes), shift_w, scale_w, gate_w)
    summed = exchanged(parts, SP)
    w_near = shifted(w_out, "yb", 1)
    block = jnp.concatenate([latent, context.reshape(rows, lanes)], axis=1)
    smem = pl.BlockSpec(memory_space=pltpu.SMEM)
    vmem = pl.BlockSpec(memory_space=pltpu.VMEM)
    any_space = pl.BlockSpec(memory_space=pl.ANY)
    pack = pl.pallas_call(
        pack_kernel,
        in_specs=[vmem, vmem],
        out_specs=vmem,
        out_shape=jax.ShapeDtypeStruct((n_y, rows, width + 2 * lanes), BF16),
        name="pack",
    )
    message = pack(near(summed), near(block))

    mine = exchanged(message, Y)
    w_other = shifted(w_out, "c", 1)
    w_far = shifted(w_near, "c", 1)
    w_side = jnp.concatenate([w_qn, w_qr, w_rope_key], axis=1)
    w_up = jnp.concatenate([w_key_up, w_value_up], axis=1)
    place = jnp.arange(tok, dtype=jnp.int32)
    place = (place // rows % n_ya * 2 + place // (tok // 2)) * (n_c * rows) + place // quarter % n_c * rows + place % rows
    cosine, sine = turn_table(sp_index * tok + place, rope, lanes)
    at = jnp.stack([lax.axis_index("c"), lax.axis_index("yb")]).astype(jnp.int32).reshape(1, 2)
    to = lax.axis_index(Q_AXIS).astype(jnp.int32).reshape(1, 1)
    other = shifted(mine, "c", 1)

    project = pl.pallas_call(
        project_kernel,
        in_specs=[smem] + [vmem] * 6 + [any_space] * 3,
        out_specs=[vmem, vmem, vmem],
        out_shape=[
            pltpu.VMEM((tok + tok // 2, lanes), BF16),
            jax.ShapeDtypeStruct((lax.axis_size(KV_AXES), 2 * (tok + n_tp) + tok // 2 + n_tp, lanes), BF16),
            jax.ShapeDtypeStruct((1, width), F32),
        ],
        scratch_shapes=[
            pltpu.VMEM((tok, lanes), F32),
            pltpu.VMEM((tok + n_tp, width), BF16),
            pltpu.VMEM(w_side.shape, BF16),
            pltpu.VMEM(w_kv_down.shape, BF16),
            pltpu.VMEM(w_up.shape, BF16),
            pltpu.SemaphoreType.DMA,
            pltpu.SemaphoreType.DMA,
            pltpu.SemaphoreType.DMA,
        ],
        name="project",
    )
    q_own, kv_copies, gate = project(
        at, near(mine), near(other), norm_gain.reshape(1, width), kv_gain.reshape(1, -1), cosine, sine, w_side, w_kv_down, w_up
    )

    queries = [q_own] + [shifted(q_own, Q_AXIS, k) for k in range(1, n_q)]
    kv = exchanged(kv_copies, KV_AXES)
    n_kv = kv.shape[0]
    attend = pl.pallas_call(
        functools.partial(attend_kernel, factor=factor, tok=tok, n_ctx=n_tp),
        in_specs=[smem, smem] + [vmem] * 5,
        out_specs=vmem,
        out_shape=jax.ShapeDtypeStruct((n_q, 2 * n_c, quarter + 8, vsize), BF16),
        scratch_shapes=[
            pltpu.VMEM((n_kv, tok, nope + rope), BF16),
            pltpu.VMEM((n_kv * n_tp, nope + rope), BF16),
            pltpu.VMEM((n_kv * n_tp, vsize), BF16),
        ],
        name="attend",
    )
    out = attend(to, ctx_bias.reshape(1, 1), *(near(q) for q in queries), near(kv))

    got = exchanged(out.reshape(n_q * 2 * n_c, quarter + 8, vsize), (Q_AXIS, "yb", "c"))
    term = pl.pallas_call(
        merge_kernel,
        in_specs=[smem, vmem] + [any_space] * 4,
        out_specs=vmem,
        out_shape=pltpu.VMEM((n_ya, rows, width), BF16),
        scratch_shapes=[
            pltpu.VMEM((4 * w_out.shape[0], width), BF16),
        ]
        + [pltpu.SemaphoreType.DMA] * 4,
        name="merge",
    )(at, near(got.reshape(n_q, 2 * n_c, quarter + 8, vsize)), w_out, w_other, w_near, w_far)
    branch = jnp.sum(exchanged(term, ("ya",)).astype(F32), axis=0)
    return (latent.astype(F32) + gate * branch).astype(BF16)


def solution(mesh):
    fine = Mesh(mesh.devices.reshape(4, 2, 4, 4, 2, 2), ("za", "zb", "x", "ya", "yb", "c"))
    row = P((*SP, *TP), None)
    placed = (
        row, P(), P(), row, P(SP, TP), P(SP, TP), P(SP, TP), P(), P(None, TP), P(None, TP), P(), P(), P(), P(None, TP),
        P(None, TP), P(TP), P(TP, None),
    )
    return jax.shard_map(step, mesh=fine, in_specs=placed, out_specs=row, check_vma=False)
```

```python
import functools

import jax
import jax.numpy as jnp
from jax import lax
from jax.experimental import pallas as pl
from jax.experimental.pallas import tpu as pltpu
from jax.sharding import Mesh
from jax.sharding import PartitionSpec as P


GRID_W = 128
EPS = 1e-06
ROPE_BASE = 10000.0
LOG2E = 1.4426950408889634
F32 = jnp.float32
BF16 = jnp.bfloat16
SP = ("za", "zb", "x")
Y = ("ya", "yb")
TP = ("ya", "yb", "c")
KV_AXES = ("zb", "x")
Q_AXIS = "za"


def near(array):
    return pltpu.with_memory_space_constraint(array, pltpu.VMEM)


def exchanged(array, axes):
    return lax.all_to_all(array, axes, 0, 0, tiled=True)


def turn_table(positions, rope_dim, lanes):
    quarter = rope_dim // 4
    lane = jnp.arange(lanes, dtype=jnp.int32) % rope_dim
    inverse = ROPE_BASE ** (-(lane // 2 % quarter).astype(F32) / quarter)
    by_row = jnp.where(lane < rope_dim // 2, inverse, 0.0)
    by_column = jnp.where(lane < rope_dim // 2, 0.0, inverse)
    row = (positions // GRID_W).astype(F32)
    column = (positions % GRID_W).astype(F32)
    angle = row[:, None] * by_row[None, :] + column[:, None] * by_column[None, :]
    sign = jnp.where(lane % 2 == 0, -1.0, 1.0)
    return jnp.cos(angle), jnp.sin(angle) * sign[None, :]


def shifted(array, axis, k):
    n = lax.axis_size(axis)
    return lax.ppermute(array, axis, [(i, (i + k) % n) for i in range(n)])


def front_kernel(at_ref, cond_ref, mod_ref, shift_ref, scale_ref, gate_ref, o_ref):
    feat = shift_ref.shape[0]
    lanes = cond_ref.shape[1]
    per = lanes // feat
    rows = []
    for ref in (cond_ref, mod_ref):
        row = ref[pl.ds(at_ref[0, 0] // per, 1), :]
        row = jnp.where(at_ref[0, 0] % per == 0, row, pltpu.roll(row, lanes - feat, 1))
        rows.append(row / (1.0 + jnp.exp(-row)))
    pair = jnp.concatenate(rows + [jnp.zeros((6, lanes), F32)], axis=0)[:, :feat]
    shift, scale, gate = (
        jnp.dot(pair, ref[...], precision=lax.Precision.HIGHEST, preferred_element_type=F32) for ref in (shift_ref, scale_ref, gate_ref)
    )
    parts = jnp.concatenate([shift[:2], scale[:2], gate[:1]], axis=0)
    for i in range(o_ref.shape[0]):
        o_ref[i] = parts


def pack_kernel(sums_ref, block_ref, o_ref):
    n_sp = sums_ref.shape[0]
    rows, width = block_ref.shape
    total = functools.reduce(jnp.add, [sums_ref[i] for i in range(n_sp)])
    high = total.astype(BF16).astype(F32)
    middle = (total - high).astype(BF16).astype(F32)
    low = total - high - middle
    spare = jnp.zeros((rows - 3 * total.shape[0], total.shape[1]), F32)
    parts = jnp.concatenate([high, middle, low, spare], axis=0).astype(BF16)
    block = block_ref[...]
    for i in range(o_ref.shape[0]):
        o_ref[i, :, :width] = block
        o_ref[i, :, width:] = parts


def project_kernel(
    at_ref, own_ref, other_ref, gain_ref, kv_gain_ref, cos_ref, sin_ref, w_side_ref, w_up_ref, w_down_hbm,
    q_ref, kv_ref, gate_ref, ctx_ref, h_ref, w_down_ref, down_sem,
):
    load = pltpu.make_async_copy(w_down_hbm, w_down_ref, down_sem)
    load.start()
    n_y, rows, _ = own_ref.shape
    side_rows = n_y * rows
    tok = 2 * side_rows
    half = tok // 2
    width = gain_ref.shape[1]
    lanes = width // rows
    n_ctx = 2 * n_y
    core = at_ref[0, 0]
    columns = []
    for y in range(n_y):
        pair = []
        for ref in (own_ref, other_ref):
            part = ref[y, :, width + lanes :].astype(F32)
            pair.append(part[0:5] + part[5:10] + part[10:15])
        columns += [jnp.where(core == 0, pair[0], pair[1]), jnp.where(core == 0, pair[1], pair[0])]
    columns = jnp.concatenate(columns, axis=1)
    shift, shift_ctx, scale, scale_ctx = (columns[j : j + 1] for j in range(4))
    gate_ref[...] = columns[4:5]
    gain = gain_ref[...]

    def modulated(values, shift, scale):
        normed = values * lax.rsqrt(jnp.mean(values * values, axis=1, keepdims=True) + EPS)
        return (normed * (gain * (1.0 + scale)) + shift).astype(BF16)

    quarter = side_rows // 2
    for side, ref in enumerate((own_ref, other_ref)):
        ctx_ref[side * side_rows : (side + 1) * side_rows, :] = (
            ref[:, :, width : width + lanes].reshape(side_rows, lanes).astype(F32)
        )
        for yb in range(2):
            at = pl.multiple_of((yb * 2 + (core + side) % 2) * quarter, quarter)
            some = jnp.concatenate([ref[y, :, :width] for y in range(yb, n_y, 2)], axis=0)
            h_ref[pl.ds(at, quarter), :] = modulated(some.astype(F32), shift, scale)
    context = jnp.concatenate([ctx_ref[pl.ds(i, n_ctx, stride=rows), :] for i in range(rows)], axis=1)
    h_ref[tok:, :] = modulated(context, shift_ctx, scale_ctx)
    h = h_ref[...]
    mixed = jnp.dot(h, w_side_ref[...], preferred_element_type=F32)
    load.wait()
    inner = jnp.dot(h, w_down_ref[...], preferred_element_type=F32)
    inner = (inner * lax.rsqrt(jnp.mean(inner * inner, axis=1, keepdims=True) + EPS) * kv_gain_ref[...]).astype(BF16)
    both = jnp.dot(inner, w_up_ref[...], preferred_element_type=F32).astype(BF16)
    q_ref[:tok, :] = mixed[:tok, :lanes].astype(BF16)
    pair = mixed[:, lanes:]
    own = pair[:tok]
    lane = lax.broadcasted_iota(jnp.int32, own.shape, 1)
    other = jnp.where(lane % 2 == 0, pltpu.roll(own, lanes - 1, 1), pltpu.roll(own, 1, 1))
    turned = own * cos_ref[...] + other * sin_ref[...]
    swapped = pltpu.roll(turned, lanes // 2, 1)
    low = lax.broadcasted_iota(jnp.int32, (half, lanes), 1) < lanes // 2
    q_ref[tok:, :] = jnp.where(low, turned[:half], swapped[half:]).astype(BF16)
    turned = jnp.where(low, swapped[:half], turned[half:]).astype(BF16)
    still = pltpu.roll(pair[tok:], lanes // 2, 1).astype(BF16)
    count = tok + n_ctx
    for i in range(kv_ref.shape[0]):
        kv_ref[i, :count, :] = both[:, :lanes]
        kv_ref[i, count : 2 * count, :] = both[:, lanes:]
        kv_ref[i, 2 * count : 2 * count + half, :] = turned
        kv_ref[i, 2 * count + half :, :] = still


def attend_kernel(place_ref, bias_ref, q0, q1, q2, q3, kv_ref, o_ref, k_ref, kc_ref, vc_ref, *, factor, tok, n_ctx):
    n_blocks, _, lanes = kv_ref.shape
    count = tok + n_ctx
    half = tok // 2
    rope = lanes // 2
    for i in range(n_blocks):
        k_ref[i, :, :lanes] = kv_ref[i, :tok]
        k_ref[i, :half, lanes:] = kv_ref[i, 2 * count : 2 * count + half, :rope]
        k_ref[i, half:, lanes:] = kv_ref[i, 2 * count : 2 * count + half, rope:]
        at = slice(i * n_ctx, (i + 1) * n_ctx)
        kc_ref[at, :lanes] = kv_ref[i, tok:count]
        kc_ref[at, lanes:] = kv_ref[i, 2 * count + half :, :rope]
        vc_ref[at, :] = kv_ref[i, count + tok : 2 * count]
    dims = (((1,), (1,)), ((), ()))
    step = factor * LOG2E
    bias = bias_ref[0, 0] * (1.0 / factor)
    blocks = (q0, q1, q2, q3)
    size = len(blocks)
    values = [kv_ref[i, count : count + tok] for i in range(n_blocks)] + [vc_ref[...]]
    quarter = tok // 4

    def scored(pair):
        pieces = []
        for block in pair:
            turned = jnp.concatenate([block[tok:, :rope], block[tok:, rope:]], axis=0)
            pieces.append(jnp.concatenate([block[:tok, :], turned], axis=1))
        q = jnp.concatenate(pieces, axis=0)
        scores = [lax.dot_general(q, k_ref[i], dims, preferred_element_type=F32) for i in range(n_blocks)]
        return scores + [lax.dot_general(q, kc_ref[...], dims, preferred_element_type=F32) + bias]

    ready = scored(blocks[:2])
    for first in range(0, size, 2):
        scores = ready
        if first + 2 < size:
            ready = scored(blocks[first + 2 : first + 4])
        widest = functools.reduce(jnp.maximum, scores[:-1])
        top = jnp.maximum(jnp.max(widest, axis=1, keepdims=True), jnp.max(scores[-1], axis=1, keepdims=True))
        weights = [jnp.exp2((s - top) * step) for s in scores]
        total = jnp.sum(functools.reduce(jnp.add, weights[:-1]), axis=1, keepdims=True) + jnp.sum(weights[-1], axis=1, keepdims=True)
        out = functools.reduce(
            jnp.add, [jnp.dot(w.astype(BF16), v, preferred_element_type=F32) for w, v in zip(weights, values, strict=True)]
        )
        out = (out / total).astype(BF16)
        lse = jnp.transpose(jnp.broadcast_to(top * step + jnp.log2(total), (2 * tok, lanes)))[:8]
        high = lse.astype(BF16).astype(F32)
        middle = (lse - high).astype(BF16).astype(F32)
        row = lax.broadcasted_iota(jnp.int32, lse.shape, 0)
        stats = jnp.where(row == 0, high, jnp.where(row == 1, middle, jnp.where(row == 2, lse - high - middle, 0.0))).astype(BF16)
        for k in range(2):
            to = (place_ref[0, 0] + (size - first - k)) % size
            for part in range(4):
                at = k * tok + part * quarter
                o_ref[to, part, :quarter, :] = out[at : at + quarter]
                o_ref[to, part, quarter:, :quarter] = stats[:, at : at + quarter]
                o_ref[to, part, quarter:, quarter:] = jnp.zeros((8, lanes - quarter), BF16)


def merge_kernel(at_ref, got_ref, *refs):
    hbm, o_ref, w_ref, sems = refs[:4], refs[4], refs[5], refs[6:]
    deep = hbm[0].shape[0]
    loads = [
        pltpu.make_async_copy(src, w_ref.at[pl.ds(i * deep, deep)], sem) for i, (src, sem) in enumerate(zip(hbm, sems, strict=True))
    ]
    for load in loads:
        load.start()
    n_q, _, height, lanes = got_ref.shape
    quarter = height - 8
    n_ya, rows, width = o_ref.shape
    core, yb = at_ref[0, 0], at_ref[0, 1]
    sources = [(yb + i) % 2 * 2 + (core + j) % 2 for i in range(2) for j in range(2)]
    shares = []
    for source in sources:
        lse = [jnp.sum(got_ref[i, source, quarter:, :].astype(F32), axis=0, keepdims=True) for i in range(n_q)]
        top = functools.reduce(jnp.maximum, lse)
        raised = [jnp.exp2(v - top) for v in lse]
        total = functools.reduce(jnp.add, raised)
        shares += [v / total for v in raised]
    shares = jnp.transpose(jnp.concatenate(shares + [jnp.zeros((lanes - len(shares), lanes), F32)], axis=0))[:quarter]
    mixed = []
    for s, source in enumerate(sources):
        pieces = [got_ref[i, source, :quarter, :].astype(F32) * shares[:, s * n_q + i : s * n_q + i + 1] for i in range(n_q)]
        mixed.append(functools.reduce(jnp.add, pieces).astype(BF16))
    for load in loads:
        load.wait()
    term = jnp.dot(jnp.concatenate(mixed, axis=1), w_ref[...], preferred_element_type=F32)
    o_ref[...] = term.astype(BF16).reshape(n_ya, rows, width)


def step(
    latent, cond, ctx_mod, context, shift_w, scale_w, gate_w, norm_gain, w_qn, w_qr, w_kv_down, w_rope_key, kv_gain,
    w_key_up, w_value_up, ctx_bias, w_out,
):
    n_tp = lax.axis_size(TP)
    n_c = lax.axis_size("c")
    n_y = lax.axis_size(Y)
    n_ya = lax.axis_size("ya")
    n_q = lax.axis_size(Q_AXIS)
    sp_index = lax.axis_index(SP)
    rows, width = latent.shape
    lanes = width // rows
    tok = rows * n_tp
    quarter = tok // (2 * n_c)
    nope = w_key_up.shape[1]
    vsize = w_value_up.shape[1]
    rope = w_rope_key.shape[1]
    factor = (nope + rope) ** (-0.5)

    smem = pl.BlockSpec(memory_space=pltpu.SMEM)
    vmem = pl.BlockSpec(memory_space=pltpu.VMEM)
    parts = pl.pallas_call(
        front_kernel,
        in_specs=[smem] + [vmem] * 5,
        out_specs=vmem,
        out_shape=jax.ShapeDtypeStruct((lax.axis_size(SP), 5, lanes), F32),
        name="front",
    )(sp_index.astype(jnp.int32).reshape(1, 1), cond.reshape(-1, lanes), ctx_mod.reshape(-1, lanes), shift_w, scale_w, gate_w)
    summed = exchanged(parts, SP)
    w_near = shifted(w_out, "yb", 1)
    block = jnp.concatenate([latent, context.reshape(rows, lanes)], axis=1)
    smem = pl.BlockSpec(memory_space=pltpu.SMEM)
    vmem = pl.BlockSpec(memory_space=pltpu.VMEM)
    any_space = pl.BlockSpec(memory_space=pl.ANY)
    pack = pl.pallas_call(
        pack_kernel,
        in_specs=[vmem, vmem],
        out_specs=vmem,
        out_shape=jax.ShapeDtypeStruct((n_y, rows, width + 2 * lanes), BF16),
        name="pack",
    )
    message = pack(near(summed), near(block))

    mine = exchanged(message, Y)
    w_other = shifted(w_out, "c", 1)
    w_far = shifted(w_near, "c", 1)
    w_side = jnp.concatenate([w_qn, w_qr, w_rope_key], axis=1)
    w_up = jnp.concatenate([w_key_up, w_value_up], axis=1)
    place = jnp.arange(tok, dtype=jnp.int32)
    place = (place // rows % n_ya * 2 + place // (tok // 2)) * (n_c * rows) + place // quarter % n_c * rows + place % rows
    cosine, sine = turn_table(sp_index * tok + place, rope, lanes)
    at = jnp.stack([lax.axis_index("c"), lax.axis_index("yb")]).astype(jnp.int32).reshape(1, 2)
    to = lax.axis_index(Q_AXIS).astype(jnp.int32).reshape(1, 1)
    other = shifted(mine, "c", 1)

    project = pl.pallas_call(
        project_kernel,
        in_specs=[smem] + [vmem] * 8 + [any_space],
        out_specs=[vmem, vmem, vmem],
        out_shape=[
            pltpu.VMEM((tok + tok // 2, lanes), BF16),
            jax.ShapeDtypeStruct((lax.axis_size(KV_AXES), 2 * (tok + n_tp) + tok // 2 + n_tp, lanes), BF16),
            jax.ShapeDtypeStruct((1, width), F32),
        ],
        scratch_shapes=[
            pltpu.VMEM((tok, lanes), F32),
            pltpu.VMEM((tok + n_tp, width), BF16),
            pltpu.VMEM(w_kv_down.shape, BF16),
            pltpu.SemaphoreType.DMA,
        ],
        name="project",
    )
    q_own, kv_copies, gate = project(
        at, near(mine), near(other), norm_gain.reshape(1, width), kv_gain.reshape(1, -1), near(cosine), near(sine), near(w_side),
        near(w_up), w_kv_down,
    )

    far = shifted(q_own, Q_AXIS, n_q // 2)
    queries = [q_own, shifted(q_own, Q_AXIS, 1), far, shifted(q_own, Q_AXIS, n_q - 1)]
    kv = exchanged(kv_copies, KV_AXES)
    n_kv = kv.shape[0]
    attend = pl.pallas_call(
        functools.partial(attend_kernel, factor=factor, tok=tok, n_ctx=n_tp),
        in_specs=[smem, smem] + [vmem] * 5,
        out_specs=vmem,
        out_shape=jax.ShapeDtypeStruct((n_q, 2 * n_c, quarter + 8, vsize), BF16),
        scratch_shapes=[
            pltpu.VMEM((n_kv, tok, nope + rope), BF16),
            pltpu.VMEM((n_kv * n_tp, nope + rope), BF16),
            pltpu.VMEM((n_kv * n_tp, vsize), BF16),
        ],
        name="attend",
    )
    out = attend(to, ctx_bias.reshape(1, 1), *(near(q) for q in queries), near(kv))

    got = exchanged(out.reshape(n_q * 2 * n_c, quarter + 8, vsize), (Q_AXIS, "yb", "c"))
    term = pl.pallas_call(
        merge_kernel,
        in_specs=[smem, vmem] + [any_space] * 4,
        out_specs=vmem,
        out_shape=pltpu.VMEM((n_ya, rows, width), BF16),
        scratch_shapes=[
            pltpu.VMEM((4 * w_out.shape[0], width), BF16),
        ]
        + [pltpu.SemaphoreType.DMA] * 4,
        name="merge",
    )(at, near(got.reshape(n_q, 2 * n_c, quarter + 8, vsize)), w_out, w_other, w_near, w_far)
    branch = jnp.sum(exchanged(term, ("ya",)).astype(F32), axis=0)
    return (latent.astype(F32) + gate * branch).astype(BF16)


def solution(mesh):
    fine = Mesh(mesh.devices.reshape(4, 2, 4, 4, 2, 2), ("za", "zb", "x", "ya", "yb", "c"))
    row = P((*SP, *TP), None)
    placed = (
        row, P(), P(), row, P(SP, TP), P(SP, TP), P(SP, TP), P(), P(None, TP), P(None, TP), P(), P(), P(), P(None, TP),
        P(None, TP), P(TP), P(TP, None),
    )
    return jax.shard_map(step, mesh=fine, in_specs=placed, out_specs=row, check_vma=False)
```
